256 devices in a mesh: grp: 2 (over y), sp: 32 (over z, core), tp: 4 (over x).
Axes of the slice: x: 4, y: 2, z: 16, core: 2. Of those that a mesh axis runs over, the one named last changes fastest.
The devices are a block of a 4x16x16 slice.
Arguments:
- queries: bfloat16 [32768, 2048], P(('grp', 'sp'), 'tp'), parts along dimension 0, may hold values from -64 to 64
- key_heads: bfloat16 [32768, 4, 64], P(('grp', 'sp'), 'tp'), parts along dimension 0, may hold values from -64 to 64
- value_heads: bfloat16 [32768, 4, 64], P(('grp', 'sp'), 'tp'), parts along dimension 0, may hold values from -6 to 6
- sink_logit: float32 [32], P('tp'), may hold values from 3 to 6
- out_weight: bfloat16 [2048, 2048], P('tp'), may hold values from -0.75 to 0.75
- residual: bfloat16 [32768, 2048], P(('grp', 'sp', 'tp')), parts along dimension 0, may hold values from -6 to 6
- norm_gain: float32 [2048], replicated, may hold values from 0.1 to 1.9
- expert_ids: int32 [32768, 2], P(('grp', 'sp', 'tp')), parts along dimension 0, may hold values from 0 to 127, all different within a row; in each aligned block of 128 rows (0 to 127, 128 to 255, ...) at most 4 rows name the same one
- route_weights: float32 [32768, 2], P(('grp', 'sp', 'tp')), parts along dimension 0, may hold values from 0.1 to 1
- gate_weight: bfloat16 [128, 2048, 512], P(('sp', 'tp')), may hold values from -0.125 to 0.125
- up_weight: bfloat16 [128, 2048, 512], P(('sp', 'tp')), may hold values from -0.125 to 0.125
- down_weight: bfloat16 [128, 512, 2048], P(('sp', 'tp')), may hold values from -0.5 to 0.5
Outputs:
- mixed: bfloat16 [32768, 2048], P(('grp', 'sp', 'tp')), parts along dimension 0
The draws below stay inside these ranges and needn't reach their ends.
There are 2 independent parts, one for each index of `grp`. The reference program is written for one: setup_inputs(seed, part) draws one part's arguments, and reference() takes and returns one part's arrays. A program takes and returns all parts, laid end to end along the dimension named above; an argument that names none is the same for every part. Nothing has to cross between parts.
Inputs may be any that keep to these rules, and one draw needn't show every extreme that they name: `expert_ids`: each row names 2 different experts. In the rows of one device (aligned blocks of 128 rows) no expert is named more than 4 times, and in some blocks one expert is named exactly 4 times.
All inputs are finite; a program needn't handle non-finite values.
Results may differ from the reference program's by a relative error of at most 0.014.
Values may be sent and summed in bfloat16 or wider, within the bound.
A program may use at most 64 MiB of HBM per device.

```python
import math
import jax
import jax.numpy as jnp
import numpy as np
from jax import lax

D = 2048
QH = 32
KVH = 4
HEAD_SIZE = 64
WINDOW = 128
FF = 512
TOP_K = 2
TOK_DEV = 128
TOKENS = 16384
EXPERTS = 128
CAP = 4


def draw_queries(key, part):
    drawn = jnp.clip(jax.random.normal(jax.random.fold_in(key, 5), (TOKENS, QH * HEAD_SIZE), jnp.float32), -6.0, 6.0)
    return drawn.astype(jnp.bfloat16)


def draw_key_heads(key, part):
    drawn = jnp.clip(jax.random.normal(jax.random.fold_in(key, 6), (TOKENS, KVH, HEAD_SIZE), jnp.float32), -6.0, 6.0)
    return drawn.astype(jnp.bfloat16)


def steps_of(own_key, dims, pieces, least, largest):
    level, own = 1.0, jax.random.fold_in(own_key, 6)
    for position, parts in pieces:
        steps = jnp.exp(jax.random.uniform(jax.random.fold_in(own, position), (parts,), jnp.float32, least / len(pieces), largest / len(pieces)))
        level = level * jnp.repeat(steps, dims[position] // parts).reshape([-1 if axis == position else 1 for axis in range(len(dims))])
    return level


def assign_block(own_key, own, number, rows, amount, top, limit, lean):
    ranking = jax.random.permutation(own_key, amount)
    crowded, ordinary = portions_of(amount, rows * top, limit, lean, True), portions_of(amount, rows * top, limit, lean, False)
    places = jnp.arange(amount)

    def named(sizes, turn):
        used = int((sizes > 0).sum())
        fixed = max(1, used // 4)
        shifted = fixed + (places - fixed + turn * (used - fixed)) % max(1, amount - fixed)
        return jnp.zeros((amount,), jnp.int32).at[ranking[jnp.where(places < fixed, places, shifted)]].set(jnp.asarray(sizes, jnp.int32))

    sizes = jnp.where(number % 4 == 0, named(crowded, number // 4), named(ordinary, number - number // 4 - 1))
    mixed = jax.random.permutation(jax.random.fold_in(own, 3), amount)
    giver, receiver = mixed[0:amount // 2 * 2:2], mixed[1:amount // 2 * 2:2]
    room = jnp.minimum(sizes[giver] - 1, limit - sizes[receiver]) // 2
    room = jnp.where((giver == ranking[0]) | (receiver == ranking[0]) | (sizes[receiver] == 0), 0, jnp.maximum(room, 0))
    shifted = jax.random.randint(jax.random.fold_in(own, 4), (amount // 2,), 0, 1 << 20) % (room + 1)
    sizes = sizes.at[giver].add(-shifted).at[receiver].add(shifted)
    members = jnp.searchsorted(jnp.cumsum(sizes), jnp.arange(rows * top), side="right").astype(jnp.int32)
    table = members.reshape(top, rows).T
    table = table[jax.random.permutation(jax.random.fold_in(own, 1), rows)]
    turn = jax.random.randint(jax.random.fold_in(own, 2), (rows, 1), 0, top)
    return jnp.take_along_axis(table, (jnp.arange(top)[None, :] + turn) % top, axis=1)


def portions_of(amount, total, limit, skew, full):
    loads = [(1 << 20) // math.isqrt(grade ** skew) + 1 for grade in range(1, amount + 1)]
    largest = limit if full else min(limit, max(-(-total // amount), total * loads[0] // sum(loads)))
    least = 1 if total - largest >= amount - 1 else 0
    holding, rest = [largest] + [least] * (amount - 1), total - largest - least * (amount - 1)
    while rest > 0:
        free = [i for i in range(1, amount) if holding[i] < largest] or [i for i in range(1, amount) if holding[i] < limit]
        whole, left = sum([loads[i] for i in free]), rest
        for i in free:
            extra = min(limit - holding[i], max(1, left * loads[i] // whole), rest)
            holding[i] = holding[i] + extra
            rest = rest - extra
    return np.array(holding)


def normal_values(rng, dims, deviation, limit, pieces=(), kind=jnp.bfloat16):
    gain = steps_of(rng, dims, pieces, -0.22, 0.18) if pieces else 1.0
    result = jax.random.normal(rng, dims, jnp.float32) * deviation * gain
    return jnp.minimum(jnp.maximum(result, -limit), limit).astype(kind)


def setup_inputs(seed: int = 0, part: int = 0) -> dict:
    key_list = jax.random.split(jax.random.key(seed), 13)
    own_keys = jax.random.split(jax.random.fold_in(key_list[12], part), 13)
    queries = draw_queries(jax.random.fold_in(jax.random.fold_in(key_list[12], part), 71), part)
    key_heads = draw_key_heads(jax.random.fold_in(jax.random.fold_in(key_list[12], part), 71), part)
    value_heads = normal_values(own_keys[2], (TOKENS, KVH, HEAD_SIZE), 1.0, 6.0, ((0, 32), (1, 4)))
    sink_logit = jnp.clip(3.0 + 3.0 * jax.random.uniform(key_list[3], (QH,), jnp.float32) ** steps_of(key_list[3], (QH,), ((0, 4),), -0.2, 0.2), 3.0, 6.0)
    out_weight = normal_values(key_list[4], (QH * HEAD_SIZE, D), (QH * HEAD_SIZE // 32) ** -0.5, 0.75, ((0, 4),))
    residual = normal_values(own_keys[5], (TOKENS, D), 1.0, 6.0, ((0, 128),))
    norm_gain = jnp.clip(1.0 + 0.18 * jax.random.normal(key_list[6], (D,), jnp.float32), 0.1, 1.9)
    expert_ids_keys = jax.random.split(jax.random.fold_in(own_keys[7], 1), TOKENS // TOK_DEV)
    expert_ids_turns = jax.random.permutation(jax.random.fold_in(own_keys[7], 3), TOKENS // TOK_DEV)
    expert_ids = jax.vmap(lambda own, number: assign_block(jax.random.fold_in(own_keys[7], 2), own, number, TOK_DEV, EXPERTS, TOP_K, CAP, 1))(expert_ids_keys, expert_ids_turns).reshape((TOKENS, TOP_K))
    route_weights = jnp.clip(jnp.exp(math.log(1.0) - 2.3025851 * jax.random.uniform(own_keys[8], (TOKENS, TOP_K), jnp.float32) ** steps_of(own_keys[8], (TOKENS, TOP_K), ((0, 128),), -0.2, 0.2)), 0.1, 1.0)
    gate_weight = normal_values(key_list[9], (EXPERTS, D, FF), D ** -0.5, 0.125, ((0, 128),))
    up_weight = normal_values(key_list[10], (EXPERTS, D, FF), D ** -0.5, 0.125, ((0, 128),))
    down_weight = normal_values(key_list[11], (EXPERTS, FF, D), (FF // 4) ** -0.5, 0.5, ((0, 128),))
    return dict(queries=queries, key_heads=key_heads, value_heads=value_heads, sink_logit=sink_logit, out_weight=out_weight, residual=residual, norm_gain=norm_gain, expert_ids=expert_ids, route_weights=route_weights, gate_weight=gate_weight, up_weight=up_weight, down_weight=down_weight)


EPS = 1e-06

def attention(queries, key_heads, value_heads, sink_logit):
    group_size = QH // KVH
    count_of_blocks = TOKENS // WINDOW
    query_blocks = queries.reshape(count_of_blocks, WINDOW, KVH, group_size, HEAD_SIZE)
    key_blocks = key_heads.reshape(count_of_blocks, WINDOW, KVH, HEAD_SIZE)
    value_blocks = value_heads.reshape(count_of_blocks, WINDOW, KVH, HEAD_SIZE)
    blank = jnp.zeros((1, WINDOW, KVH, HEAD_SIZE), key_heads.dtype)
    key_span = jnp.concatenate([jnp.concatenate([blank, key_blocks[:-1]], 0), key_blocks], 1)
    value_span = jnp.concatenate([jnp.concatenate([blank, value_blocks[:-1]], 0), value_blocks], 1)
    query_pos = jnp.arange(WINDOW, dtype=jnp.int32)[:, None]
    key_pos = jnp.arange(2 * WINDOW, dtype=jnp.int32)[None, :]
    distance = query_pos + WINDOW - key_pos
    band = (distance >= 0) & (distance < WINDOW)
    key_start = jnp.arange(count_of_blocks, dtype=jnp.int32)[:, None] * WINDOW - WINDOW + key_pos
    allowed = band[None, :, :] & (key_start >= 0)[:, None, :]
    sinks = sink_logit.reshape(KVH, group_size)

    def one_head(packed):
        query_per_head, key_per_head, value_per_head, head_sink = packed
        logit_scores = jnp.einsum('szue,sje->suzj', query_per_head.astype(jnp.float32), key_per_head.astype(jnp.float32)) * HEAD_SIZE ** (-0.5)
        logit_scores = jnp.where(allowed[:, None], logit_scores, -jnp.inf)
        sink_col = head_sink[None, :, None, None]
        row_max = jnp.maximum(lax.optimization_barrier(jnp.max(logit_scores, axis=-1, keepdims=True)), sink_col)
        expd = jnp.exp(logit_scores - row_max)
        row_total = lax.optimization_barrier(jnp.sum(expd, axis=-1, keepdims=True)) + jnp.exp(sink_col - row_max)
        attention_probabilities = (expd / row_total).astype(jnp.bfloat16)
        return jnp.einsum('vjwu,vuo->vwjo', attention_probabilities.astype(jnp.float32), value_per_head.astype(jnp.float32)).astype(jnp.bfloat16)
    outputs = lax.map(one_head, (jnp.moveaxis(query_blocks, 2, 0), jnp.moveaxis(key_span, 2, 0), jnp.moveaxis(value_span, 2, 0), sinks))
    return jnp.moveaxis(outputs, 0, 2).reshape(TOKENS, QH * HEAD_SIZE)

def reference(queries, key_heads, value_heads, sink_logit, out_weight, residual, norm_gain, expert_ids, route_weights, gate_weight, up_weight, down_weight):
    attended = attention(queries, key_heads, value_heads, sink_logit)
    projected = jnp.dot(attended, out_weight, preferred_element_type=jnp.float32)
    stream = (residual.astype(jnp.float32) + projected).astype(jnp.bfloat16)
    wide = stream.astype(jnp.float32)
    normed = (wide * lax.rsqrt(lax.optimization_barrier(jnp.mean(wide * wide, axis=-1, keepdims=True)) + EPS) * norm_gain).astype(jnp.bfloat16)
    device_count = TOKENS // TOK_DEV
    pairs = TOK_DEV * TOP_K
    flat_ids = expert_ids.reshape(device_count, pairs)
    onehot = (flat_ids[:, :, None] == jnp.arange(EXPERTS, dtype=jnp.int32)[None, None, :]).astype(jnp.int32)
    earlier = jnp.cumsum(onehot, axis=1) - onehot
    slot_rank = lax.optimization_barrier(jnp.sum(earlier * onehot, axis=-1))
    flat_slot = (flat_ids * CAP + slot_rank).astype(jnp.int32)
    device_row = jnp.arange(device_count, dtype=jnp.int32)[:, None]
    owner_row = device_row * TOK_DEV + (jnp.arange(pairs, dtype=jnp.int32) // TOP_K)[None, :]
    shares = route_weights / lax.optimization_barrier(jnp.sum(route_weights, axis=-1, keepdims=True))
    token_in_slot = jnp.zeros((device_count, EXPERTS * CAP), jnp.int32).at[device_row, flat_slot].set(owner_row)
    slot_share = jnp.zeros((device_count, EXPERTS * CAP), jnp.float32).at[device_row, flat_slot].set(shares.reshape(device_count, pairs))

    def expert_step(summed, packed):
        w_gate_e, w_up_e, w_down_e, expert = packed
        row_index = lax.dynamic_slice_in_dim(token_in_slot, expert * CAP, CAP, 1).reshape(-1)
        row_share = lax.dynamic_slice_in_dim(slot_share, expert * CAP, CAP, 1).reshape(-1)
        rows = normed[row_index]
        gate = jnp.dot(rows, w_gate_e, preferred_element_type=jnp.float32)
        upward = jnp.dot(rows, w_up_e, preferred_element_type=jnp.float32)
        expert_hidden = (jax.nn.silu(gate) * upward).astype(jnp.bfloat16)
        expert_rows = jnp.dot(expert_hidden, w_down_e, preferred_element_type=jnp.float32).astype(jnp.bfloat16)
        summed = summed.at[row_index].add(row_share[:, None] * expert_rows.astype(jnp.float32))
        return (summed, None)
    start = jnp.zeros((TOKENS, D), jnp.float32)
    summed, _ = lax.scan(expert_step, start, (gate_weight, up_weight, down_weight, jnp.arange(EXPERTS, dtype=jnp.int32)))
    return (stream.astype(jnp.float32) + summed).astype(jnp.bfloat16)
```

```python
import functools

import jax
import jax.numpy as jnp
from jax import lax
from jax.experimental import pallas as pl
from jax.experimental.pallas import tpu as pltpu
from jax.sharding import PartitionSpec as P

MESH = pl.DeviceIdType.MESH
BF = jnp.bfloat16
F32 = jnp.float32
CORES = 2
WINDOW = 128
EPS = 1e-06


def mm(a, b):
    return jnp.dot(a, b, preferred_element_type=F32)


def mm_nt(a, b):
    return lax.dot_general(a, b, (((1,), (1,)), ((), ())), preferred_element_type=F32)


def mm_tn(a, b):
    return lax.dot_general(a, b, (((0,), (0,)), ((), ())), preferred_element_type=F32)


def iota(shape, dim):
    return lax.broadcasted_iota(jnp.int32, shape, dim)


def layer(
    dims,
    q_hbm,
    kt_hbm,
    vt_hbm,
    sink_ref,
    wo_hbm,
    res_ref,
    gain_ref,
    ids_ref,
    rw_ref,
    wg_hbm,
    wu_hbm,
    wd_hbm,
    out_ref,
    qv,
    kv,
    wo,
    wg,
    wu,
    wd,
    att,
    s2,
    r2,
    sp,
    sm,
    rp,
    rm,
    acc,
    stream,
    normed,
    own_a,
    ring,
    meta,
    table,
    place,
    sel,
    xin,
    yout,
    zin,
    ret,
    cbuf,
    load_sem,
    halo_sem,
    rs_send,
    rs_recv,
    d_send,
    d_recv,
    m_send,
    m_recv,
    p_send,
    p_recv,
    y_send,
    y_recv,
    b_send,
    b_recv,
):
    T, D, Z, TP, SP, CAP, HEADS, HD = dims
    PL = TP * CORES
    CH = PL * CAP
    HALF = D // 2
    HOPS = (Z // 2, Z // 2 - 1)
    PAIRS = Z // 4
    GR = 4 * CAP

    s = lax.axis_index("sp")
    x = lax.axis_index("tp")
    z = lax.div(s, CORES)
    c = lax.rem(s, CORES)
    me = c * TP + x
    step_a = 1 - 2 * c + Z
    z_next = (lax.rem(z + step_a, Z), lax.rem(z + 2 * Z - step_a, Z))

    def chip(zz):
        return {"sp": zz * CORES + c, "tp": x}

    ahead = (chip(z_next[0]), chip(z_next[1]))
    behind = (ahead[1], ahead[0])

    def to_x(k):
        return {"sp": s, "tp": lax.rem(x + k + TP, TP)}

    def peer(k):
        cc = lax.rem(c + k // TP, CORES)
        return {"sp": z * CORES + cc, "tp": lax.rem(x + k % TP, TP)}

    def peer_rank(k):
        return lax.rem(c + k // TP, CORES) * TP + lax.rem(x + k % TP, TP)

    def from_rank(k):
        return lax.rem(c + CORES - k // TP, CORES) * TP + lax.rem(x + TP - k % TP, TP)

    s_after = {"sp": lax.rem(s + 1, SP), "tp": x}
    s_before = {"sp": lax.rem(s + SP - 1, SP), "tp": x}

    loads = [
        pltpu.make_async_copy(q_hbm, qv, load_sem.at[0]),
        pltpu.make_async_copy(wo_hbm, wo, load_sem.at[1]),
        pltpu.make_async_copy(wg_hbm.at[0], wg, load_sem.at[2]),
        pltpu.make_async_copy(wu_hbm.at[0], wu, load_sem.at[3]),
        pltpu.make_async_copy(wd_hbm.at[0], wd, load_sem.at[4]),
    ]
    kv_loads = []
    for b in range(TP):
        cols = pl.ds(b * T, T)
        kv_loads.append(
            pltpu.make_async_copy(kt_hbm.at[:, cols], kv.at[b + 1, pl.ds(0, HD)], load_sem.at[5 + b])
        )
        kv_loads.append(
            pltpu.make_async_copy(
                vt_hbm.at[:, cols], kv.at[b + 1, pl.ds(HD, HD)], load_sem.at[5 + TP + b]
            )
        )
    for copy in kv_loads[::-1]:
        copy.start()
    loads[0].start()
    loads[1].start()

    barrier = pltpu.get_barrier_semaphore()
    greeted = [ahead[0], ahead[1], s_after, s_before] + [peer(k) for k in range(1, PL)]
    for device in greeted:
        pl.semaphore_signal(barrier, inc=1, device_id=device, device_id_type=MESH)
    for copy in kv_loads:
        copy.wait()
    pl.semaphore_wait(barrier, len(greeted))

    halo = pltpu.make_async_remote_copy(
        src_ref=kv.at[TP],
        dst_ref=kv.at[0],
        send_sem=halo_sem.at[0],
        recv_sem=halo_sem.at[1],
        device_id=s_after,
        device_id_type=MESH,
    )
    halo.start()
    for copy in loads[2:]:
        copy.start()

    row_i = iota((T, 2 * T), 0)
    col_j = iota((T, 2 * T), 1)

    def attend(b, slot):
        first = jnp.where(s * TP + b == 0, T, 0)
        allowed = (col_j > row_i) & (col_j <= row_i + T) & (col_j >= first)
        rows = pl.ds(pl.multiple_of(b * T, T), T)
        low = kv[b].astype(F32)
        high = kv[b + 1].astype(F32)
        both = jnp.concatenate([low, high], axis=1)
        kt, vt = both[:HD], both[HD:]
        none = jnp.zeros((HD, 2 * T), F32)
        keys = (jnp.concatenate([kt, none], 0).astype(BF), jnp.concatenate([none, kt], 0).astype(BF))
        values = (jnp.concatenate([vt, none], 0).astype(BF), jnp.concatenate([none, vt], 0).astype(BF))
        for pair in range(HEADS // 2):
            lanes = pl.ds(pair * 2 * HD, 2 * HD)
            query = qv[rows, lanes]
            total = None
            for side in range(2):
                sink = sink_ref[pair * 2 + side]
                score = mm(query, keys[side]) * (HD ** (-0.5))
                score = jnp.where(allowed, score, -jnp.inf)
                top = jnp.maximum(jnp.max(score, axis=1, keepdims=True), sink)
                grown = jnp.exp(score - top)
                weight = jnp.sum(grown, axis=1, keepdims=True) + jnp.exp(sink - top)
                mixed = mm_nt(grown.astype(BF), values[side]) / weight
                total = mixed if total is None else total + mixed
            att[slot, :, lanes] = total.astype(BF)

    def rs_copy(src, dst, index, device):
        return pltpu.make_async_remote_copy(
            src_ref=src,
            dst_ref=dst,
            send_sem=rs_send.at[index],
            recv_sem=rs_recv.at[index],
            device_id=device,
            device_id_type=MESH,
        )

    def project(slot, half):
        return mm(att[slot], wo[:, pl.ds(half * HALF, HALF)])

    right, left = to_x(1), to_x(-1)
    loads[0].wait()
    halo.wait()
    attend(lax.rem(x + 2, TP), 0)
    loads[1].wait()
    copies = []
    for half, device in ((0, right), (1, left)):
        s2[half] = project(0, half).astype(BF)
        copy = rs_copy(s2.at[half], r2.at[half], half, device)
        copy.start()
        copies.append(copy)
    attend(lax.rem(x + 1, TP), 1)
    sp[1] = project(1, 1).astype(BF)
    send_p1 = rs_copy(sp.at[1], rp.at[1], 2, right)
    send_p1.start()
    attend(lax.rem(x + TP - 1, TP), 2)
    sm[0] = project(2, 0).astype(BF)
    send_m0 = rs_copy(sm.at[0], rm.at[0], 3, left)
    send_m0.start()
    copies[0].wait_recv()
    sp[0] = (project(1, 0) + r2[0].astype(F32)).astype(BF)
    send_p0 = rs_copy(sp.at[0], rp.at[0], 4, right)
    send_p0.start()
    copies[1].wait_recv()
    sm[1] = (project(2, 1) + r2[1].astype(F32)).astype(BF)
    send_m1 = rs_copy(sm.at[1], rm.at[1], 5, left)
    send_m1.start()
    attend(x, 3)
    for half in range(2):
        cols = pl.ds(half * HALF, HALF)
        acc[:, cols] = project(3, half) + res_ref[:, cols].astype(F32)

    E = Z * PL
    e_sub = iota((E, T), 0)
    t_lane = iota((E, T), 1)
    first_id = ids_ref[0:1, :]
    second_id = ids_ref[1:2, :]
    took0 = jnp.where(e_sub == first_id, 1.0, 0.0).astype(F32)
    took1 = jnp.where(e_sub == second_id, 1.0, 0.0).astype(F32)
    took = took0 + took1
    before = jnp.where(iota((T, T), 0) < iota((T, T), 1), 1.0, 0.0).astype(BF)
    rank = mm(took.astype(BF), before)
    weight_a = rw_ref[0:1, :]
    weight_b = rw_ref[1:2, :]
    whole = weight_a + weight_b
    share = took0 * (weight_a / whole) + took1 * (weight_b / whole)
    plane_bits = PL.bit_length() - 1
    e_plane = lax.shift_right_logical(e_sub, plane_bits)
    rel = (e_plane - z) * (1 - 2 * c) + 2 * Z
    rel = rel & (Z - 1)
    is_a = (rel >= 1) & (rel <= HOPS[0])
    dist = (
        jnp.where(is_a, rel, 0).astype(F32),
        jnp.where(rel > HOPS[0], Z - rel, 0).astype(F32),
    )
    t_sub = iota((T, T), 0)
    t_col = iota((T, T), 1)
    positions = []
    for way in range(2):
        far = jnp.max(took * dist[way], axis=0, keepdims=True)
        along = jnp.broadcast_to(far, (T, T))
        down = along.T
        ahead_of = (down > along) | ((down == along) & (t_sub < t_col))
        positions.append(jnp.sum(jnp.where(ahead_of, 1.0, 0.0), axis=0, keepdims=True))
    for way in range(2):
        place[way] = jnp.where(positions[way] == t_sub.astype(F32), 1.0, 0.0).astype(BF)
    slot_value = jnp.where(is_a, positions[0] + 1.0, positions[1] + (1.0 + T))
    hop_number = jnp.where(is_a, rel, jnp.where(rel > HOPS[0], Z - rel, HOPS[0]))
    base = (
        (e_sub & (PL - 1)) * GR
        + ((hop_number - 1) & 1) * (2 * CAP)
        + jnp.where(is_a, 0, CAP)
    )
    spread_t = jnp.zeros((E, T), F32)
    spread_w = jnp.zeros((E, T), F32)
    for r in range(CAP):
        here = took * jnp.where(rank == float(r), 1.0, 0.0)
        value_col = jnp.sum(here * slot_value, axis=1, keepdims=True)
        share_col = jnp.sum(here * share, axis=1, keepdims=True)
        hit = t_lane == base + r
        spread_t = spread_t + jnp.where(hit, value_col, 0.0)
        spread_w = spread_w + jnp.where(hit, share_col, 0.0)
    plane_of = jnp.where(
        lax.shift_right_logical(iota((Z, E), 1), plane_bits) == iota((Z, E), 0), 1.0, 0.0
    ).astype(BF)
    OWN = HOPS[0] - 1
    meta[OWN, 1, pl.ds(0, Z)] = mm(plane_of, spread_t.astype(BF)).astype(BF)
    meta[OWN, 1, pl.ds(Z, Z)] = mm(plane_of, spread_w.astype(BF)).astype(BF)

    def prefix(way, hop):
        return min(T, CH * (HOPS[way] - hop + 1)) if hop <= HOPS[way] else 0

    for way in range(2):
        for hop in range(1, HOPS[way] + 1):
            n = prefix(way, hop)
            if n < T:
                ring[hop - 1, way, pl.ds(n, T - n)] = jnp.zeros((T - n, D), BF)

    send_p1.wait_recv()
    send_p0.wait_recv()
    send_m0.wait_recv()
    send_m1.wait_recv()
    ROWS = 32
    for r in range(T // ROWS):
        rows = pl.ds(r * ROWS, ROWS)
        square = jnp.zeros((ROWS, 1), F32)
        for half in range(2):
            cols = pl.ds(half * HALF, HALF)
            total = acc[rows, cols] + rp[half, rows].astype(F32) + rm[half, rows].astype(F32)
            kept = total.astype(BF)
            stream[rows, cols] = kept
            wide = kept.astype(F32)
            square = square + jnp.sum(wide * wide, axis=1, keepdims=True)
        scale = lax.rsqrt(square * (1.0 / D) + EPS)
        for half in range(2):
            cols = pl.ds(half * HALF, HALF)
            wide = stream[rows, cols].astype(F32)
            normed[rows, cols] = (wide * scale * gain_ref[:, cols]).astype(BF)

    def d_index(way, hop, j):
        return (way * HOPS[0] + hop - 1) * (T // CH) + j

    def packet_copy(way, hop, j):
        rows = pl.ds(j * CH, CH)
        if hop == 1:
            src = own_a.at[rows] if way == 0 else ring.at[OWN, 1, rows]
        else:
            src = ring.at[hop - 2, way, rows]
        index = d_index(way, hop, j)
        return pltpu.make_async_remote_copy(
            src_ref=src,
            dst_ref=ring.at[hop - 1, way, rows],
            send_sem=d_send.at[index],
            recv_sem=d_recv.at[index],
            device_id=ahead[way],
            device_id_type=MESH,
        )

    def meta_copy(way, hop):
        src = meta.at[OWN, 1] if hop == 1 else meta.at[hop - 2, way]
        index = way * HOPS[0] + hop - 1
        return pltpu.make_async_remote_copy(
            src_ref=src,
            dst_ref=meta.at[hop - 1, way],
            send_sem=m_send.at[index],
            recv_sem=m_recv.at[index],
            device_id=ahead[way],
            device_id_type=MESH,
        )

    for way in range(2):
        meta_copy(way, 1).start()
    for j in range(T // CH):
        rows = pl.ds(j * CH, CH)
        own_a[rows] = mm(place[0, rows], normed[...]).astype(BF)
        ring[OWN, 1, rows] = mm(place[1, rows], normed[...]).astype(BF)
        for way in range(2):
            packet_copy(way, 1, j).start()

    def pair_table(p):
        picked_t = jnp.zeros((1, T), F32)
        picked_w = jnp.zeros((1, T), F32)
        sub = iota((Z, T), 0)
        lane = iota((1, T), 1)
        for side in range(2):
            hop = 2 * p + 1 + side
            for way in range(2):
                known = meta[hop - 1, way].astype(F32)
                mine = sub == z
                picked_t = picked_t + jnp.sum(jnp.where(mine, known[:Z], 0.0), axis=0, keepdims=True)
                picked_w = picked_w + jnp.sum(jnp.where(mine, known[Z:], 0.0), axis=0, keepdims=True)
        late = (lane & (2 * CAP)) != 0
        picked_t = picked_t + jnp.where(late & (picked_t > 0.0), 2.0 * T, 0.0)
        table[p, 0:1] = picked_t
        table[p, 1:2] = picked_w

    def chosen(p):
        return (iota((4 * T, T), 0) + 1).astype(F32) == table[p, 0:1]

    def plane_copy(buffer_from, buffer_to, sends, recvs, p, k):
        index = p * PL + k
        rank_to = pl.ds(pl.multiple_of(peer_rank(k) * GR, GR), GR)
        rank_me = pl.ds(pl.multiple_of(me * GR, GR), GR)
        return pltpu.make_async_remote_copy(
            src_ref=buffer_from.at[p, rank_to],
            dst_ref=buffer_to.at[p, rank_me],
            send_sem=sends.at[index],
            recv_sem=recvs.at[index],
            device_id=peer(k),
            device_id_type=MESH,
        )

    def plane_wait(buffer_from, buffer_to, sends, recvs, p, k):
        index = p * PL + k
        rank_from = pl.ds(pl.multiple_of(from_rank(k) * GR, GR), GR)
        pltpu.make_async_remote_copy(
            src_ref=buffer_from.at[p, rank_from],
            dst_ref=buffer_to.at[p, rank_from],
            send_sem=sends.at[index],
            recv_sem=recvs.at[index],
            device_id=peer(k),
            device_id_type=MESH,
        ).wait_recv()

    mine_rows = pl.ds(pl.multiple_of(me * GR, GR), GR)
    COLS = 512

    def select(p):
        pair_table(p)
        hot = jnp.where(chosen(p), 1.0, 0.0).astype(BF)
        for n in range(D // COLS):
            cols = pl.ds(n * COLS, COLS)
            rows = ring[pl.ds(2 * p, 2), :, :, cols].reshape(4 * T, COLS)
            sel[p, :, cols] = mm_tn(hot, rows).astype(BF)
        for k in range(1, PL):
            plane_copy(sel, xin, p_send, p_recv, p, k).start()
        xin[p, mine_rows] = sel[p, mine_rows]

    def experts(p):
        for k in range(1, PL):
            plane_wait(sel, xin, p_send, p_recv, p, k)
        rows = xin[p]
        gate = mm(rows, wg[...])
        upward = mm(rows, wu[...])
        hidden = (gate / (1.0 + jnp.exp(-gate)) * upward).astype(BF)
        for n in range(D // COLS):
            cols = pl.ds(n * COLS, COLS)
            yout[p, :, cols] = mm(hidden, wd[:, cols]).astype(BF)
        for k in range(1, PL):
            plane_copy(yout, zin, y_send, y_recv, p, k).start()
        zin[p, mine_rows] = yout[p, mine_rows]

    for copy in loads[2:]:
        copy.wait()
    for hop in range(1, HOPS[0] + 1):
        for way in range(2):
            if hop <= HOPS[way]:
                meta_copy(way, hop).wait_recv()
                if hop < HOPS[way]:
                    meta_copy(way, hop + 1).start()
        for j in range(T // CH):
            for way in range(2):
                if j * CH < prefix(way, hop):
                    packet_copy(way, hop, j).wait_recv()
                if j * CH < prefix(way, hop + 1):
                    packet_copy(way, hop + 1, j).start()
        if hop % 2 == 0:
            p = hop // 2 - 1
            select(p)
            if p > 0:
                experts(p - 1)
    experts(PAIRS - 1)

    def back_copy(way, hop, j):
        rows = pl.ds(j * CH, CH)
        index = d_index(way, hop, j)
        return pltpu.make_async_remote_copy(
            src_ref=ret.at[hop, way, rows],
            dst_ref=ret.at[hop - 1, way, rows],
            send_sem=b_send.at[index],
            recv_sem=b_recv.at[index],
            device_id=behind[way],
            device_id_type=MESH,
        )

    def weighted(hop, way, n):
        p, side = (hop - 1) // 2, (hop - 1) % 2
        at = (side * 2 + way) * T
        hit = (iota((n, T), 0) + (at + 1)).astype(F32) == table[p, 0:1]
        mix = jnp.where(hit, table[p, 1:2], 0.0).astype(BF)
        for half in range(2):
            cols = pl.ds(half * HALF, HALF)
            cbuf[way, pl.ds(0, n), cols] = mm(mix, zin[p, :, cols])

    for hop in range(HOPS[0], 0, -1):
        if hop % 2 == 0:
            p = hop // 2 - 1
            for k in range(1, PL):
                plane_wait(yout, zin, y_send, y_recv, p, k)
        if hop == HOPS[0]:
            weighted(hop, 1, T)
            acc[...] = cbuf[1]
        for way in range(2):
            if hop <= HOPS[way]:
                weighted(hop, way, prefix(way, hop))
        for j in range(T // CH):
            rows = pl.ds(j * CH, CH)
            for way in range(2):
                if j * CH >= prefix(way, hop):
                    continue
                part = cbuf[way, rows]
                if j * CH < prefix(way, hop + 1):
                    back_copy(way, hop + 1, j).wait_recv()
                    part = part + ret[hop, way, rows].astype(F32)
                ret[hop, way, rows] = part.astype(BF)
                back_copy(way, hop, j).start()

    for j in range(T // CH):
        rows = pl.ds(j * CH, CH)
        for way in range(2):
            back_copy(way, 1, j).wait_recv()
        ret[0, 1, rows] = (ret[0, 1, rows].astype(F32) + acc[rows]).astype(BF)
    unsort = place[...].reshape(2 * T, T)
    for n in range(D // COLS):
        cols = pl.ds(n * COLS, COLS)
        came = ret[0, :, :, cols].reshape(2 * T, COLS)
        out_ref[:, cols] = (stream[:, cols].astype(F32) + mm_tn(unsort, came)).astype(BF)

    for copy in copies + [send_p1, send_m0, send_p0, send_m1]:
        copy.wait_send()
    for way in range(2):
        for hop in range(1, HOPS[way] + 1):
            meta_copy(way, hop).wait_send()
            for j in range(T // CH):
                if j * CH < prefix(way, hop):
                    packet_copy(way, hop, j).wait_send()
                    back_copy(way, hop, j).wait_send()
    for p in range(PAIRS):
        for k in range(1, PL):
            plane_copy(sel, xin, p_send, p_recv, p, k).wait_send()
            plane_copy(yout, zin, y_send, y_recv, p, k).wait_send()


def solution(mesh):
    sp_count = mesh.shape["sp"]
    tp_count = mesh.shape["tp"]

    def on_device(
        queries,
        key_heads,
        value_heads,
        sink_logit,
        out_weight,
        residual,
        norm_gain,
        expert_ids,
        route_weights,
        gate_weight,
        up_weight,
        down_weight,
    ):
        T, D = residual.shape
        HD = key_heads.shape[2]
        HEADS = queries.shape[1] // HD
        FF = gate_weight.shape[2]
        Z = sp_count // CORES
        PL = tp_count * CORES
        top_k = expert_ids.shape[1]
        CAP = max(2, 2 * top_k * T // (sp_count * tp_count))
        PAIRS = Z // 4
        GR = 4 * CAP
        HOP = Z // 2
        keys_t = jnp.transpose(key_heads, (1, 2, 0)).reshape(HD, -1)
        values_t = jnp.transpose(value_heads, (1, 2, 0)).reshape(HD, -1)
        dma = pltpu.SemaphoreType.DMA
        vm = pltpu.VMEM
        any_space = pl.BlockSpec(memory_space=pl.ANY)
        in_vmem = pl.BlockSpec(memory_space=pltpu.VMEM)
        dims = (T, D, Z, tp_count, sp_count, CAP, HEADS, HD)
        chunks = T // (PL * CAP)
        return pl.pallas_call(
            functools.partial(layer, dims),
            out_shape=jax.ShapeDtypeStruct((T, D), BF),
            in_specs=[
                any_space,
                any_space,
                any_space,
                pl.BlockSpec(memory_space=pltpu.SMEM),
                any_space,
                in_vmem,
                in_vmem,
                in_vmem,
                in_vmem,
                any_space,
                any_space,
                any_space,
            ],
            out_specs=in_vmem,
            scratch_shapes=[
                vm(queries.shape, BF),
                vm((tp_count + 1, 2 * HD, T), BF),
                vm(out_weight.shape, BF),
                vm((D, FF), BF),
                vm((D, FF), BF),
                vm((FF, D), BF),
                vm((4, T, HEADS * HD), BF),
                vm((2, T, D // 2), BF),
                vm((2, T, D // 2), BF),
                vm((2, T, D // 2), BF),
                vm((2, T, D // 2), BF),
                vm((2, T, D // 2), BF),
                vm((2, T, D // 2), BF),
                vm((T, D), F32),
                vm((T, D), BF),
                vm((T, D), BF),
                vm((T, D), BF),
                vm((HOP, 2, T, D), BF),
                vm((HOP, 2, 2 * Z, T), BF),
                vm((PAIRS, 8, T), F32),
                vm((2, T, T), BF),
                vm((PAIRS, PL * GR, D), BF),
                vm((PAIRS, PL * GR, D), BF),
                vm((PAIRS, PL * GR, D), BF),
                vm((PAIRS, PL * GR, D), BF),
                vm((HOP + 1, 2, T, D), BF),
                vm((2, T, D), F32),
                dma((5 + 2 * tp_count,)),
                dma((2,)),
                dma((6,)),
                dma((6,)),
                dma((2 * HOP * chunks,)),
                dma((2 * HOP * chunks,)),
                dma((2 * HOP,)),
                dma((2 * HOP,)),
                dma((PAIRS * PL,)),
                dma((PAIRS * PL,)),
                dma((PAIRS * PL,)),
                dma((PAIRS * PL,)),
                dma((2 * HOP * chunks,)),
                dma((2 * HOP * chunks,)),
            ],
            compiler_params=pltpu.CompilerParams(
                collective_id=0, has_side_effects=True, vmem_limit_bytes=62 * 1024 * 1024
            ),
        )(
            queries,
            keys_t,
            values_t,
            sink_logit,
            out_weight,
            residual,
            norm_gain.reshape(1, D),
            expert_ids.T,
            route_weights.T,
            gate_weight,
            up_weight,
            down_weight,
        )

    return jax.shard_map(
        on_device,
        mesh=mesh,
        in_specs=(
            P(("grp", "sp"), "tp"),
            P(("grp", "sp"), "tp", None),
            P(("grp", "sp"), "tp", None),
            P("tp"),
            P("tp", None),
            P(("grp", "sp", "tp"), None),
            P(),
            P(("grp", "sp", "tp"), None),
            P(("grp", "sp", "tp"), None),
            P(("sp", "tp"), None, None),
            P(("sp", "tp"), None, None),
            P(("sp", "tp"), None, None),
        ),
        out_specs=P(("grp", "sp", "tp"), None),
        check_vma=False,
    )
```

```python
import functools

import jax
import jax.numpy as jnp
from jax import lax
from jax.experimental import pallas as pl
from jax.experimental.pallas import tpu as pltpu
from jax.sharding import PartitionSpec as P

MESH = pl.DeviceIdType.MESH
BF = jnp.bfloat16
F32 = jnp.float32
CORES = 2
WINDOW = 128
EPS = 1e-06


def mm(a, b):
    return jnp.dot(a, b, preferred_element_type=F32)


def mm_nt(a, b):
    return lax.dot_general(a, b, (((1,), (1,)), ((), ())), preferred_element_type=F32)


def mm_tn(a, b):
    return lax.dot_general(a, b, (((0,), (0,)), ((), ())), preferred_element_type=F32)


def iota(shape, dim):
    return lax.broadcasted_iota(jnp.int32, shape, dim)


def layer(
    dims,
    q_hbm,
    kt_hbm,
    vt_hbm,
    sink_ref,
    wo_hbm,
    res_ref,
    gain_ref,
    ids_ref,
    rw_ref,
    wg_hbm,
    wu_hbm,
    wd_hbm,
    out_ref,
    qv,
    kv,
    wo,
    wg,
    wu,
    wd,
    att,
    s2,
    r2,
    sp,
    sm,
    rp,
    rm,
    acc,
    stream,
    normed,
    own_a,
    ring,
    meta,
    table,
    place,
    sel,
    xin,
    yout,
    zin,
    ret,
    cbuf,
    load_sem,
    halo_sem,
    rs_send,
    rs_recv,
    d_send,
    d_recv,
    m_send,
    m_recv,
    p_send,
    p_recv,
    y_send,
    y_recv,
    b_send,
    b_recv,
):
    T, D, Z, TP, SP, CAP, HEADS, HD = dims
    LAST = Z // 2
    PL = TP * CORES
    CH = PL * CAP
    HALF = D // 2
    HOPS = (Z // 2, Z // 2 - 1)
    GR = 2 * CAP
    SEL = PL * GR

    s = lax.axis_index("sp")
    x = lax.axis_index("tp")
    z = lax.div(s, CORES)
    c = lax.rem(s, CORES)
    me = c * TP + x
    step_a = 1 - 2 * c + Z
    z_next = (lax.rem(z + step_a, Z), lax.rem(z + 2 * Z - step_a, Z))

    def chip(zz):
        return {"sp": zz * CORES + c, "tp": x}

    ahead = (chip(z_next[0]), chip(z_next[1]))
    behind = (ahead[1], ahead[0])

    def to_x(k):
        return {"sp": s, "tp": lax.rem(x + k + TP, TP)}

    def peer(k):
        cc = lax.rem(c + k // TP, CORES)
        return {"sp": z * CORES + cc, "tp": lax.rem(x + k % TP, TP)}

    def peer_rank(k):
        return lax.rem(c + k // TP, CORES) * TP + lax.rem(x + k % TP, TP)

    def from_rank(k):
        return lax.rem(c + CORES - k // TP, CORES) * TP + lax.rem(x + TP - k % TP, TP)

    s_after = {"sp": lax.rem(s + 1, SP), "tp": x}
    s_before = {"sp": lax.rem(s + SP - 1, SP), "tp": x}

    loads = [
        pltpu.make_async_copy(q_hbm, qv, load_sem.at[0]),
        pltpu.make_async_copy(wo_hbm, wo, load_sem.at[1]),
        pltpu.make_async_copy(wg_hbm.at[0], wg, load_sem.at[2]),
        pltpu.make_async_copy(wu_hbm.at[0], wu, load_sem.at[3]),
        pltpu.make_async_copy(wd_hbm.at[0], wd, load_sem.at[4]),
    ]
    kv_loads = []
    for b in range(TP):
        cols = pl.ds(b * T, T)
        kv_loads.append(
            pltpu.make_async_copy(kt_hbm.at[:, cols], kv.at[b + 1, pl.ds(0, HD)], load_sem.at[5 + b])
        )
        kv_loads.append(
            pltpu.make_async_copy(
                vt_hbm.at[:, cols], kv.at[b + 1, pl.ds(HD, HD)], load_sem.at[5 + TP + b]
            )
        )
    barrier = pltpu.get_barrier_semaphore()
    greeted = [ahead[0], ahead[1], s_after, s_before] + [peer(k) for k in range(1, PL)]
    for device in greeted:
        pl.semaphore_signal(barrier, inc=1, device_id=device, device_id_type=MESH)
    for copy in kv_loads[::-1]:
        copy.start()
    loads[0].start()
    loads[1].start()

    halo = pltpu.make_async_remote_copy(
        src_ref=kv.at[TP],
        dst_ref=kv.at[0],
        send_sem=halo_sem.at[0],
        recv_sem=halo_sem.at[1],
        device_id=s_after,
        device_id_type=MESH,
    )

    row_i = iota((T, 2 * T), 0)
    col_j = iota((T, 2 * T), 1)

    def attend(b, slot):
        first = jnp.where(s * TP + b == 0, T, 0)
        allowed = (col_j > row_i) & (col_j <= row_i + T) & (col_j >= first)
        rows = pl.ds(pl.multiple_of(b * T, T), T)
        low = kv[b].astype(F32)
        high = kv[b + 1].astype(F32)
        both = jnp.concatenate([low, high], axis=1)
        kt, vt = both[:HD], both[HD:]
        none = jnp.zeros((HD, 2 * T), F32)
        keys = (jnp.concatenate([kt, none], 0).astype(BF), jnp.concatenate([none, kt], 0).astype(BF))
        values = (jnp.concatenate([vt, none], 0).astype(BF), jnp.concatenate([none, vt], 0).astype(BF))
        for pair in range(HEADS // 2):
            lanes = pl.ds(pair * 2 * HD, 2 * HD)
            query = qv[rows, lanes]
            total = None
            for side in range(2):
                sink = sink_ref[pair * 2 + side]
                score = mm(query, keys[side]) * (HD ** (-0.5))
                score = jnp.where(allowed, score, -jnp.inf)
                top = jnp.maximum(jnp.max(score, axis=1, keepdims=True), sink)
                grown = jnp.exp(score - top)
                weight = jnp.sum(grown, axis=1, keepdims=True) + jnp.exp(sink - top)
                mixed = mm_nt(grown.astype(BF), values[side]) / weight
                total = mixed if total is None else total + mixed
            att[slot, :, lanes] = total.astype(BF)

    def rs_copy(src, dst, index, device):
        return pltpu.make_async_remote_copy(
            src_ref=src,
            dst_ref=dst,
            send_sem=rs_send.at[index],
            recv_sem=rs_recv.at[index],
            device_id=device,
            device_id_type=MESH,
        )

    def project(slot, half):
        return mm(att[slot], wo[:, pl.ds(half * HALF, HALF)])

    right, left = to_x(1), to_x(-1)
    for copy in kv_loads:
        copy.wait()
    loads[0].wait()
    attend(1, 1)
    pl.semaphore_wait(barrier, len(greeted))
    halo.start()
    for copy in loads[2:]:
        copy.start()
    for b in range(2, TP):
        attend(b, b)
    loads[1].wait()
    halo.wait()
    attend(0, 0)
    far, after, prior = lax.rem(x + 2, TP), lax.rem(x + 1, TP), lax.rem(x + TP - 1, TP)
    copies = []
    for half, device in ((0, right), (1, left)):
        s2[half] = project(far, half).astype(BF)
        copy = rs_copy(s2.at[half], r2.at[half], half, device)
        copy.start()
        copies.append(copy)
    sp[1] = project(after, 1).astype(BF)
    send_p1 = rs_copy(sp.at[1], rp.at[1], 2, right)
    send_p1.start()
    sm[0] = project(prior, 0).astype(BF)
    send_m0 = rs_copy(sm.at[0], rm.at[0], 3, left)
    send_m0.start()
    for half in range(2):
        cols = pl.ds(half * HALF, HALF)
        acc[:, cols] = project(x, half) + res_ref[:, cols].astype(F32)
    early = project(after, 0)
    copies[0].wait_recv()
    sp[0] = (early + r2[0].astype(F32)).astype(BF)
    send_p0 = rs_copy(sp.at[0], rp.at[0], 4, right)
    send_p0.start()
    early = project(prior, 1)
    copies[1].wait_recv()
    sm[1] = (early + r2[1].astype(F32)).astype(BF)
    send_m1 = rs_copy(sm.at[1], rm.at[1], 5, left)
    send_m1.start()

    E = Z * PL
    e_sub = iota((E, T), 0)
    t_lane = iota((E, T), 1)
    first_id = ids_ref[0:1, :]
    second_id = ids_ref[1:2, :]
    took0 = jnp.where(e_sub == first_id, 1.0, 0.0).astype(F32)
    took1 = jnp.where(e_sub == second_id, 1.0, 0.0).astype(F32)
    took = took0 + took1
    before = jnp.where(iota((T, T), 0) < iota((T, T), 1), 1.0, 0.0).astype(BF)
    rank = mm(took.astype(BF), before)
    weight_a = rw_ref[0:1, :]
    weight_b = rw_ref[1:2, :]
    whole = weight_a + weight_b
    share = took0 * (weight_a / whole) + took1 * (weight_b / whole)
    plane_bits = PL.bit_length() - 1
    e_plane = lax.shift_right_logical(e_sub, plane_bits)
    rel = (e_plane - z) * (1 - 2 * c) + 2 * Z
    rel = rel & (Z - 1)
    is_a = (rel >= 1) & (rel <= HOPS[0])
    dist = (
        jnp.where(is_a, rel, 0).astype(F32),
        jnp.where(rel > HOPS[0], Z - rel, 0).astype(F32),
    )
    t_sub = iota((T, T), 0)
    t_col = iota((T, T), 1)
    positions = []
    for way in range(2):
        far = jnp.max(took * dist[way], axis=0, keepdims=True)
        along = jnp.broadcast_to(far, (T, T))
        down = along.T
        ahead_of = (down > along) | ((down == along) & (t_sub < t_col))
        positions.append(jnp.sum(jnp.where(ahead_of, 1.0, 0.0), axis=0, keepdims=True))
    for way in range(2):
        place[way] = jnp.where(positions[way] == t_sub.astype(F32), 1.0, 0.0).astype(BF)
    slot_value = jnp.where(is_a, positions[0] + 1.0, positions[1] + (1.0 + T))
    base = (e_sub & (PL - 1)) * GR + jnp.where(is_a, 0, CAP)
    spread_t = jnp.zeros((E, T), F32)
    spread_w = jnp.zeros((E, T), F32)
    for r in range(CAP):
        here = took * jnp.where(rank == float(r), 1.0, 0.0)
        value_col = jnp.sum(here * slot_value, axis=1, keepdims=True)
        share_col = jnp.sum(here * share, axis=1, keepdims=True)
        hit = t_lane == base + r
        spread_t = spread_t + jnp.where(hit, value_col, 0.0)
        spread_w = spread_w + jnp.where(hit, share_col, 0.0)
    plane_of = jnp.where(
        lax.shift_right_logical(iota((Z, E), 1), plane_bits) == iota((Z, E), 0), 1.0, 0.0
    ).astype(BF)
    OWN = HOPS[0] - 1
    meta[OWN, 1, pl.ds(0, Z)] = mm(plane_of, spread_t.astype(BF)).astype(BF)
    meta[OWN, 1, pl.ds(Z, Z)] = mm(plane_of, spread_w.astype(BF)).astype(BF)

    def prefix(way, hop):
        return min(T, CH * (HOPS[way] - hop + 1)) if hop <= HOPS[way] else 0

    for way in range(2):
        for hop in range(1, HOPS[way] + 1):
            n = prefix(way, hop)
            if n < T:
                ring[hop - 1, way, pl.ds(n, T - n)] = jnp.zeros((T - n, D), BF)

    send_p1.wait_recv()
    send_p0.wait_recv()
    send_m0.wait_recv()
    send_m1.wait_recv()
    ROWS = 32
    for r in range(T // ROWS):
        rows = pl.ds(r * ROWS, ROWS)
        square = jnp.zeros((ROWS, 1), F32)
        for half in range(2):
            cols = pl.ds(half * HALF, HALF)
            total = acc[rows, cols] + rp[half, rows].astype(F32) + rm[half, rows].astype(F32)
            kept = total.astype(BF)
            stream[rows, cols] = kept
            wide = kept.astype(F32)
            square = square + jnp.sum(wide * wide, axis=1, keepdims=True)
        scale = lax.rsqrt(square * (1.0 / D) + EPS)
        for half in range(2):
            cols = pl.ds(half * HALF, HALF)
            wide = stream[rows, cols].astype(F32)
            normed[rows, cols] = (wide * scale * gain_ref[:, cols]).astype(BF)

    def d_index(way, hop, j):
        return (way * HOPS[0] + hop - 1) * (T // CH) + j

    def packet_copy(way, hop, j):
        rows = pl.ds(j * CH, CH)
        if hop == 1:
            src = own_a.at[rows] if way == 0 else ring.at[OWN, 1, rows]
        else:
            src = ring.at[hop - 2, way, rows]
        index = d_index(way, hop, j)
        return pltpu.make_async_remote_copy(
            src_ref=src,
            dst_ref=ring.at[hop - 1, way, rows],
            send_sem=d_send.at[index],
            recv_sem=d_recv.at[index],
            device_id=ahead[way],
            device_id_type=MESH,
        )

    def meta_copy(way, hop):
        src = meta.at[OWN, 1] if hop == 1 else meta.at[hop - 2, way]
        index = way * HOPS[0] + hop - 1
        return pltpu.make_async_remote_copy(
            src_ref=src,
            dst_ref=meta.at[hop - 1, way],
            send_sem=m_send.at[index],
            recv_sem=m_recv.at[index],
            device_id=ahead[way],
            device_id_type=MESH,
        )

    for way in range(2):
        meta_copy(way, 1).start()
    for j in range(T // CH):
        rows = pl.ds(j * CH, CH)
        own_a[rows] = mm(place[0, rows], normed[...]).astype(BF)
        ring[OWN, 1, rows] = mm(place[1, rows], normed[...]).astype(BF)
        if j < 2:
            for way in range(2):
                packet_copy(way, 1, j).start()

    def hop_table(hop):
        picked_t = jnp.zeros((1, T), F32)
        picked_w = jnp.zeros((1, T), F32)
        mine = iota((Z, T), 0) == z
        for way in range(2):
            known = meta[hop - 1, way].astype(F32)
            picked_t = picked_t + jnp.sum(jnp.where(mine, known[:Z], 0.0), axis=0, keepdims=True)
            picked_w = picked_w + jnp.sum(jnp.where(mine, known[Z:], 0.0), axis=0, keepdims=True)
        table[hop - 1, 0:1] = picked_t
        table[hop - 1, 1:2] = picked_w

    def plane_copy(buffer_from, buffer_to, sends, recvs, hop, k):
        index = (hop - 1) * PL + k
        return pltpu.make_async_remote_copy(
            src_ref=buffer_from.at[hop - 1, peer_rank(k)],
            dst_ref=buffer_to.at[hop - 1, me],
            send_sem=sends.at[index],
            recv_sem=recvs.at[index],
            device_id=peer(k),
            device_id_type=MESH,
        )

    def plane_wait(buffer_from, buffer_to, sends, recvs, hop, k):
        index = (hop - 1) * PL + k
        pltpu.make_async_remote_copy(
            src_ref=buffer_from.at[hop - 1, from_rank(k)],
            dst_ref=buffer_to.at[hop - 1, from_rank(k)],
            send_sem=sends.at[index],
            recv_sem=recvs.at[index],
            device_id=peer(k),
            device_id_type=MESH,
        ).wait_recv()

    COLS = 512

    def select(hop):
        hop_table(hop)
        spot = (iota((2 * T, SEL), 0) + 1).astype(F32)
        hot = jnp.where(spot == table[hop - 1, 0:1, 0:SEL], 1.0, 0.0).astype(BF)
        for n in range(D // COLS):
            cols = pl.ds(n * COLS, COLS)
            rows = ring[hop - 1, :, :, cols].reshape(2 * T, COLS)
            sel[hop - 1, :, :, cols] = mm_tn(hot, rows).reshape(PL, GR, COLS).astype(BF)
        for k in range(1, PL):
            plane_copy(sel, xin, p_send, p_recv, hop, k).start()
        xin[hop - 1, me] = sel[hop - 1, me]

    def experts(*hops):
        for hop in hops:
            for k in range(1, PL):
                plane_wait(sel, xin, p_send, p_recv, hop, k)
        rows = jnp.concatenate(
            [xin[hop - 1].astype(F32).reshape(SEL, D).astype(BF) for hop in hops], axis=0
        )
        gate = mm(rows, wg[...])
        upward = mm(rows, wu[...])
        hidden = (gate / (1.0 + jnp.exp(-gate)) * upward).astype(BF)
        for n in range(D // COLS):
            cols = pl.ds(n * COLS, COLS)
            product = mm(hidden, wd[:, cols])
            for i, hop in enumerate(hops):
                part = product[i * SEL : (i + 1) * SEL]
                yout[hop - 1, :, :, cols] = part.reshape(PL, GR, COLS).astype(BF)
        for hop in hops:
            for k in range(1, PL):
                plane_copy(yout, zin, y_send, y_recv, hop, k).start()
            zin[hop - 1, me] = yout[hop - 1, me]

    def back_copy(way, hop, j):
        rows = pl.ds(j * CH, CH)
        index = d_index(way, hop, j)
        return pltpu.make_async_remote_copy(
            src_ref=ret.at[hop, way, rows],
            dst_ref=ret.at[hop - 1, way, rows],
            send_sem=b_send.at[index],
            recv_sem=b_recv.at[index],
            device_id=behind[way],
            device_id_type=MESH,
        )

    def weighted(hop, ways):
        for k in range(1, PL):
            plane_wait(yout, zin, y_send, y_recv, hop, k)
        mixes = []
        for way, n in ways:
            spot = (iota((n, SEL), 0) + (way * T + 1)).astype(F32)
            hit = spot == table[hop - 1, 0:1, 0:SEL]
            mixes.append(jnp.where(hit, table[hop - 1, 1:2, 0:SEL], 0.0).astype(BF))
        for n in range(D // COLS):
            cols = pl.ds(n * COLS, COLS)
            rows = zin[hop - 1, :, :, cols].astype(F32).reshape(SEL, COLS).astype(BF)
            for (way, count), mix in zip(ways, mixes):
                cbuf[way, pl.ds(0, count), cols] = mm(mix, rows)

    def send_back(hop):
        if hop == LAST:
            weighted(hop, [(0, prefix(0, hop)), (1, T)])
            acc[...] = cbuf[1]
        else:
            weighted(hop, [(way, prefix(way, hop)) for way in range(2)])
        for i in range(T // CH):
            for way in range(2):
                j = prefix(way, hop) // CH - 1 - i
                if j < 0:
                    continue
                rows = pl.ds(j * CH, CH)
                part = cbuf[way, rows]
                if j * CH < prefix(way, hop + 1):
                    back_copy(way, hop + 1, j).wait_recv()
                    part = part + ret[hop, way, rows].astype(F32)
                ret[hop, way, rows] = part.astype(BF)
                back_copy(way, hop, j).start()

    def pass_on(way, hop, j):
        if j * CH < prefix(way, hop):
            packet_copy(way, hop, j).wait_recv()
        if j * CH < prefix(way, hop + 1):
            packet_copy(way, hop + 1, j).start()

    for copy in loads[2:]:
        copy.wait()
    for hop in range(1, LAST + 1):
        for way in range(2):
            if hop <= HOPS[way]:
                meta_copy(way, hop).wait_recv()
                if hop < HOPS[way]:
                    meta_copy(way, hop + 1).start()
        for j in range(2):
            for way in range(2):
                pass_on(way, hop, j)
                if hop == HOPS[way] - 1:
                    packet_copy(way, 1, 2 + j).start()
    select(LAST)
    select(LAST - 1)
    for hop in range(1, LAST - 1):
        for j in range(2, 4):
            for way in range(2):
                pass_on(way, hop, j)
        select(hop)
        if hop == 2:
            experts(LAST, LAST - 1)
        if hop == LAST - 3:
            send_back(LAST)
    send_back(LAST - 1)
    experts(LAST - 2, LAST - 3)
    experts(1, 2)
    experts(3, 4)
    for hop in range(LAST - 2, 0, -1):
        send_back(hop)

    for j in range(T // CH):
        rows = pl.ds(j * CH, CH)
        for way in range(2):
            back_copy(way, 1, j).wait_recv()
        ret[0, 1, rows] = (ret[0, 1, rows].astype(F32) + acc[rows]).astype(BF)
    unsort = place[...].reshape(2 * T, T)
    for n in range(D // COLS):
        cols = pl.ds(n * COLS, COLS)
        came = ret[0, :, :, cols].reshape(2 * T, COLS)
        out_ref[:, cols] = (stream[:, cols].astype(F32) + mm_tn(unsort, came)).astype(BF)

    for copy in copies + [send_p1, send_m0, send_p0, send_m1]:
        copy.wait_send()
    for way in range(2):
        for hop in range(1, HOPS[way] + 1):
            meta_copy(way, hop).wait_send()
            for j in range(T // CH):
                if j * CH < prefix(way, hop):
                    packet_copy(way, hop, j).wait_send()
                    back_copy(way, hop, j).wait_send()
    for hop in range(1, LAST + 1):
        for k in range(1, PL):
            plane_copy(sel, xin, p_send, p_recv, hop, k).wait_send()
            plane_copy(yout, zin, y_send, y_recv, hop, k).wait_send()


def solution(mesh):
    sp_count = mesh.shape["sp"]
    tp_count = mesh.shape["tp"]

    def on_device(
        queries,
        key_heads,
        value_heads,
        sink_logit,
        out_weight,
        residual,
        norm_gain,
        expert_ids,
        route_weights,
        gate_weight,
        up_weight,
        down_weight,
    ):
        T, D = residual.shape
        HD = key_heads.shape[2]
        HEADS = queries.shape[1] // HD
        FF = gate_weight.shape[2]
        Z = sp_count // CORES
        PL = tp_count * CORES
        top_k = expert_ids.shape[1]
        CAP = max(2, 2 * top_k * T // (sp_count * tp_count))
        GR = 2 * CAP
        HOP = Z // 2
        keys_t = jnp.transpose(key_heads, (1, 2, 0)).reshape(HD, -1)
        values_t = jnp.transpose(value_heads, (1, 2, 0)).reshape(HD, -1)
        dma = pltpu.SemaphoreType.DMA
        vm = pltpu.VMEM
        any_space = pl.BlockSpec(memory_space=pl.ANY)
        in_vmem = pl.BlockSpec(memory_space=pltpu.VMEM)
        dims = (T, D, Z, tp_count, sp_count, CAP, HEADS, HD)
        chunks = T // (PL * CAP)
        return pl.pallas_call(
            functools.partial(layer, dims),
            out_shape=jax.ShapeDtypeStruct((T, D), BF),
            in_specs=[
                any_space,
                any_space,
                any_space,
                pl.BlockSpec(memory_space=pltpu.SMEM),
                any_space,
                in_vmem,
                in_vmem,
                in_vmem,
                in_vmem,
                any_space,
                any_space,
                any_space,
            ],
            out_specs=in_vmem,
            scratch_shapes=[
                vm(queries.shape, BF),
                vm((tp_count + 1, 2 * HD, T), BF),
                vm(out_weight.shape, BF),
                vm((D, FF), BF),
                vm((D, FF), BF),
                vm((FF, D), BF),
                vm((4, T, HEADS * HD), BF),
                vm((2, T, D // 2), BF),
                vm((2, T, D // 2), BF),
                vm((2, T, D // 2), BF),
                vm((2, T, D // 2), BF),
                vm((2, T, D // 2), BF),
                vm((2, T, D // 2), BF),
                vm((T, D), F32),
                vm((T, D), BF),
                vm((T, D), BF),
                vm((T, D), BF),
                vm((HOP, 2, T, D), BF),
                vm((HOP, 2, 2 * Z, T), BF),
                vm((HOP, 8, T), F32),
                vm((2, T, T), BF),
                vm((HOP, PL, GR, D), BF),
                vm((HOP, PL, GR, D), BF),
                vm((HOP, PL, GR, D), BF),
                vm((HOP, PL, GR, D), BF),
                vm((HOP + 1, 2, T, D), BF),
                vm((2, T, D), F32),
                dma((5 + 2 * tp_count,)),
                dma((2,)),
                dma((6,)),
                dma((6,)),
                dma((2 * HOP * chunks,)),
                dma((2 * HOP * chunks,)),
                dma((2 * HOP,)),
                dma((2 * HOP,)),
                dma((HOP * PL,)),
                dma((HOP * PL,)),
                dma((HOP * PL,)),
                dma((HOP * PL,)),
                dma((2 * HOP * chunks,)),
                dma((2 * HOP * chunks,)),
            ],
            compiler_params=pltpu.CompilerParams(
                collective_id=0, has_side_effects=True, vmem_limit_bytes=62 * 1024 * 1024
            ),
        )(
            queries,
            keys_t,
            values_t,
            sink_logit,
            out_weight,
            residual,
            norm_gain.reshape(1, D),
            expert_ids.T,
            route_weights.T,
            gate_weight,
            up_weight,
            down_weight,
        )

    return jax.shard_map(
        on_device,
        mesh=mesh,
        in_specs=(
            P(("grp", "sp"), "tp"),
            P(("grp", "sp"), "tp", None),
            P(("grp", "sp"), "tp", None),
            P("tp"),
            P("tp", None),
            P(("grp", "sp", "tp"), None),
            P(),
            P(("grp", "sp", "tp"), None),
            P(("grp", "sp", "tp"), None),
            P(("sp", "tp"), None, None),
            P(("sp", "tp"), None, None),
            P(("sp", "tp"), None, None),
        ),
        out_specs=P(("grp", "sp", "tp"), None),
        check_vma=False,
    )
```

```python
import functools

import jax
import jax.numpy as jnp
from jax import lax
from jax.experimental import pallas as pl
from jax.experimental.pallas import tpu as pltpu
from jax.sharding import PartitionSpec as P

MESH = pl.DeviceIdType.MESH
BF = jnp.bfloat16
F32 = jnp.float32
CORES = 2
WINDOW = 128
EPS = 1e-06


def mm(a, b):
    return jnp.dot(a, b, preferred_element_type=F32)


def mm_nt(a, b):
    return lax.dot_general(a, b, (((1,), (1,)), ((), ())), preferred_element_type=F32)


def mm_tn(a, b):
    return lax.dot_general(a, b, (((0,), (0,)), ((), ())), preferred_element_type=F32)


def iota(shape, dim):
    return lax.broadcasted_iota(jnp.int32, shape, dim)


PIECE = 16


def prefix_rows(hops, rows, share):
    def prefix(way, hop):
        return min(rows, share * (hops[way] - hop + 1)) if hop <= hops[way] else 0

    return prefix


def ring_order(prefix, rows, ready, latency=3.0, waiting=1):
    queue, left, now, clock = ([], []), [0.0, 0.0], [None, None], 0.0
    own = [list(range(rows // PIECE)) for _ in range(2)]
    coming, events = [], []
    while True:
        for way in range(2):
            while (
                own[way]
                and ready[own[way][0]] <= clock + 1e-6
                and len(queue[way]) + (now[way] is not None) <= waiting
            ):
                piece = own[way].pop(0)
                queue[way].append((piece, 1))
                events.append((clock, "own", way, piece, 1))
            if now[way] is None and queue[way]:
                now[way], left[way] = queue[way].pop(0), 1.0
        busy = [way for way in range(2) if now[way] is not None]
        steps = [clock + left[way] * len(busy) for way in busy]
        steps += [item[0] for item in coming]
        steps += [ready[own[way][0]] for way in range(2) if own[way] and ready[own[way][0]] > clock]
        if not steps:
            return events
        later = min(steps)
        for way in busy:
            left[way] -= (later - clock) / len(busy)
        clock = later
        for way in busy:
            if left[way] < 1e-6:
                coming.append((clock + latency, way) + now[way])
                now[way] = None
        coming.sort()
        while coming and coming[0][0] <= clock + 1e-6:
            _, way, piece, hop = coming.pop(0)
            events.append((clock, "pass", way, piece, hop))
            if piece * PIECE < prefix(way, hop + 1):
                queue[way].append((piece, hop + 1))


def layer(
    dims,
    q_hbm,
    kt_hbm,
    vt_hbm,
    sink_ref,
    wo_hbm,
    res_ref,
    gain_ref,
    ids_ref,
    rw_ref,
    wg_hbm,
    wu_hbm,
    wd_hbm,
    out_ref,
    qv,
    kv,
    wo,
    wg,
    wu,
    wd,
    att,
    s2,
    r2,
    sp,
    sm,
    rp,
    rm,
    acc,
    stream,
    normed,
    own_a,
    ring,
    meta,
    table,
    place,
    sel,
    xin,
    yout,
    zin,
    ret,
    cbuf,
    load_sem,
    halo_sem,
    rs_send,
    rs_recv,
    d_send,
    d_recv,
    m_send,
    m_recv,
    p_send,
    p_recv,
    y_send,
    y_recv,
    b_send,
    b_recv,
):
    T, D, Z, TP, SP, CAP, HEADS, HD = dims
    LAST = Z // 2
    PL = TP * CORES
    CH = PL * CAP
    HALF = D // 2
    HOPS = (Z // 2, Z // 2 - 1)
    GR = 2 * CAP
    SEL = PL * GR

    s = lax.axis_index("sp")
    x = lax.axis_index("tp")
    z = lax.div(s, CORES)
    c = lax.rem(s, CORES)
    me = c * TP + x
    step_a = 1 - 2 * c + Z
    z_next = (lax.rem(z + step_a, Z), lax.rem(z + 2 * Z - step_a, Z))

    def chip(zz):
        return {"sp": zz * CORES + c, "tp": x}

    ahead = (chip(z_next[0]), chip(z_next[1]))
    behind = (ahead[1], ahead[0])

    def to_x(k):
        return {"sp": s, "tp": lax.rem(x + k + TP, TP)}

    def peer(k):
        cc = lax.rem(c + k // TP, CORES)
        return {"sp": z * CORES + cc, "tp": lax.rem(x + k % TP, TP)}

    def peer_rank(k):
        return lax.rem(c + k // TP, CORES) * TP + lax.rem(x + k % TP, TP)

    def from_rank(k):
        return lax.rem(c + CORES - k // TP, CORES) * TP + lax.rem(x + TP - k % TP, TP)

    s_after = {"sp": lax.rem(s + 1, SP), "tp": x}
    s_before = {"sp": lax.rem(s + SP - 1, SP), "tp": x}

    loads = [
        pltpu.make_async_copy(q_hbm, qv, load_sem.at[0]),
        pltpu.make_async_copy(wo_hbm, wo, load_sem.at[1]),
        pltpu.make_async_copy(wg_hbm.at[0], wg, load_sem.at[2]),
        pltpu.make_async_copy(wu_hbm.at[0], wu, load_sem.at[3]),
        pltpu.make_async_copy(wd_hbm.at[0], wd, load_sem.at[4]),
    ]
    kv_loads = []
    for b in range(TP):
        cols = pl.ds(b * T, T)
        kv_loads.append(
            pltpu.make_async_copy(kt_hbm.at[:, cols], kv.at[b + 1, pl.ds(0, HD)], load_sem.at[5 + b])
        )
        kv_loads.append(
            pltpu.make_async_copy(
                vt_hbm.at[:, cols], kv.at[b + 1, pl.ds(HD, HD)], load_sem.at[5 + TP + b]
            )
        )
    barrier = pltpu.get_barrier_semaphore()
    greeted = [ahead[0], ahead[1], s_after, s_before] + [peer(k) for k in range(1, PL)]
    for device in greeted:
        pl.semaphore_signal(barrier, inc=1, device_id=device, device_id_type=MESH)
    for copy in kv_loads[::-1]:
        copy.start()
    loads[0].start()
    loads[1].start()

    halo = pltpu.make_async_remote_copy(
        src_ref=kv.at[TP],
        dst_ref=kv.at[0],
        send_sem=halo_sem.at[0],
        recv_sem=halo_sem.at[1],
        device_id=s_after,
        device_id_type=MESH,
    )

    row_i = iota((T, 2 * T), 0)
    col_j = iota((T, 2 * T), 1)

    def attend(b, slot):
        first = jnp.where(s * TP + b == 0, T, 0)
        allowed = (col_j > row_i) & (col_j <= row_i + T) & (col_j >= first)
        rows = pl.ds(pl.multiple_of(b * T, T), T)
        low = kv[b].astype(F32)
        high = kv[b + 1].astype(F32)
        both = jnp.concatenate([low, high], axis=1)
        kt, vt = both[:HD], both[HD:]
        none = jnp.zeros((HD, 2 * T), F32)
        keys = (jnp.concatenate([kt, none], 0).astype(BF), jnp.concatenate([none, kt], 0).astype(BF))
        values = (jnp.concatenate([vt, none], 0).astype(BF), jnp.concatenate([none, vt], 0).astype(BF))
        for pair in range(HEADS // 2):
            lanes = pl.ds(pair * 2 * HD, 2 * HD)
            query = qv[rows, lanes]
            total = None
            for side in range(2):
                sink = sink_ref[pair * 2 + side]
                score = mm(query, keys[side]) * (HD ** (-0.5))
                score = jnp.where(allowed, score, -jnp.inf)
                top = jnp.maximum(jnp.max(score, axis=1, keepdims=True), sink)
                grown = jnp.exp(score - top)
                weight = jnp.sum(grown, axis=1, keepdims=True) + jnp.exp(sink - top)
                mixed = mm_nt(grown.astype(BF), values[side]) / weight
                total = mixed if total is None else total + mixed
            att[slot, :, lanes] = total.astype(BF)

    def rs_copy(src, dst, index, device):
        return pltpu.make_async_remote_copy(
            src_ref=src,
            dst_ref=dst,
            send_sem=rs_send.at[index],
            recv_sem=rs_recv.at[index],
            device_id=device,
            device_id_type=MESH,
        )

    def project(slot, half):
        return mm(att[slot], wo[:, pl.ds(half * HALF, HALF)])

    right, left = to_x(1), to_x(-1)
    for copy in kv_loads:
        copy.wait()
    loads[0].wait()
    attend(1, 1)
    pl.semaphore_wait(barrier, len(greeted))
    halo.start()
    for copy in loads[2:]:
        copy.start()
    for b in range(2, TP):
        attend(b, b)
    loads[1].wait()
    halo.wait()
    attend(0, 0)
    far, after, prior = lax.rem(x + 2, TP), lax.rem(x + 1, TP), lax.rem(x + TP - 1, TP)
    copies = []
    for half, device in ((0, right), (1, left)):
        s2[half] = project(far, half).astype(BF)
        copy = rs_copy(s2.at[half], r2.at[half], half, device)
        copy.start()
        copies.append(copy)
    sp[1] = project(after, 1).astype(BF)
    send_p1 = rs_copy(sp.at[1], rp.at[1], 2, right)
    send_p1.start()
    sm[0] = project(prior, 0).astype(BF)
    send_m0 = rs_copy(sm.at[0], rm.at[0], 3, left)
    send_m0.start()
    for half in range(2):
        cols = pl.ds(half * HALF, HALF)
        acc[:, cols] = project(x, half) + res_ref[:, cols].astype(F32)
    early = project(after, 0)
    copies[0].wait_recv()
    sp[0] = (early + r2[0].astype(F32)).astype(BF)
    send_p0 = rs_copy(sp.at[0], rp.at[0], 4, right)
    send_p0.start()
    early = project(prior, 1)
    copies[1].wait_recv()
    sm[1] = (early + r2[1].astype(F32)).astype(BF)
    send_m1 = rs_copy(sm.at[1], rm.at[1], 5, left)
    send_m1.start()

    E = Z * PL
    e_sub = iota((E, T), 0)
    t_lane = iota((E, T), 1)
    first_id = ids_ref[0:1, :]
    second_id = ids_ref[1:2, :]
    took0 = jnp.where(e_sub == first_id, 1.0, 0.0).astype(F32)
    took1 = jnp.where(e_sub == second_id, 1.0, 0.0).astype(F32)
    took = took0 + took1
    before = jnp.where(iota((T, T), 0) < iota((T, T), 1), 1.0, 0.0).astype(BF)
    rank = mm(took.astype(BF), before)
    weight_a = rw_ref[0:1, :]
    weight_b = rw_ref[1:2, :]
    whole = weight_a + weight_b
    share = took0 * (weight_a / whole) + took1 * (weight_b / whole)
    plane_bits = PL.bit_length() - 1
    e_plane = lax.shift_right_logical(e_sub, plane_bits)
    rel = (e_plane - z) * (1 - 2 * c) + 2 * Z
    rel = rel & (Z - 1)
    is_a = (rel >= 1) & (rel <= HOPS[0])
    dist = (
        jnp.where(is_a, rel, 0).astype(F32),
        jnp.where(rel > HOPS[0], Z - rel, 0).astype(F32),
    )
    t_sub = iota((T, T), 0)
    t_col = iota((T, T), 1)
    positions = []
    for way in range(2):
        far = jnp.max(took * dist[way], axis=0, keepdims=True)
        along = jnp.broadcast_to(far, (T, T))
        down = along.T
        ahead_of = (down > along) | ((down == along) & (t_sub < t_col))
        positions.append(jnp.sum(jnp.where(ahead_of, 1.0, 0.0), axis=0, keepdims=True))
    for way in range(2):
        place[way] = jnp.where(positions[way] == t_sub.astype(F32), 1.0, 0.0).astype(BF)
    slot_value = jnp.where(is_a, positions[0] + 1.0, positions[1] + (1.0 + T))
    base = (e_sub & (PL - 1)) * GR + jnp.where(is_a, 0, CAP)
    spread_t = jnp.zeros((E, T), F32)
    spread_w = jnp.zeros((E, T), F32)
    for r in range(CAP):
        here = took * jnp.where(rank == float(r), 1.0, 0.0)
        value_col = jnp.sum(here * slot_value, axis=1, keepdims=True)
        share_col = jnp.sum(here * share, axis=1, keepdims=True)
        hit = t_lane == base + r
        spread_t = spread_t + jnp.where(hit, value_col, 0.0)
        spread_w = spread_w + jnp.where(hit, share_col, 0.0)
    plane_of = jnp.where(
        lax.shift_right_logical(iota((Z, E), 1), plane_bits) == iota((Z, E), 0), 1.0, 0.0
    ).astype(BF)
    OWN = HOPS[0] - 1
    meta[OWN, 1, pl.ds(0, Z)] = mm(plane_of, spread_t.astype(BF)).astype(BF)
    meta[OWN, 1, pl.ds(Z, Z)] = mm(plane_of, spread_w.astype(BF)).astype(BF)

    prefix = prefix_rows(HOPS, T, CH)
    for way in range(2):
        for hop in range(1, HOPS[way] + 1):
            n = prefix(way, hop)
            if n < T:
                ring[hop - 1, way, pl.ds(n, T - n)] = jnp.zeros((T - n, D), BF)

    send_p1.wait_recv()
    send_p0.wait_recv()
    send_m0.wait_recv()
    send_m1.wait_recv()
    ROWS = 32
    for r in range(T // ROWS):
        rows = pl.ds(r * ROWS, ROWS)
        square = jnp.zeros((ROWS, 1), F32)
        for half in range(2):
            cols = pl.ds(half * HALF, HALF)
            total = acc[rows, cols] + rp[half, rows].astype(F32) + rm[half, rows].astype(F32)
            kept = total.astype(BF)
            stream[rows, cols] = kept
            wide = kept.astype(F32)
            square = square + jnp.sum(wide * wide, axis=1, keepdims=True)
        scale = lax.rsqrt(square * (1.0 / D) + EPS)
        for half in range(2):
            cols = pl.ds(half * HALF, HALF)
            wide = stream[rows, cols].astype(F32)
            normed[rows, cols] = (wide * scale * gain_ref[:, cols]).astype(BF)

    def d_index(way, hop, j):
        return (way * HOPS[0] + hop - 1) * (T // PIECE) + j

    def packet_copy(way, hop, j):
        rows = pl.ds(j * PIECE, PIECE)
        if hop == 1:
            src = own_a.at[rows] if way == 0 else ring.at[OWN, 1, rows]
        else:
            src = ring.at[hop - 2, way, rows]
        index = d_index(way, hop, j)
        return pltpu.make_async_remote_copy(
            src_ref=src,
            dst_ref=ring.at[hop - 1, way, rows],
            send_sem=d_send.at[index],
            recv_sem=d_recv.at[index],
            device_id=ahead[way],
            device_id_type=MESH,
        )

    def meta_copy(way, hop):
        src = meta.at[OWN, 1] if hop == 1 else meta.at[hop - 2, way]
        index = way * HOPS[0] + hop - 1
        return pltpu.make_async_remote_copy(
            src_ref=src,
            dst_ref=meta.at[hop - 1, way],
            send_sem=m_send.at[index],
            recv_sem=m_recv.at[index],
            device_id=ahead[way],
            device_id_type=MESH,
        )

    for way in range(2):
        meta_copy(way, 1).start()
    for j in range(T // CH):
        rows = pl.ds(j * CH, CH)
        own_a[rows] = mm(place[0, rows], normed[...]).astype(BF)
        ring[OWN, 1, rows] = mm(place[1, rows], normed[...]).astype(BF)
        if j == 0:
            for way in range(2):
                for i in range(2):
                    packet_copy(way, 1, i).start()

    def hop_table(hop):
        picked_t = jnp.zeros((1, T), F32)
        picked_w = jnp.zeros((1, T), F32)
        mine = iota((Z, T), 0) == z
        for way in range(2):
            known = meta[hop - 1, way].astype(F32)
            picked_t = picked_t + jnp.sum(jnp.where(mine, known[:Z], 0.0), axis=0, keepdims=True)
            picked_w = picked_w + jnp.sum(jnp.where(mine, known[Z:], 0.0), axis=0, keepdims=True)
        table[hop - 1, 0:1] = picked_t
        table[hop - 1, 1:2] = picked_w

    def plane_copy(buffer_from, buffer_to, sends, recvs, hop, k):
        index = (hop - 1) * PL + k
        return pltpu.make_async_remote_copy(
            src_ref=buffer_from.at[hop - 1, peer_rank(k)],
            dst_ref=buffer_to.at[hop - 1, me],
            send_sem=sends.at[index],
            recv_sem=recvs.at[index],
            device_id=peer(k),
            device_id_type=MESH,
        )

    def plane_wait(buffer_from, buffer_to, sends, recvs, hop, k):
        index = (hop - 1) * PL + k
        pltpu.make_async_remote_copy(
            src_ref=buffer_from.at[hop - 1, from_rank(k)],
            dst_ref=buffer_to.at[hop - 1, from_rank(k)],
            send_sem=sends.at[index],
            recv_sem=recvs.at[index],
            device_id=peer(k),
            device_id_type=MESH,
        ).wait_recv()

    COLS = 512

    def select(hop):
        hop_table(hop)
        spot = (iota((2 * T, SEL), 0) + 1).astype(F32)
        hot = jnp.where(spot == table[hop - 1, 0:1, 0:SEL], 1.0, 0.0).astype(BF)
        for n in range(D // COLS):
            cols = pl.ds(n * COLS, COLS)
            rows = ring[hop - 1, :, :, cols].reshape(2 * T, COLS)
            sel[hop - 1, :, :, cols] = mm_tn(hot, rows).reshape(PL, GR, COLS).astype(BF)
        for k in range(1, PL):
            plane_copy(sel, xin, p_send, p_recv, hop, k).start()
        xin[hop - 1, me] = sel[hop - 1, me]

    def experts(*hops):
        for hop in hops:
            for k in range(1, PL):
                plane_wait(sel, xin, p_send, p_recv, hop, k)
        rows = jnp.concatenate(
            [xin[hop - 1].astype(F32).reshape(SEL, D).astype(BF) for hop in hops], axis=0
        )
        gate = mm(rows, wg[...])
        upward = mm(rows, wu[...])
        hidden = (gate / (1.0 + jnp.exp(-gate)) * upward).astype(BF)
        for n in range(D // COLS):
            cols = pl.ds(n * COLS, COLS)
            product = mm(hidden, wd[:, cols])
            for i, hop in enumerate(hops):
                part = product[i * SEL : (i + 1) * SEL]
                yout[hop - 1, :, :, cols] = part.reshape(PL, GR, COLS).astype(BF)
        for hop in hops:
            for k in range(1, PL):
                plane_copy(yout, zin, y_send, y_recv, hop, k).start()
            zin[hop - 1, me] = yout[hop - 1, me]

    def back_copy(way, hop, j):
        rows = pl.ds(j * PIECE, PIECE)
        index = d_index(way, hop, j)
        return pltpu.make_async_remote_copy(
            src_ref=ret.at[hop, way, rows],
            dst_ref=ret.at[hop - 1, way, rows],
            send_sem=b_send.at[index],
            recv_sem=b_recv.at[index],
            device_id=behind[way],
            device_id_type=MESH,
        )

    def weighted(hop, ways):
        for k in range(1, PL):
            plane_wait(yout, zin, y_send, y_recv, hop, k)
        mixes = []
        for way, n in ways:
            spot = (iota((n, SEL), 0) + (way * T + 1)).astype(F32)
            hit = spot == table[hop - 1, 0:1, 0:SEL]
            mixes.append(jnp.where(hit, table[hop - 1, 1:2, 0:SEL], 0.0).astype(BF))
        for n in range(D // COLS):
            cols = pl.ds(n * COLS, COLS)
            rows = zin[hop - 1, :, :, cols].astype(F32).reshape(SEL, COLS).astype(BF)
            for (way, count), mix in zip(ways, mixes):
                cbuf[way, pl.ds(0, count), cols] = mm(mix, rows)

    def send_back(hop):
        if hop == LAST:
            weighted(hop, [(0, prefix(0, hop)), (1, T)])
            acc[...] = cbuf[1]
        else:
            weighted(hop, [(way, prefix(way, hop)) for way in range(2)])
        for i in range(T // PIECE):
            for way in range(2):
                j = prefix(way, hop) // PIECE - 1 - i
                if j < 0:
                    continue
                rows = pl.ds(j * PIECE, PIECE)
                part = cbuf[way, rows]
                if j * PIECE < prefix(way, hop + 1):
                    back_copy(way, hop + 1, j).wait_recv()
                    part = part + ret[hop, way, rows].astype(F32)
                ret[hop, way, rows] = part.astype(BF)
                back_copy(way, hop, j).start()

    def pass_on(way, hop, j):
        if j * PIECE < prefix(way, hop):
            packet_copy(way, hop, j).wait_recv()
        if j * PIECE < prefix(way, hop + 1):
            packet_copy(way, hop + 1, j).start()

    for copy in loads[2:]:
        copy.wait()
    def meta_on(way, hop):
        meta_copy(way, hop).wait_recv()
        if hop < HOPS[way]:
            meta_copy(way, hop + 1).start()

    events = ring_order(prefix, T, [0.0] * (T // PIECE))
    missing = {
        hop: sum(-(-prefix(way, hop) // PIECE) for way in range(2)) for hop in range(1, LAST + 1)
    }
    deferred = []
    begun = {(0, 0), (0, 1), (1, 0), (1, 1)}
    seen = set()
    for when, action, way, piece, hop in events:
        while deferred and deferred[0][0] <= when:
            deferred.pop(0)[1]()
        if action == "own":
            if (way, piece) not in begun:
                packet_copy(way, 1, piece).start()
            continue
        if (way, hop) not in seen:
            seen.add((way, hop))
            meta_on(way, hop)
        pass_on(way, hop, piece)
        missing[hop] -= 1
        if missing[hop] == 0:
            select(hop)
            if not missing[LAST] and not missing[LAST - 1] and not deferred and hop >= LAST - 1:
                deferred = [
                    (when + 12.0, lambda: experts(LAST, LAST - 1)),
                    (when + 23.0, lambda: send_back(LAST)),
                ]
    for _, work in deferred:
        work()
    send_back(LAST - 1)
    experts(LAST - 2, LAST - 3)
    experts(1, 2)
    experts(3, 4)
    for hop in range(LAST - 2, 0, -1):
        send_back(hop)

    for j in range(T // PIECE):
        rows = pl.ds(j * PIECE, PIECE)
        for way in range(2):
            back_copy(way, 1, j).wait_recv()
        ret[0, 1, rows] = (ret[0, 1, rows].astype(F32) + acc[rows]).astype(BF)
    unsort = place[...].reshape(2 * T, T)
    for n in range(D // COLS):
        cols = pl.ds(n * COLS, COLS)
        came = ret[0, :, :, cols].reshape(2 * T, COLS)
        out_ref[:, cols] = (stream[:, cols].astype(F32) + mm_tn(unsort, came)).astype(BF)

    for copy in copies + [send_p1, send_m0, send_p0, send_m1]:
        copy.wait_send()
    for way in range(2):
        for hop in range(1, HOPS[way] + 1):
            meta_copy(way, hop).wait_send()
            for j in range(T // PIECE):
                if j * PIECE < prefix(way, hop):
                    packet_copy(way, hop, j).wait_send()
                    back_copy(way, hop, j).wait_send()
    for hop in range(1, LAST + 1):
        for k in range(1, PL):
            plane_copy(sel, xin, p_send, p_recv, hop, k).wait_send()
            plane_copy(yout, zin, y_send, y_recv, hop, k).wait_send()


def solution(mesh):
    sp_count = mesh.shape["sp"]
    tp_count = mesh.shape["tp"]

    def on_device(
        queries,
        key_heads,
        value_heads,
        sink_logit,
        out_weight,
        residual,
        norm_gain,
        expert_ids,
        route_weights,
        gate_weight,
        up_weight,
        down_weight,
    ):
        T, D = residual.shape
        HD = key_heads.shape[2]
        HEADS = queries.shape[1] // HD
        FF = gate_weight.shape[2]
        Z = sp_count // CORES
        PL = tp_count * CORES
        top_k = expert_ids.shape[1]
        CAP = max(2, 2 * top_k * T // (sp_count * tp_count))
        GR = 2 * CAP
        HOP = Z // 2
        keys_t = jnp.transpose(key_heads, (1, 2, 0)).reshape(HD, -1)
        values_t = jnp.transpose(value_heads, (1, 2, 0)).reshape(HD, -1)
        dma = pltpu.SemaphoreType.DMA
        vm = pltpu.VMEM
        any_space = pl.BlockSpec(memory_space=pl.ANY)
        in_vmem = pl.BlockSpec(memory_space=pltpu.VMEM)
        dims = (T, D, Z, tp_count, sp_count, CAP, HEADS, HD)
        chunks = T // PIECE
        return pl.pallas_call(
            functools.partial(layer, dims),
            out_shape=jax.ShapeDtypeStruct((T, D), BF),
            in_specs=[
                any_space,
                any_space,
                any_space,
                pl.BlockSpec(memory_space=pltpu.SMEM),
                any_space,
                in_vmem,
                in_vmem,
                in_vmem,
                in_vmem,
                any_space,
                any_space,
                any_space,
            ],
            out_specs=in_vmem,
            scratch_shapes=[
                vm(queries.shape, BF),
                vm((tp_count + 1, 2 * HD, T), BF),
                vm(out_weight.shape, BF),
                vm((D, FF), BF),
                vm((D, FF), BF),
                vm((FF, D), BF),
                vm((4, T, HEADS * HD), BF),
                vm((2, T, D // 2), BF),
                vm((2, T, D // 2), BF),
                vm((2, T, D // 2), BF),
                vm((2, T, D // 2), BF),
                vm((2, T, D // 2), BF),
                vm((2, T, D // 2), BF),
                vm((T, D), F32),
                vm((T, D), BF),
                vm((T, D), BF),
                vm((T, D), BF),
                vm((HOP, 2, T, D), BF),
                vm((HOP, 2, 2 * Z, T), BF),
                vm((HOP, 8, T), F32),
                vm((2, T, T), BF),
                vm((HOP, PL, GR, D), BF),
                vm((HOP, PL, GR, D), BF),
                vm((HOP, PL, GR, D), BF),
                vm((HOP, PL, GR, D), BF),
                vm((HOP + 1, 2, T, D), BF),
                vm((2, T, D), F32),
                dma((5 + 2 * tp_count,)),
                dma((2,)),
                dma((6,)),
                dma((6,)),
                dma((2 * HOP * chunks,)),
                dma((2 * HOP * chunks,)),
                dma((2 * HOP,)),
                dma((2 * HOP,)),
                dma((HOP * PL,)),
                dma((HOP * PL,)),
                dma((HOP * PL,)),
                dma((HOP * PL,)),
                dma((2 * HOP * chunks,)),
                dma((2 * HOP * chunks,)),
            ],
            compiler_params=pltpu.CompilerParams(
                collective_id=0, has_side_effects=True, vmem_limit_bytes=62 * 1024 * 1024
            ),
        )(
            queries,
            keys_t,
            values_t,
            sink_logit,
            out_weight,
            residual,
            norm_gain.reshape(1, D),
            expert_ids.T,
            route_weights.T,
            gate_weight,
            up_weight,
            down_weight,
        )

    return jax.shard_map(
        on_device,
        mesh=mesh,
        in_specs=(
            P(("grp", "sp"), "tp"),
            P(("grp", "sp"), "tp", None),
            P(("grp", "sp"), "tp", None),
            P("tp"),
            P("tp", None),
            P(("grp", "sp", "tp"), None),
            P(),
            P(("grp", "sp", "tp"), None),
            P(("grp", "sp", "tp"), None),
            P(("sp", "tp"), None, None),
            P(("sp", "tp"), None, None),
            P(("sp", "tp"), None, None),
        ),
        out_specs=P(("grp", "sp", "tp"), None),
        check_vma=False,
    )
```

```python
import functools

import jax
import jax.numpy as jnp
from jax import lax
from jax.experimental import pallas as pl
from jax.experimental.pallas import tpu as pltpu
from jax.sharding import PartitionSpec as P

MESH = pl.DeviceIdType.MESH
BF = jnp.bfloat16
F32 = jnp.float32
CORES = 2
WINDOW = 128
EPS = 1e-06


def mm(a, b):
    return jnp.dot(a, b, preferred_element_type=F32)


def mm_nt(a, b):
    return lax.dot_general(a, b, (((1,), (1,)), ((), ())), preferred_element_type=F32)


def mm_tn(a, b):
    return lax.dot_general(a, b, (((0,), (0,)), ((), ())), preferred_element_type=F32)


def iota(shape, dim):
    return lax.broadcasted_iota(jnp.int32, shape, dim)


PIECE = 16


def prefix_rows(hops, rows, share):
    def prefix(way, hop):
        return min(rows, share * (hops[way] - hop + 1)) if hop <= hops[way] else 0

    return prefix


def ring_order(prefix, rows, ready, latency=3.0, waiting=1):
    queue, left, now, clock = ([], []), [0.0, 0.0], [None, None], 0.0
    own = [list(range(rows // PIECE)) for _ in range(2)]
    coming, events = [], []
    while True:
        for way in range(2):
            while (
                own[way]
                and ready[own[way][0]] <= clock + 1e-6
                and len(queue[way]) + (now[way] is not None) <= waiting
            ):
                piece = own[way].pop(0)
                queue[way].append((piece, 1))
                events.append((clock, "own", way, piece, 1))
            if now[way] is None and queue[way]:
                now[way], left[way] = queue[way].pop(0), 1.0
        busy = [way for way in range(2) if now[way] is not None]
        steps = [clock + left[way] * len(busy) for way in busy]
        steps += [item[0] for item in coming]
        steps += [ready[own[way][0]] for way in range(2) if own[way] and ready[own[way][0]] > clock]
        if not steps:
            return events
        later = min(steps)
        for way in busy:
            left[way] -= (later - clock) / len(busy)
        clock = later
        for way in busy:
            if left[way] < 1e-6:
                coming.append((clock + latency, way) + now[way])
                now[way] = None
        coming.sort()
        while coming and coming[0][0] <= clock + 1e-6:
            _, way, piece, hop = coming.pop(0)
            events.append((clock, "pass", way, piece, hop))
            if piece * PIECE < prefix(way, hop + 1):
                queue[way].append((piece, hop + 1))


def layer(
    dims,
    q_hbm,
    kt_hbm,
    vt_hbm,
    sink_hbm,
    wo_hbm,
    res_hbm,
    gain_hbm,
    ids_hbm,
    rw_hbm,
    wg_hbm,
    wu_hbm,
    wd_hbm,
    out_ref,
    qv,
    kv,
    wo,
    wg,
    wu,
    wd,
    sink_ref,
    res_ref,
    gain_ref,
    ids_ref,
    rw_ref,
    att,
    att_c,
    s2,
    r2,
    sp,
    sm,
    rp,
    rm,
    acc,
    stream,
    normed,
    own_a,
    ring,
    meta,
    table,
    place,
    sorter,
    sel,
    xin,
    yout,
    zin,
    ret,
    cbuf,
    load_sem,
    kv_sem,
    halo_sem,
    ids_send,
    ids_recv,
    rs_send,
    rs_recv,
    d_send,
    d_recv,
    m_send,
    m_recv,
    p_send,
    p_recv,
    y_send,
    y_recv,
    b_send,
    b_recv,
):
    T, D, Z, TP, SP, CAP, HEADS, HD = dims
    LAST = Z // 2
    PL = TP * CORES
    CH = PL * CAP
    HALF = D // 2
    HOPS = (Z // 2, Z // 2 - 1)
    GR = 2 * CAP
    SEL = PL * GR

    s = lax.axis_index("sp")
    x = lax.axis_index("tp")
    z = lax.div(s, CORES)
    c = lax.rem(s, CORES)
    me = c * TP + x
    step_a = 1 - 2 * c + Z
    z_next = (lax.rem(z + step_a, Z), lax.rem(z + 2 * Z - step_a, Z))

    def chip(zz):
        return {"sp": zz * CORES + c, "tp": x}

    ahead = (chip(z_next[0]), chip(z_next[1]))
    behind = (ahead[1], ahead[0])

    def to_x(k):
        return {"sp": s, "tp": lax.rem(x + k + TP, TP)}

    def peer(k):
        cc = lax.rem(c + k // TP, CORES)
        return {"sp": z * CORES + cc, "tp": lax.rem(x + k % TP, TP)}

    def peer_rank(k):
        return lax.rem(c + k // TP, CORES) * TP + lax.rem(x + k % TP, TP)

    def from_rank(k):
        return lax.rem(c + CORES - k // TP, CORES) * TP + lax.rem(x + TP - k % TP, TP)

    s_after = {"sp": lax.rem(s + 1, SP), "tp": x}
    s_before = {"sp": lax.rem(s + SP - 1, SP), "tp": x}

    small = [
        pltpu.make_async_copy(src, dst, load_sem.at[i])
        for i, (src, dst) in enumerate(
            (
                (q_hbm, qv),
                (sink_hbm, sink_ref),
                (ids_hbm, ids_ref.at[0]),
                (rw_hbm, rw_ref),
            )
        )
    ]
    wo_load = pltpu.make_async_copy(wo_hbm, wo, load_sem.at[4])
    large = [
        pltpu.make_async_copy(src, dst, load_sem.at[5 + i])
        for i, (src, dst) in enumerate(
            (
                (res_hbm, res_ref),
                (gain_hbm, gain_ref),
                (wg_hbm.at[0], wg),
                (wu_hbm.at[0], wu),
                (wd_hbm.at[0], wd),
            )
        )
    ]
    kv_loads = []
    for b in range(TP):
        cols = pl.ds(b * T, T)
        for i, src in enumerate((kt_hbm, vt_hbm)):
            kv_loads.append(
                pltpu.make_async_copy(
                    src.at[:, cols], kv.at[b + 1, pl.ds(i * HD, HD)], kv_sem.at[2 * b + i]
                )
            )
    barrier = pltpu.get_barrier_semaphore()
    greeted = [ahead[0], ahead[1], s_after, s_before] + [peer(k) for k in range(1, PL)]
    for device in greeted:
        pl.semaphore_signal(barrier, inc=1, device_id=device, device_id_type=MESH)
    for copy in kv_loads + small + [wo_load]:
        copy.start()

    halo = pltpu.make_async_remote_copy(
        src_ref=kv.at[TP],
        dst_ref=kv.at[0],
        send_sem=halo_sem.at[0],
        recv_sem=halo_sem.at[1],
        device_id=s_after,
        device_id_type=MESH,
    )

    row_i = iota((T, 2 * T), 0)
    col_j = iota((T, 2 * T), 1)

    def attend(b, slot):
        first = jnp.where(s * TP + b == 0, T, 0)
        allowed = (col_j > row_i) & (col_j <= row_i + T) & (col_j >= first)
        rows = pl.ds(pl.multiple_of(b * T, T), T)
        low = kv[b].astype(F32)
        high = kv[b + 1].astype(F32)
        both = jnp.concatenate([low, high], axis=1)
        kt, vt = both[:HD], both[HD:]
        none = jnp.zeros((HD, 2 * T), F32)
        keys = (jnp.concatenate([kt, none], 0).astype(BF), jnp.concatenate([none, kt], 0).astype(BF))
        values = (jnp.concatenate([vt, none], 0).astype(BF), jnp.concatenate([none, vt], 0).astype(BF))
        for pair in range(HEADS // 2):
            lanes = pl.ds(pair * 2 * HD, 2 * HD)
            query = qv[rows, lanes]
            total = None
            for side in range(2):
                head = pair * 2 + side
                sink = sink_ref[0:1, head : head + 1]
                score = mm(query, keys[side]) * (HD ** (-0.5))
                score = jnp.where(allowed, score, -jnp.inf)
                top = jnp.maximum(jnp.max(score, axis=1, keepdims=True), sink)
                grown = jnp.exp(score - top)
                weight = jnp.sum(grown, axis=1, keepdims=True) + jnp.exp(sink - top)
                mixed = mm_nt(grown.astype(BF), values[side]) / weight
                total = mixed if total is None else total + mixed
            att[slot, :, lanes] = total.astype(BF)

    E = Z * PL
    plane_bits = PL.bit_length() - 1
    e_sub = iota((E, T), 0)
    t_sub = iota((T, T), 0)
    t_col = iota((T, T), 1)
    rel = (lax.shift_right_logical(e_sub, plane_bits) - z) * (1 - 2 * c) + 2 * Z
    rel = rel & (Z - 1)
    is_a = (rel >= 1) & (rel <= HOPS[0])
    dist = (
        jnp.where(is_a, rel, 0).astype(F32),
        jnp.where(rel > HOPS[0], Z - rel, 0).astype(F32),
    )

    def rank_of(key):
        along = jnp.broadcast_to(key, (T, T))
        down = along.T
        ahead_of = (down > along) | ((down == along) & (t_sub < t_col))
        return jnp.sum(jnp.where(ahead_of, 1.0, 0.0), axis=0, keepdims=True)

    def orders(slot):
        took = [
            jnp.where(e_sub == ids_ref[slot, k : k + 1, :], 1.0, 0.0).astype(F32) for k in range(2)
        ]
        both = took[0] + took[1]
        ways = [rank_of(jnp.max(both * d, axis=0, keepdims=True)) for d in dist]
        return took, ways, rank_of(-jnp.minimum(ways[0], ways[1]))

    def placing(position):
        return jnp.where(position == t_sub.astype(F32), 1.0, 0.0).astype(BF)

    right, left = to_x(1), to_x(-1)
    QUARTERS = T // CH

    def rs_copy(kind, q):
        src, dst, half, device, group = (
            (s2, r2, 0, right, 0),
            (s2, r2, 1, left, 0),
            (sp, rp, 1, right, 1),
            (sm, rm, 0, left, 2),
            (sp, rp, 0, right, 1),
            (sm, rm, 1, left, 2),
        )[kind]
        rows = pl.ds(q * CH, CH)
        return pltpu.make_async_remote_copy(
            src_ref=src.at[half, rows],
            dst_ref=dst.at[half, rows],
            send_sem=rs_send.at[group],
            recv_sem=rs_recv.at[kind * QUARTERS + q],
            device_id=device,
            device_id_type=MESH,
        )

    def first_leg(q):
        rs_copy(0, q).start()
        rs_copy(1, q).start()

    def alone(q):
        rs_copy(2, q).start()
        rs_copy(3, q).start()

    def joined(q):
        rows = pl.ds(q * CH, CH)
        for kind, dst, half in ((0, sp, 0), (1, sm, 1)):
            rs_copy(kind, q).wait_recv()
            total = cbuf[half, rows, pl.ds(0, HALF)] + r2[half, rows].astype(F32)
            dst[half, rows] = total.astype(BF)
            rs_copy(4 + kind, q).start()

    def project(slot, half):
        return mm(att_c[slot], wo[:, pl.ds(half * HALF, HALF)])

    def ids_copy(m):
        return pltpu.make_async_remote_copy(
            src_ref=ids_ref.at[0],
            dst_ref=ids_ref.at[m],
            send_sem=ids_send.at[m],
            recv_sem=ids_recv.at[m],
            device_id=to_x(-m),
            device_id_type=MESH,
        )

    for copy in kv_loads + small:
        copy.wait()
    attend(1, 1)
    pl.semaphore_wait(barrier, len(greeted))
    halo.start()
    for m in range(1, TP):
        ids_copy(m).start()
    for copy in large:
        copy.start()
    for b in range(2, TP):
        attend(b, b)
    took, positions, position_c = orders(0)
    place[0] = placing(positions[0])
    place[1] = placing(positions[1])
    place[2] = placing(position_c)
    halo.wait_recv()
    attend(0, 0)
    for m in range(1, TP):
        ids_copy(m).wait_recv()

    def arrange(m, placed):
        att_c[m] = mm(placed, att[lax.rem(x + m, TP)]).astype(BF)

    far, after, prior = 2, 1, TP - 1
    arrange(far, placing(orders(far)[2]))
    wo_load.wait()
    for half in range(2):
        s2[half] = project(far, half).astype(BF)
    first_leg(0)
    for m in (after, prior):
        arrange(m, placing(orders(m)[2]))
    sp[1] = project(after, 1).astype(BF)
    sm[0] = project(prior, 0).astype(BF)
    alone(0)
    first_leg(1)
    first_leg(2)
    cbuf[0, :, pl.ds(0, HALF)] = project(after, 0)
    cbuf[1, :, pl.ds(0, HALF)] = project(prior, 1)
    joined(0)
    alone(1)
    first_leg(3)
    large[0].wait()
    large[1].wait()
    arrange(0, place[2])
    for half in range(2):
        cols = pl.ds(half * HALF, HALF)
        acc[:, cols] = project(0, half) + mm(place[2], res_ref[:, cols])
    joined(1)
    alone(2)

    t_lane = iota((E, T), 1)
    either = took[0] + took[1]
    before = jnp.where(t_sub < t_col, 1.0, 0.0).astype(BF)
    rank = mm(either.astype(BF), before)
    weight_a = rw_ref[0:1, :]
    weight_b = rw_ref[1:2, :]
    whole = weight_a + weight_b
    share = took[0] * (weight_a / whole) + took[1] * (weight_b / whole)
    slot_value = jnp.where(is_a, positions[0] + 1.0, positions[1] + (1.0 + T))
    base = (e_sub & (PL - 1)) * GR + jnp.where(is_a, 0, CAP)
    spread_t = jnp.zeros((E, T), F32)
    spread_w = jnp.zeros((E, T), F32)
    for r in range(CAP):
        here = either * jnp.where(rank == float(r), 1.0, 0.0)
        value_col = jnp.sum(here * slot_value, axis=1, keepdims=True)
        share_col = jnp.sum(here * share, axis=1, keepdims=True)
        hit = t_lane == base + r
        spread_t = spread_t + jnp.where(hit, value_col, 0.0)
        spread_w = spread_w + jnp.where(hit, share_col, 0.0)
    plane_of = jnp.where(
        lax.shift_right_logical(iota((Z, E), 1), plane_bits) == iota((Z, E), 0), 1.0, 0.0
    ).astype(BF)
    OWN = HOPS[0] - 1
    meta[OWN, 1, pl.ds(0, Z)] = mm(plane_of, spread_t.astype(BF)).astype(BF)
    meta[OWN, 1, pl.ds(Z, Z)] = mm(plane_of, spread_w.astype(BF)).astype(BF)
    for way in range(2):
        sorter[way] = mm_nt(place[way], place[2]).astype(BF)
    normed[...] = jnp.zeros((T, D), BF)

    prefix = prefix_rows(HOPS, T, CH)
    for way in range(2):
        for hop in range(1, HOPS[way] + 1):
            n = prefix(way, hop)
            if n < T:
                ring[hop - 1, way, pl.ds(n, T - n)] = jnp.zeros((T - n, D), BF)
    joined(2)
    alone(3)

    def prepare(q):
        for kind in range(2, 6):
            rs_copy(kind, q).wait_recv()
        rows = pl.ds(q * CH, CH)
        square = jnp.zeros((CH, 1), F32)
        for half in range(2):
            cols = pl.ds(half * HALF, HALF)
            total = acc[rows, cols] + rp[half, rows].astype(F32) + rm[half, rows].astype(F32)
            kept = total.astype(BF)
            stream[rows, cols] = kept
            wide = kept.astype(F32)
            square = square + jnp.sum(wide * wide, axis=1, keepdims=True)
        scale = lax.rsqrt(square * (1.0 / D) + EPS)
        for half in range(2):
            cols = pl.ds(half * HALF, HALF)
            wide = stream[rows, cols].astype(F32)
            normed[rows, cols] = (wide * scale * gain_ref[:, cols]).astype(BF)
        count = PIECE if q < QUARTERS - 1 else T - q * PIECE
        rows = pl.ds(q * PIECE, count)
        own_a[rows] = mm(sorter[0, rows], normed[...]).astype(BF)
        ring[OWN, 1, rows] = mm(sorter[1, rows], normed[...]).astype(BF)

    first_index, pieces = {}, 0
    for way in range(2):
        for hop in range(1, HOPS[way] + 1):
            first_index[way, hop] = pieces
            pieces += prefix(way, hop) // PIECE

    def d_index(way, hop, j):
        return first_index[way, hop] + j

    def hop_index(way, hop):
        return way * HOPS[0] + hop - 1

    def packet_copy(way, hop, j):
        rows = pl.ds(j * PIECE, PIECE)
        if hop == 1:
            src = own_a.at[rows] if way == 0 else ring.at[OWN, 1, rows]
        else:
            src = ring.at[hop - 2, way, rows]
        index = d_index(way, hop, j)
        return pltpu.make_async_remote_copy(
            src_ref=src,
            dst_ref=ring.at[hop - 1, way, rows],
            send_sem=d_send.at[hop_index(way, hop)],
            recv_sem=d_recv.at[index],
            device_id=ahead[way],
            device_id_type=MESH,
        )

    def meta_copy(way, hop):
        src = meta.at[OWN, 1] if hop == 1 else meta.at[hop - 2, way]
        index = hop_index(way, hop)
        return pltpu.make_async_remote_copy(
            src_ref=src,
            dst_ref=meta.at[hop - 1, way],
            send_sem=m_send.at[index],
            recv_sem=m_recv.at[index],
            device_id=ahead[way],
            device_id_type=MESH,
        )

    for way in range(2):
        meta_copy(way, 1).start()
    prepare(0)
    for way in range(2):
        packet_copy(way, 1, 0).start()
    joined(QUARTERS - 1)

    def hop_table(hop):
        picked_t = jnp.zeros((1, T), F32)
        picked_w = jnp.zeros((1, T), F32)
        mine = iota((Z, T), 0) == z
        for way in range(2):
            known = meta[hop - 1, way].astype(F32)
            picked_t = picked_t + jnp.sum(jnp.where(mine, known[:Z], 0.0), axis=0, keepdims=True)
            picked_w = picked_w + jnp.sum(jnp.where(mine, known[Z:], 0.0), axis=0, keepdims=True)
        table[hop - 1, 0:1] = picked_t
        table[hop - 1, 1:2] = picked_w

    def plane_copy(buffer_from, buffer_to, sends, recvs, hop, k):
        return pltpu.make_async_remote_copy(
            src_ref=buffer_from.at[hop - 1, peer_rank(k)],
            dst_ref=buffer_to.at[hop - 1, me],
            send_sem=sends.at[hop - 1],
            recv_sem=recvs.at[hop - 1],
            device_id=peer(k),
            device_id_type=MESH,
        )

    def plane_all(buffer_from, buffer_to, sends, recvs, hop):
        blocks = pl.ds(0, PL - 1)
        return pltpu.make_async_remote_copy(
            src_ref=buffer_from.at[hop - 1, blocks],
            dst_ref=buffer_to.at[hop - 1, blocks],
            send_sem=sends.at[hop - 1],
            recv_sem=recvs.at[hop - 1],
            device_id=peer(1),
            device_id_type=MESH,
        )

    COLS = 512

    def select(hop):
        hop_table(hop)
        spot = (iota((2 * T, SEL), 0) + 1).astype(F32)
        hot = jnp.where(spot == table[hop - 1, 0:1, 0:SEL], 1.0, 0.0).astype(BF)
        for n in range(D // COLS):
            cols = pl.ds(n * COLS, COLS)
            rows = ring[hop - 1, :, :, cols].reshape(2 * T, COLS)
            sel[hop - 1, :, :, cols] = mm_tn(hot, rows).reshape(PL, GR, COLS).astype(BF)
        for k in range(1, PL):
            plane_copy(sel, xin, p_send, p_recv, hop, k).start()
        xin[hop - 1, me] = sel[hop - 1, me]

    def experts(*hops):
        for hop in hops:
            plane_all(sel, xin, p_send, p_recv, hop).wait_recv()
        rows = jnp.concatenate(
            [xin[hop - 1].astype(F32).reshape(SEL, D).astype(BF) for hop in hops], axis=0
        )
        gate = mm(rows, wg[...])
        upward = mm(rows, wu[...])
        hidden = (gate / (1.0 + jnp.exp(-gate)) * upward).astype(BF)
        for n in range(D // COLS):
            cols = pl.ds(n * COLS, COLS)
            product = mm(hidden, wd[:, cols])
            for i, hop in enumerate(hops):
                part = product[i * SEL : (i + 1) * SEL]
                yout[hop - 1, :, :, cols] = part.reshape(PL, GR, COLS).astype(BF)
        for hop in hops:
            for k in range(1, PL):
                plane_copy(yout, zin, y_send, y_recv, hop, k).start()
            zin[hop - 1, me] = yout[hop - 1, me]

    def back_copy(way, hop, j):
        rows = pl.ds(j * PIECE, PIECE)
        index = d_index(way, hop, j)
        return pltpu.make_async_remote_copy(
            src_ref=ret.at[hop, way, rows],
            dst_ref=ret.at[hop - 1, way, rows],
            send_sem=b_send.at[hop_index(way, hop)],
            recv_sem=b_recv.at[index],
            device_id=behind[way],
            device_id_type=MESH,
        )

    def weighted(hop, ways):
        plane_all(yout, zin, y_send, y_recv, hop).wait_recv()
        mixes = []
        for way, n in ways:
            spot = (iota((n, SEL), 0) + (way * T + 1)).astype(F32)
            hit = spot == table[hop - 1, 0:1, 0:SEL]
            mixes.append(jnp.where(hit, table[hop - 1, 1:2, 0:SEL], 0.0).astype(BF))
        for n in range(D // COLS):
            cols = pl.ds(n * COLS, COLS)
            rows = zin[hop - 1, :, :, cols].astype(F32).reshape(SEL, COLS).astype(BF)
            for (way, count), mix in zip(ways, mixes):
                cbuf[way, pl.ds(0, count), cols] = mm(mix, rows)

    def send_back(hop):
        if hop == LAST:
            weighted(hop, [(0, prefix(0, hop)), (1, T)])
            acc[...] = cbuf[1]
        else:
            weighted(hop, [(way, prefix(way, hop)) for way in range(2)])
        for i in range(T // PIECE):
            for way in range(2):
                j = prefix(way, hop) // PIECE - 1 - i
                if j < 0:
                    continue
                rows = pl.ds(j * PIECE, PIECE)
                part = cbuf[way, rows]
                if j * PIECE < prefix(way, hop + 1):
                    back_copy(way, hop + 1, j).wait_recv()
                    part = part + ret[hop, way, rows].astype(F32)
                ret[hop, way, rows] = part.astype(BF)
                back_copy(way, hop, j).start()

    def pass_on(way, hop, j):
        if j * PIECE < prefix(way, hop):
            packet_copy(way, hop, j).wait_recv()
        if j * PIECE < prefix(way, hop + 1):
            packet_copy(way, hop + 1, j).start()

    for copy in large[2:]:
        copy.wait()
    def meta_on(way, hop):
        meta_copy(way, hop).wait_recv()
        if hop < HOPS[way]:
            meta_copy(way, hop + 1).start()

    ready = [0.0, 6.0, 10.0] + [14.0] * (T // PIECE - QUARTERS + 1)
    events = ring_order(prefix, T, ready)
    prepared = 1
    missing = {
        hop: sum(-(-prefix(way, hop) // PIECE) for way in range(2)) for hop in range(1, LAST + 1)
    }
    deferred = []
    seen = set()
    for when, action, way, piece, hop in events:
        while deferred and deferred[0][0] <= when:
            deferred.pop(0)[1]()
        if action == "own":
            if prepared < QUARTERS and piece >= prepared:
                prepare(prepared)
                prepared += 1
            if piece > 0:
                packet_copy(way, 1, piece).start()
            continue
        if (way, hop) not in seen:
            seen.add((way, hop))
            meta_on(way, hop)
        pass_on(way, hop, piece)
        missing[hop] -= 1
        if missing[hop] == 0:
            select(hop)
            if not missing[LAST] and not missing[LAST - 1] and not deferred and hop >= LAST - 1:
                deferred = [(when + 12.0, lambda: experts(LAST, LAST - 1))]
    for _, work in deferred:
        work()
    send_back(LAST)
    send_back(LAST - 1)
    experts(LAST - 2, LAST - 3)
    experts(1, 2)
    experts(3, 4)
    for hop in range(LAST - 2, 0, -1):
        send_back(hop)

    for j in range(T // PIECE):
        rows = pl.ds(j * PIECE, PIECE)
        for way in range(2):
            back_copy(way, 1, j).wait_recv()
        ret[0, 1, rows] = (ret[0, 1, rows].astype(F32) + acc[rows]).astype(BF)
    unsort = place[pl.ds(0, 2)].reshape(2 * T, T)
    for n in range(D // COLS):
        cols = pl.ds(n * COLS, COLS)
        came = ret[0, :, :, cols].reshape(2 * T, COLS)
        out_ref[:, cols] = (mm_tn(place[2], stream[:, cols]) + mm_tn(unsort, came)).astype(BF)

    halo.wait_send()
    for m in range(1, TP):
        ids_copy(m).wait_send()
    for group, (src, dst) in enumerate(((s2, r2), (sp, rp), (sm, rm))):
        pltpu.make_async_remote_copy(
            src_ref=src,
            dst_ref=dst,
            send_sem=rs_send.at[group],
            recv_sem=rs_recv.at[0],
            device_id=right,
            device_id_type=MESH,
        ).wait_send()
    for way in range(2):
        for hop in range(1, HOPS[way] + 1):
            meta_copy(way, hop).wait_send()
            rows = pl.ds(0, prefix(way, hop))
            for buffer, sems, recvs in ((ring, d_send, d_recv), (ret, b_send, b_recv)):
                pltpu.make_async_remote_copy(
                    src_ref=buffer.at[hop - 1, way, rows],
                    dst_ref=buffer.at[hop - 1, way, rows],
                    send_sem=sems.at[hop_index(way, hop)],
                    recv_sem=recvs.at[0],
                    device_id=ahead[way],
                    device_id_type=MESH,
                ).wait_send()
    for hop in range(1, LAST + 1):
        plane_all(sel, xin, p_send, p_recv, hop).wait_send()
        plane_all(yout, zin, y_send, y_recv, hop).wait_send()


def solution(mesh):
    sp_count = mesh.shape["sp"]
    tp_count = mesh.shape["tp"]

    def on_device(
        queries,
        key_heads,
        value_heads,
        sink_logit,
        out_weight,
        residual,
        norm_gain,
        expert_ids,
        route_weights,
        gate_weight,
        up_weight,
        down_weight,
    ):
        T, D = residual.shape
        HD = key_heads.shape[2]
        HEADS = queries.shape[1] // HD
        FF = gate_weight.shape[2]
        Z = sp_count // CORES
        PL = tp_count * CORES
        top_k = expert_ids.shape[1]
        CAP = max(2, 2 * top_k * T // (sp_count * tp_count))
        GR = 2 * CAP
        HOP = Z // 2
        keys_t = jnp.transpose(key_heads, (1, 2, 0)).reshape(HD, -1)
        values_t = jnp.transpose(value_heads, (1, 2, 0)).reshape(HD, -1)
        dma = pltpu.SemaphoreType.DMA
        vm = pltpu.VMEM
        any_space = pl.BlockSpec(memory_space=pl.ANY)
        in_vmem = pl.BlockSpec(memory_space=pltpu.VMEM)
        dims = (T, D, Z, tp_count, sp_count, CAP, HEADS, HD)
        quarters = T // (PL * CAP)
        prefix = prefix_rows((HOP, HOP - 1), T, PL * CAP)
        pieces = sum(prefix(way, hop) // PIECE for way in range(2) for hop in range(1, HOP + 1))
        return pl.pallas_call(
            functools.partial(layer, dims),
            out_shape=jax.ShapeDtypeStruct((T, D), BF),
            in_specs=[any_space] * 12,
            out_specs=in_vmem,
            scratch_shapes=[
                vm(queries.shape, BF),
                vm((tp_count + 1, 2 * HD, T), BF),
                vm(out_weight.shape, BF),
                vm((D, FF), BF),
                vm((D, FF), BF),
                vm((FF, D), BF),
                vm((1, HEADS), F32),
                vm((T, D), BF),
                vm((1, D), F32),
                vm((tp_count, top_k, T), jnp.int32),
                vm((top_k, T), F32),
                vm((tp_count, T, HEADS * HD), BF),
                vm((tp_count, T, HEADS * HD), BF),
                vm((2, T, D // 2), BF),
                vm((2, T, D // 2), BF),
                vm((2, T, D // 2), BF),
                vm((2, T, D // 2), BF),
                vm((2, T, D // 2), BF),
                vm((2, T, D // 2), BF),
                vm((T, D), F32),
                vm((T, D), BF),
                vm((T, D), BF),
                vm((T, D), BF),
                vm((HOP, 2, T, D), BF),
                vm((HOP, 2, 2 * Z, T), BF),
                vm((HOP, 8, T), F32),
                vm((3, T, T), BF),
                vm((2, T, T), BF),
                vm((HOP, PL, GR, D), BF),
                vm((HOP, PL, GR, D), BF),
                vm((HOP, PL, GR, D), BF),
                vm((HOP, PL, GR, D), BF),
                vm((HOP + 1, 2, T, D), BF),
                vm((2, T, D), F32),
                dma((10,)),
                dma((2 * tp_count,)),
                dma((2,)),
                dma((tp_count,)),
                dma((tp_count,)),
                dma((3,)),
                dma((6 * quarters,)),
                dma((2 * HOP,)),
                dma((pieces,)),
                dma((2 * HOP,)),
                dma((2 * HOP,)),
                dma((HOP,)),
                dma((HOP,)),
                dma((HOP,)),
                dma((HOP,)),
                dma((2 * HOP,)),
                dma((pieces,)),
            ],
            compiler_params=pltpu.CompilerParams(
                collective_id=0, has_side_effects=True, vmem_limit_bytes=62 * 1024 * 1024
            ),
        )(
            queries,
            keys_t,
            values_t,
            sink_logit.reshape(1, HEADS),
            out_weight,
            residual,
            norm_gain.reshape(1, D),
            expert_ids.T,
            route_weights.T,
            gate_weight,
            up_weight,
            down_weight,
        )

    return jax.shard_map(
        on_device,
        mesh=mesh,
        in_specs=(
            P(("grp", "sp"), "tp"),
            P(("grp", "sp"), "tp", None),
            P(("grp", "sp"), "tp", None),
            P("tp"),
            P("tp", None),
            P(("grp", "sp", "tp"), None),
            P(),
            P(("grp", "sp", "tp"), None),
            P(("grp", "sp", "tp"), None),
            P(("sp", "tp"), None, None),
            P(("sp", "tp"), None, None),
            P(("sp", "tp"), None, None),
        ),
        out_specs=P(("grp", "sp", "tp"), None),
        check_vma=False,
    )
```

```python
import functools

import jax
import jax.numpy as jnp
from jax import lax
from jax.experimental import pallas as pl
from jax.experimental.pallas import tpu as pltpu
from jax.sharding import PartitionSpec as P

MESH = pl.DeviceIdType.MESH
BF = jnp.bfloat16
F32 = jnp.float32
CORES = 2
WINDOW = 128
EPS = 1e-06


def mm(a, b):
    return jnp.dot(a, b, preferred_element_type=F32)


def mm_nt(a, b):
    return lax.dot_general(a, b, (((1,), (1,)), ((), ())), preferred_element_type=F32)


def mm_tn(a, b):
    return lax.dot_general(a, b, (((0,), (0,)), ((), ())), preferred_element_type=F32)


def iota(shape, dim):
    return lax.broadcasted_iota(jnp.int32, shape, dim)


PIECE = 16


def prefix_rows(hops, rows, share):
    def prefix(way, hop):
        return min(rows, share * (hops[way] - hop + 1)) if hop <= hops[way] else 0

    return prefix


def ring_order(prefix, order, ready, waiting, latency=3.0):
    queue, left, now, clock = ([], []), [0.0, 0.0], [None, None], 0.0
    own = [list(order), list(order)]
    coming, events = [], []
    while True:
        for way in range(2):
            while (
                own[way]
                and ready[own[way][0]] <= clock + 1e-6
                and len(queue[way]) + (now[way] is not None) <= waiting[own[way][0]]
            ):
                piece = own[way].pop(0)
                queue[way].append((piece, 1))
                events.append((clock, "own", way, piece, 1))
            if now[way] is None and queue[way]:
                now[way], left[way] = queue[way].pop(0), 1.0
        busy = [way for way in range(2) if now[way] is not None]
        steps = [clock + left[way] * len(busy) for way in busy]
        steps += [item[0] for item in coming]
        steps += [ready[own[way][0]] for way in range(2) if own[way] and ready[own[way][0]] > clock]
        if not steps:
            return events
        later = min(steps)
        for way in busy:
            left[way] -= (later - clock) / len(busy)
        clock = later
        for way in busy:
            if left[way] < 1e-6:
                coming.append((clock + latency, way) + now[way])
                now[way] = None
        coming.sort()
        while coming and coming[0][0] <= clock + 1e-6:
            _, way, piece, hop = coming.pop(0)
            events.append((clock, "pass", way, piece, hop))
            if piece * PIECE < prefix(way, hop + 1):
                queue[way].append((piece, hop + 1))


def layer(
    dims,
    q_hbm,
    kt_hbm,
    vt_hbm,
    sink_hbm,
    wo_hbm,
    res_hbm,
    gain_hbm,
    ids_hbm,
    rw_hbm,
    wg_hbm,
    wu_hbm,
    wd_hbm,
    out_ref,
    qv,
    kv,
    wo,
    wg,
    wu,
    wd,
    sink_ref,
    res_ref,
    gain_ref,
    ids_ref,
    rw_ref,
    att,
    att_c,
    s2,
    r2,
    sp,
    sm,
    rp,
    rm,
    acc,
    stream,
    normed,
    own_a,
    ring,
    meta,
    table,
    place,
    sorter,
    sel,
    xin,
    yout,
    zin,
    ret,
    cbuf,
    load_sem,
    kv_sem,
    halo_sem,
    ids_send,
    ids_recv,
    rs_send,
    rs_recv,
    d_send,
    d_recv,
    m_send,
    m_recv,
    p_send,
    p_recv,
    y_send,
    y_recv,
    b_send,
    b_recv,
):
    T, D, Z, TP, SP, CAP, HEADS, HD = dims
    LAST = Z // 2
    PL = TP * CORES
    CH = PL * CAP
    HALF = D // 2
    HOPS = (Z // 2, Z // 2 - 1)
    GR = 2 * CAP
    SEL = PL * GR

    s = lax.axis_index("sp")
    x = lax.axis_index("tp")
    z = lax.div(s, CORES)
    c = lax.rem(s, CORES)
    me = c * TP + x
    step_a = 1 - 2 * c + Z
    z_next = (lax.rem(z + step_a, Z), lax.rem(z + 2 * Z - step_a, Z))

    def chip(zz):
        return {"sp": zz * CORES + c, "tp": x}

    ahead = (chip(z_next[0]), chip(z_next[1]))
    behind = (ahead[1], ahead[0])

    def to_x(k):
        return {"sp": s, "tp": lax.rem(x + k + TP, TP)}

    def peer(k):
        cc = lax.rem(c + k // TP, CORES)
        return {"sp": z * CORES + cc, "tp": lax.rem(x + k % TP, TP)}

    def peer_rank(k):
        return lax.rem(c + k // TP, CORES) * TP + lax.rem(x + k % TP, TP)

    def from_rank(k):
        return lax.rem(c + CORES - k // TP, CORES) * TP + lax.rem(x + TP - k % TP, TP)

    s_after = {"sp": lax.rem(s + 1, SP), "tp": x}
    s_before = {"sp": lax.rem(s + SP - 1, SP), "tp": x}

    small = [
        pltpu.make_async_copy(src, dst, load_sem.at[i])
        for i, (src, dst) in enumerate(
            (
                (q_hbm, qv),
                (sink_hbm, sink_ref),
                (ids_hbm, ids_ref.at[0]),
                (rw_hbm, rw_ref),
            )
        )
    ]
    wo_load = pltpu.make_async_copy(wo_hbm, wo, load_sem.at[4])
    large = [
        pltpu.make_async_copy(src, dst, load_sem.at[5 + i])
        for i, (src, dst) in enumerate(
            (
                (res_hbm, res_ref),
                (gain_hbm, gain_ref),
                (wg_hbm.at[0], wg),
                (wu_hbm.at[0], wu),
                (wd_hbm.at[0], wd),
            )
        )
    ]
    kv_loads = []
    for b in range(TP):
        cols = pl.ds(b * T, T)
        for i, src in enumerate((kt_hbm, vt_hbm)):
            kv_loads.append(
                pltpu.make_async_copy(
                    src.at[:, cols], kv.at[b + 1, pl.ds(i * HD, HD)], kv_sem.at[2 * b + i]
                )
            )
    barrier = pltpu.get_barrier_semaphore()
    greeted = [ahead[0], ahead[1], s_after, s_before] + [peer(k) for k in range(1, PL)]
    for device in greeted:
        pl.semaphore_signal(barrier, inc=1, device_id=device, device_id_type=MESH)
    for copy in kv_loads + small + [wo_load]:
        copy.start()

    halo = pltpu.make_async_remote_copy(
        src_ref=kv.at[TP],
        dst_ref=kv.at[0],
        send_sem=halo_sem.at[0],
        recv_sem=halo_sem.at[1],
        device_id=s_after,
        device_id_type=MESH,
    )

    row_i = iota((T, 2 * T), 0)
    col_j = iota((T, 2 * T), 1)

    def attend(b, slot):
        first = jnp.where(s * TP + b == 0, T, 0)
        allowed = (col_j > row_i) & (col_j <= row_i + T) & (col_j >= first)
        rows = pl.ds(pl.multiple_of(b * T, T), T)
        low = kv[b].astype(F32)
        high = kv[b + 1].astype(F32)
        both = jnp.concatenate([low, high], axis=1)
        kt, vt = both[:HD], both[HD:]
        none = jnp.zeros((HD, 2 * T), F32)
        keys = (jnp.concatenate([kt, none], 0).astype(BF), jnp.concatenate([none, kt], 0).astype(BF))
        values = (jnp.concatenate([vt, none], 0).astype(BF), jnp.concatenate([none, vt], 0).astype(BF))
        for pair in range(HEADS // 2):
            lanes = pl.ds(pair * 2 * HD, 2 * HD)
            query = qv[rows, lanes]
            total = None
            for side in range(2):
                head = pair * 2 + side
                sink = sink_ref[0, head]
                score = mm(query, keys[side]) * (HD ** (-0.5))
                score = jnp.where(allowed, score, -jnp.inf)
                top = jnp.maximum(jnp.max(score, axis=1, keepdims=True), sink)
                grown = jnp.exp(score - top)
                weight = jnp.sum(grown, axis=1, keepdims=True) + jnp.exp(sink - top)
                mixed = mm_nt(grown.astype(BF), values[side]) / weight
                total = mixed if total is None else total + mixed
            att[slot, :, lanes] = total.astype(BF)

    E = Z * PL
    plane_bits = PL.bit_length() - 1
    e_sub = iota((E, T), 0)
    t_sub = iota((T, T), 0)
    t_col = iota((T, T), 1)
    rel = (lax.shift_right_logical(e_sub, plane_bits) - z) * (1 - 2 * c) + 2 * Z
    rel = rel & (Z - 1)
    is_a = (rel >= 1) & (rel <= HOPS[0])
    dist = (
        jnp.where(is_a, rel, 0).astype(F32),
        jnp.where(rel > HOPS[0], Z - rel, 0).astype(F32),
    )

    def rank_of(key):
        along = jnp.broadcast_to(key, (T, T))
        down = along.T
        ahead_of = (down > along) | ((down == along) & (t_sub < t_col))
        return jnp.sum(jnp.where(ahead_of, 1.0, 0.0), axis=0, keepdims=True)

    def orders(slot):
        took = [
            jnp.where(e_sub == ids_ref[slot, k : k + 1, :], 1.0, 0.0).astype(F32) for k in range(2)
        ]
        both = took[0] + took[1]
        ways = [rank_of(jnp.max(both * d, axis=0, keepdims=True)) for d in dist]
        return took, ways, rank_of(-jnp.minimum(ways[0], ways[1]))

    def placing(position):
        return jnp.where(position == t_sub.astype(F32), 1.0, 0.0).astype(BF)

    right, left = to_x(1), to_x(-1)
    QUARTERS = T // CH

    def rs_copy(kind, q):
        src, dst, half, device, group = (
            (s2, r2, 0, right, 0),
            (s2, r2, 1, left, 0),
            (sp, rp, 1, right, 1),
            (sm, rm, 0, left, 2),
            (sp, rp, 0, right, 1),
            (sm, rm, 1, left, 2),
        )[kind]
        rows = pl.ds(q * CH, CH)
        return pltpu.make_async_remote_copy(
            src_ref=src.at[half, rows],
            dst_ref=dst.at[half, rows],
            send_sem=rs_send.at[group],
            recv_sem=rs_recv.at[kind * QUARTERS + q],
            device_id=device,
            device_id_type=MESH,
        )

    def first_leg(q):
        rs_copy(0, q).start()
        rs_copy(1, q).start()

    def alone(q):
        rs_copy(2, q).start()
        rs_copy(3, q).start()

    def joined(q):
        rows = pl.ds(q * CH, CH)
        for kind, dst, half in ((0, sp, 0), (1, sm, 1)):
            rs_copy(kind, q).wait_recv()
            total = cbuf[half, rows, pl.ds(0, HALF)] + r2[half, rows].astype(F32)
            dst[half, rows] = total.astype(BF)
            rs_copy(4 + kind, q).start()

    def project(slot, half):
        return mm(att_c[slot], wo[:, pl.ds(half * HALF, HALF)])

    def ids_copy(m):
        return pltpu.make_async_remote_copy(
            src_ref=ids_ref.at[0],
            dst_ref=ids_ref.at[m],
            send_sem=ids_send.at[m],
            recv_sem=ids_recv.at[m],
            device_id=to_x(-m),
            device_id_type=MESH,
        )

    for copy in kv_loads + small:
        copy.wait()
    attend(1, 1)
    pl.semaphore_wait(barrier, len(greeted))
    halo.start()
    for m in range(1, TP):
        ids_copy(m).start()
    for copy in large:
        copy.start()
    for b in range(2, TP):
        attend(b, b)
    took, positions, position_c = orders(0)
    place[0] = placing(positions[0])
    place[1] = placing(positions[1])
    place[2] = placing(position_c)
    halo.wait_recv()
    attend(0, 0)
    for m in range(1, TP):
        ids_copy(m).wait_recv()

    def arrange(m, placed):
        att_c[m] = mm(placed, att[lax.rem(x + m, TP)]).astype(BF)

    far, after, prior = 2, 1, TP - 1
    arrange(far, placing(orders(far)[2]))
    wo_load.wait()
    for half in range(2):
        s2[half] = project(far, half).astype(BF)
        rs_copy(half, 0).start()
    for m in (after, prior):
        arrange(m, placing(orders(m)[2]))
    sp[1] = project(after, 1).astype(BF)
    sm[0] = project(prior, 0).astype(BF)
    alone(0)
    first_leg(1)
    first_leg(2)
    cbuf[0, :, pl.ds(0, HALF)] = project(after, 0)
    cbuf[1, :, pl.ds(0, HALF)] = project(prior, 1)
    joined(0)
    alone(1)
    first_leg(3)
    large[0].wait()
    large[1].wait()
    arrange(0, place[2])
    for half in range(2):
        cols = pl.ds(half * HALF, HALF)
        acc[:, cols] = project(0, half) + mm(place[2], res_ref[:, cols])
    joined(1)
    alone(2)

    t_lane = iota((E, T), 1)
    either = took[0] + took[1]
    before = jnp.where(t_sub < t_col, 1.0, 0.0).astype(BF)
    rank = mm(either.astype(BF), before)
    weight_a = rw_ref[0:1, :]
    weight_b = rw_ref[1:2, :]
    whole = weight_a + weight_b
    share = took[0] * (weight_a / whole) + took[1] * (weight_b / whole)
    slot_value = jnp.where(is_a, positions[0] + 1.0, positions[1] + (1.0 + T))
    base = (e_sub & (PL - 1)) * GR + jnp.where(is_a, 0, CAP)
    spread_t = jnp.zeros((E, T), F32)
    spread_w = jnp.zeros((E, T), F32)
    for r in range(CAP):
        here = either * jnp.where(rank == float(r), 1.0, 0.0)
        value_col = jnp.sum(here * slot_value, axis=1, keepdims=True)
        share_col = jnp.sum(here * share, axis=1, keepdims=True)
        hit = t_lane == base + r
        spread_t = spread_t + jnp.where(hit, value_col, 0.0)
        spread_w = spread_w + jnp.where(hit, share_col, 0.0)
    plane_of = jnp.where(
        lax.shift_right_logical(iota((Z, E), 1), plane_bits) == iota((Z, E), 0), 1.0, 0.0
    ).astype(BF)
    OWN = HOPS[0] - 1
    meta[OWN, 1, pl.ds(0, Z)] = mm(plane_of, spread_t.astype(BF)).astype(BF)
    meta[OWN, 1, pl.ds(Z, Z)] = mm(plane_of, spread_w.astype(BF)).astype(BF)
    for way in range(2):
        sorter[way] = mm_nt(place[way], place[2]).astype(BF)
    normed[...] = jnp.zeros((T, D), BF)

    prefix = prefix_rows(HOPS, T, CH)
    for way in range(2):
        for hop in range(1, HOPS[way] + 1):
            n = prefix(way, hop)
            if n < T:
                ring[hop - 1, way, pl.ds(n, T - n)] = jnp.zeros((T - n, D), BF)
    joined(2)
    alone(3)

    def prepare(q):
        for kind in range(2, 6):
            rs_copy(kind, q).wait_recv()
        rows = pl.ds(q * CH, CH)
        square = jnp.zeros((CH, 1), F32)
        for half in range(2):
            cols = pl.ds(half * HALF, HALF)
            total = acc[rows, cols] + rp[half, rows].astype(F32) + rm[half, rows].astype(F32)
            kept = total.astype(BF)
            stream[rows, cols] = kept
            wide = kept.astype(F32)
            square = square + jnp.sum(wide * wide, axis=1, keepdims=True)
        scale = lax.rsqrt(square * (1.0 / D) + EPS)
        for half in range(2):
            cols = pl.ds(half * HALF, HALF)
            wide = stream[rows, cols].astype(F32)
            normed[rows, cols] = (wide * scale * gain_ref[:, cols]).astype(BF)
        count = PIECE if q < QUARTERS - 1 else T - q * PIECE
        rows = pl.ds(q * PIECE, count)
        own_a[rows] = mm(sorter[0, rows], normed[...]).astype(BF)
        ring[OWN, 1, rows] = mm(sorter[1, rows], normed[...]).astype(BF)

    first_index, pieces = {}, 0
    for way in range(2):
        for hop in range(1, HOPS[way] + 1):
            first_index[way, hop] = pieces
            pieces += prefix(way, hop) // PIECE

    def d_index(way, hop, j):
        return first_index[way, hop] + j

    def hop_index(way, hop):
        return way * HOPS[0] + hop - 1

    def packet_copy(way, hop, j):
        rows = pl.ds(j * PIECE, PIECE)
        if hop == 1:
            src = own_a.at[rows] if way == 0 else ring.at[OWN, 1, rows]
        else:
            src = ring.at[hop - 2, way, rows]
        index = d_index(way, hop, j)
        return pltpu.make_async_remote_copy(
            src_ref=src,
            dst_ref=ring.at[hop - 1, way, rows],
            send_sem=d_send.at[hop_index(way, hop)],
            recv_sem=d_recv.at[index],
            device_id=ahead[way],
            device_id_type=MESH,
        )

    def meta_copy(way, hop):
        src = meta.at[OWN, 1] if hop == 1 else meta.at[hop - 2, way]
        index = hop_index(way, hop)
        return pltpu.make_async_remote_copy(
            src_ref=src,
            dst_ref=meta.at[hop - 1, way],
            send_sem=m_send.at[index],
            recv_sem=m_recv.at[index],
            device_id=ahead[way],
            device_id_type=MESH,
        )

    for way in range(2):
        meta_copy(way, 1).start()
    prepare(0)
    for way in range(2):
        packet_copy(way, 1, 0).start()
    joined(QUARTERS - 1)

    def hop_table(hop):
        picked_t = jnp.zeros((1, T), F32)
        picked_w = jnp.zeros((1, T), F32)
        mine = iota((Z, T), 0) == z
        for way in range(2):
            known = meta[hop - 1, way].astype(F32)
            picked_t = picked_t + jnp.sum(jnp.where(mine, known[:Z], 0.0), axis=0, keepdims=True)
            picked_w = picked_w + jnp.sum(jnp.where(mine, known[Z:], 0.0), axis=0, keepdims=True)
        table[hop - 1, 0:1] = picked_t
        table[hop - 1, 1:2] = picked_w

    def plane_copy(buffer_from, buffer_to, sends, recvs, hop, k):
        return pltpu.make_async_remote_copy(
            src_ref=buffer_from.at[hop - 1, peer_rank(k)],
            dst_ref=buffer_to.at[hop - 1, me],
            send_sem=sends.at[hop - 1],
            recv_sem=recvs.at[hop - 1],
            device_id=peer(k),
            device_id_type=MESH,
        )

    def plane_all(buffer_from, buffer_to, sends, recvs, hop):
        blocks = pl.ds(0, PL - 1)
        return pltpu.make_async_remote_copy(
            src_ref=buffer_from.at[hop - 1, blocks],
            dst_ref=buffer_to.at[hop - 1, blocks],
            send_sem=sends.at[hop - 1],
            recv_sem=recvs.at[hop - 1],
            device_id=peer(1),
            device_id_type=MESH,
        )

    COLS = 512

    def select(hop):
        hop_table(hop)
        spot = (iota((2 * T, SEL), 0) + 1).astype(F32)
        hot = jnp.where(spot == table[hop - 1, 0:1, 0:SEL], 1.0, 0.0).astype(BF)
        for n in range(D // COLS):
            cols = pl.ds(n * COLS, COLS)
            rows = ring[hop - 1, :, :, cols].reshape(2 * T, COLS)
            sel[hop - 1, :, :, cols] = mm_tn(hot, rows).reshape(PL, GR, COLS).astype(BF)
        for k in range(1, PL):
            plane_copy(sel, xin, p_send, p_recv, hop, k).start()
        xin[hop - 1, me] = sel[hop - 1, me]

    def experts(*hops):
        for hop in hops:
            plane_all(sel, xin, p_send, p_recv, hop).wait_recv()
        rows = jnp.concatenate(
            [xin[hop - 1].astype(F32).reshape(SEL, D).astype(BF) for hop in hops], axis=0
        )
        gate = mm(rows, wg[...])
        upward = mm(rows, wu[...])
        hidden = (gate / (1.0 + jnp.exp(-gate)) * upward).astype(BF)
        for n in range(D // COLS):
            cols = pl.ds(n * COLS, COLS)
            product = mm(hidden, wd[:, cols])
            for i, hop in enumerate(hops):
                part = product[i * SEL : (i + 1) * SEL]
                yout[hop - 1, :, :, cols] = part.reshape(PL, GR, COLS).astype(BF)
        for hop in hops:
            for k in range(1, PL):
                plane_copy(yout, zin, y_send, y_recv, hop, k).start()
            zin[hop - 1, me] = yout[hop - 1, me]

    def back_copy(way, hop, j):
        rows = pl.ds(j * PIECE, PIECE)
        index = d_index(way, hop, j)
        return pltpu.make_async_remote_copy(
            src_ref=ret.at[hop, way, rows],
            dst_ref=ret.at[hop - 1, way, rows],
            send_sem=b_send.at[hop_index(way, hop)],
            recv_sem=b_recv.at[index],
            device_id=behind[way],
            device_id_type=MESH,
        )

    def weighted(hop, ways):
        plane_all(yout, zin, y_send, y_recv, hop).wait_recv()
        mixes = []
        for way, n in ways:
            spot = (iota((n, SEL), 0) + (way * T + 1)).astype(F32)
            hit = spot == table[hop - 1, 0:1, 0:SEL]
            mixes.append(jnp.where(hit, table[hop - 1, 1:2, 0:SEL], 0.0).astype(BF))
        for n in range(D // COLS):
            cols = pl.ds(n * COLS, COLS)
            rows = zin[hop - 1, :, :, cols].astype(F32).reshape(SEL, COLS).astype(BF)
            for (way, count), mix in zip(ways, mixes):
                cbuf[way, pl.ds(0, count), cols] = mm(mix, rows)

    def send_back(hop):
        if hop == LAST:
            weighted(hop, [(0, prefix(0, hop)), (1, T)])
            acc[...] = cbuf[1]
        else:
            weighted(hop, [(way, prefix(way, hop)) for way in range(2)])
        for i in range(T // PIECE):
            for way in range(2):
                j = prefix(way, hop) // PIECE - 1 - i
                if j < 0:
                    continue
                rows = pl.ds(j * PIECE, PIECE)
                part = cbuf[way, rows]
                if j * PIECE < prefix(way, hop + 1):
                    back_copy(way, hop + 1, j).wait_recv()
                    part = part + ret[hop, way, rows].astype(F32)
                ret[hop, way, rows] = part.astype(BF)
                back_copy(way, hop, j).start()

    def pass_on(way, hop, j):
        if j * PIECE < prefix(way, hop):
            packet_copy(way, hop, j).wait_recv()
        if j * PIECE < prefix(way, hop + 1):
            packet_copy(way, hop + 1, j).start()

    for copy in large[2:]:
        copy.wait()
    def meta_on(way, hop):
        meta_copy(way, hop).wait_recv()
        if hop < HOPS[way]:
            meta_copy(way, hop + 1).start()

    last_quarter = T // PIECE - QUARTERS + 1
    ready = [0.0, 5.8, 9.6] + [13.5] * last_quarter
    events = ring_order(prefix, (0, 1, 2, 4, 5, 3, 6, 7), ready, (3, 3, 3, 3, 3, 3, 2, 2))
    prepared = 1
    missing = {
        hop: sum(prefix(way, hop) // PIECE for way in range(2)) for hop in range(1, LAST + 1)
    }
    groups = [(LAST, LAST - 1), (LAST - 2,)]
    later = []
    seen = set()
    for when, action, way, piece, hop in events:
        while later and later[0][0] <= when:
            experts(*later.pop(0)[1])
        if action == "own":
            while prepared <= min(piece, QUARTERS - 1):
                prepare(prepared)
                prepared += 1
            if piece > 0:
                packet_copy(way, 1, piece).start()
            continue
        if (way, hop) not in seen:
            seen.add((way, hop))
            meta_on(way, hop)
        pass_on(way, hop, piece)
        missing[hop] -= 1
        if missing[hop] == 0:
            select(hop)
            for group in groups:
                if hop in group and not any(missing[h] for h in group):
                    later.append((when + 12.0, group))
    for _, group in later:
        experts(*group)
    send_back(LAST)
    send_back(LAST - 1)
    experts(LAST - 3)
    send_back(LAST - 2)
    experts(1, 2)
    experts(3, 4)
    for hop in range(LAST - 3, 0, -1):
        send_back(hop)

    for j in range(T // PIECE):
        rows = pl.ds(j * PIECE, PIECE)
        for way in range(2):
            back_copy(way, 1, j).wait_recv()
        ret[0, 1, rows] = (ret[0, 1, rows].astype(F32) + acc[rows]).astype(BF)
    unsort = place[pl.ds(0, 2)].reshape(2 * T, T)
    for n in range(D // COLS):
        cols = pl.ds(n * COLS, COLS)
        came = ret[0, :, :, cols].reshape(2 * T, COLS)
        out_ref[:, cols] = (mm_tn(place[2], stream[:, cols]) + mm_tn(unsort, came)).astype(BF)

    halo.wait_send()
    for m in range(1, TP):
        ids_copy(m).wait_send()
    for group, (src, dst) in enumerate(((s2, r2), (sp, rp), (sm, rm))):
        pltpu.make_async_remote_copy(
            src_ref=src,
            dst_ref=dst,
            send_sem=rs_send.at[group],
            recv_sem=rs_recv.at[0],
            device_id=right,
            device_id_type=MESH,
        ).wait_send()
    for way in range(2):
        for hop in range(1, HOPS[way] + 1):
            meta_copy(way, hop).wait_send()
            rows = pl.ds(0, prefix(way, hop))
            for buffer, sems, recvs in ((ring, d_send, d_recv), (ret, b_send, b_recv)):
                pltpu.make_async_remote_copy(
                    src_ref=buffer.at[hop - 1, way, rows],
                    dst_ref=buffer.at[hop - 1, way, rows],
                    send_sem=sems.at[hop_index(way, hop)],
                    recv_sem=recvs.at[0],
                    device_id=ahead[way],
                    device_id_type=MESH,
                ).wait_send()
    for hop in range(1, LAST + 1):
        plane_all(sel, xin, p_send, p_recv, hop).wait_send()
        plane_all(yout, zin, y_send, y_recv, hop).wait_send()


def solution(mesh):
    sp_count = mesh.shape["sp"]
    tp_count = mesh.shape["tp"]

    def on_device(
        queries,
        key_heads,
        value_heads,
        sink_logit,
        out_weight,
        residual,
        norm_gain,
        expert_ids,
        route_weights,
        gate_weight,
        up_weight,
        down_weight,
    ):
        T, D = residual.shape
        HD = key_heads.shape[2]
        HEADS = queries.shape[1] // HD
        FF = gate_weight.shape[2]
        Z = sp_count // CORES
        PL = tp_count * CORES
        top_k = expert_ids.shape[1]
        CAP = max(2, 2 * top_k * T // (sp_count * tp_count))
        GR = 2 * CAP
        HOP = Z // 2
        keys_t = jnp.transpose(key_heads, (1, 2, 0)).reshape(HD, -1)
        values_t = jnp.transpose(value_heads, (1, 2, 0)).reshape(HD, -1)
        dma = pltpu.SemaphoreType.DMA
        vm = pltpu.VMEM
        any_space = pl.BlockSpec(memory_space=pl.ANY)
        in_vmem = pl.BlockSpec(memory_space=pltpu.VMEM)
        dims = (T, D, Z, tp_count, sp_count, CAP, HEADS, HD)
        quarters = T // (PL * CAP)
        prefix = prefix_rows((HOP, HOP - 1), T, PL * CAP)
        pieces = sum(prefix(way, hop) // PIECE for way in range(2) for hop in range(1, HOP + 1))
        return pl.pallas_call(
            functools.partial(layer, dims),
            out_shape=jax.ShapeDtypeStruct((T, D), BF),
            in_specs=[any_space] * 12,
            out_specs=in_vmem,
            scratch_shapes=[
                vm(queries.shape, BF),
                vm((tp_count + 1, 2 * HD, T), BF),
                vm(out_weight.shape, BF),
                vm((D, FF), BF),
                vm((D, FF), BF),
                vm((FF, D), BF),
                pltpu.SMEM((1, HEADS), F32),
                vm((T, D), BF),
                vm((1, D), F32),
                vm((tp_count, top_k, T), jnp.int32),
                vm((top_k, T), F32),
                vm((tp_count, T, HEADS * HD), BF),
                vm((tp_count, T, HEADS * HD), BF),
                vm((2, T, D // 2), BF),
                vm((2, T, D // 2), BF),
                vm((2, T, D // 2), BF),
                vm((2, T, D // 2), BF),
                vm((2, T, D // 2), BF),
                vm((2, T, D // 2), BF),
                vm((T, D), F32),
                vm((T, D), BF),
                vm((T, D), BF),
                vm((T, D), BF),
                vm((HOP, 2, T, D), BF),
                vm((HOP, 2, 2 * Z, T), BF),
                vm((HOP, 8, T), F32),
                vm((3, T, T), BF),
                vm((2, T, T), BF),
                vm((HOP, PL, GR, D), BF),
                vm((HOP, PL, GR, D), BF),
                vm((HOP, PL, GR, D), BF),
                vm((HOP, PL, GR, D), BF),
                vm((HOP + 1, 2, T, D), BF),
                vm((2, T, D), F32),
                dma((10,)),
                dma((2 * tp_count,)),
                dma((2,)),
                dma((tp_count,)),
                dma((tp_count,)),
                dma((3,)),
                dma((6 * quarters,)),
                dma((2 * HOP,)),
                dma((pieces,)),
                dma((2 * HOP,)),
                dma((2 * HOP,)),
                dma((HOP,)),
                dma((HOP,)),
                dma((HOP,)),
                dma((HOP,)),
                dma((2 * HOP,)),
                dma((pieces,)),
            ],
            compiler_params=pltpu.CompilerParams(
                collective_id=0, has_side_effects=True, vmem_limit_bytes=62 * 1024 * 1024
            ),
        )(
            queries,
            keys_t,
            values_t,
            sink_logit.reshape(1, HEADS),
            out_weight,
            residual,
            norm_gain.reshape(1, D),
            expert_ids.T,
            route_weights.T,
            gate_weight,
            up_weight,
            down_weight,
        )

    return jax.shard_map(
        on_device,
        mesh=mesh,
        in_specs=(
            P(("grp", "sp"), "tp"),
            P(("grp", "sp"), "tp", None),
            P(("grp", "sp"), "tp", None),
            P("tp"),
            P("tp", None),
            P(("grp", "sp", "tp"), None),
            P(),
            P(("grp", "sp", "tp"), None),
            P(("grp", "sp", "tp"), None),
            P(("sp", "tp"), None, None),
            P(("sp", "tp"), None, None),
            P(("sp", "tp"), None, None),
        ),
        out_specs=P(("grp", "sp", "tp"), None),
        check_vma=False,
    )
```

```python
import functools

import jax
import jax.numpy as jnp
from jax import lax
from jax.experimental import pallas as pl
from jax.experimental.pallas import tpu as pltpu
from jax.sharding import PartitionSpec as P

MESH = pl.DeviceIdType.MESH
BF = jnp.bfloat16
F32 = jnp.float32
CORES = 2
WINDOW = 128
EPS = 1e-06


def mm(a, b):
    return jnp.dot(a, b, preferred_element_type=F32)


def mm_nt(a, b):
    return lax.dot_general(a, b, (((1,), (1,)), ((), ())), preferred_element_type=F32)


def mm_tn(a, b):
    return lax.dot_general(a, b, (((0,), (0,)), ((), ())), preferred_element_type=F32)


def iota(shape, dim):
    return lax.broadcasted_iota(jnp.int32, shape, dim)


PIECE = 16
ORDER = (0, 1, 2, 3, 4, 5, 6, 7)
WAITING = (1, 1, 1, 1, 1, 1, 1, 1)
READY = (0.0, 5.8, 9.6, 13.5)
LATENCY = 3.9
EARLY = ((8, 7),)
TAIL = 0
PEERS = (1, 2, 3, 4, 5, 6, 7)


def prefix_rows(hops, rows, share):
    def prefix(way, hop):
        return min(rows, share * (hops[way] - hop + 1)) if hop <= hops[way] else 0

    return prefix


def ring_order(prefix, order, ready, waiting, latency=3.0):
    queue, left, now, clock = ([], []), [0.0, 0.0], [None, None], 0.0
    own = [list(order), list(order)]
    coming, events = [], []
    while True:
        for way in range(2):
            while (
                own[way]
                and ready[own[way][0]] <= clock + 1e-6
                and len(queue[way]) + (now[way] is not None) <= waiting[own[way][0]]
            ):
                piece = own[way].pop(0)
                queue[way].append((piece, 1))
                events.append((clock, "own", way, piece, 1))
            if now[way] is None and queue[way]:
                now[way], left[way] = queue[way].pop(0), 1.0
        busy = [way for way in range(2) if now[way] is not None]
        steps = [clock + left[way] * len(busy) for way in busy]
        steps += [item[0] for item in coming]
        steps += [ready[own[way][0]] for way in range(2) if own[way] and ready[own[way][0]] > clock]
        if not steps:
            return events
        later = min(steps)
        for way in busy:
            left[way] -= (later - clock) / len(busy)
        clock = later
        for way in busy:
            if left[way] < 1e-6:
                coming.append((clock + latency, way) + now[way])
                now[way] = None
        coming.sort()
        while coming and coming[0][0] <= clock + 1e-6:
            _, way, piece, hop = coming.pop(0)
            events.append((clock, "pass", way, piece, hop))
            if piece * PIECE < prefix(way, hop + 1):
                queue[way].append((piece, hop + 1))


def layer(
    dims,
    q_hbm,
    kt_hbm,
    vt_hbm,
    sink_hbm,
    wo_hbm,
    res_hbm,
    gain_hbm,
    ids_hbm,
    rw_hbm,
    wg_hbm,
    wu_hbm,
    wd_hbm,
    out_ref,
    qv,
    kv,
    wo,
    wg,
    wu,
    wd,
    sink_ref,
    res_ref,
    gain_ref,
    ids_ref,
    rw_ref,
    att,
    att_c,
    s2,
    r2,
    sp,
    sm,
    rp,
    rm,
    acc,
    stream,
    normed,
    own_a,
    ring,
    meta,
    table,
    place,
    sorter,
    sel,
    xin,
    yout,
    zin,
    ret,
    cbuf,
    load_sem,
    kv_sem,
    halo_sem,
    ids_send,
    ids_recv,
    rs_send,
    rs_recv,
    d_send,
    d_recv,
    m_send,
    m_recv,
    p_send,
    p_recv,
    y_send,
    y_recv,
    b_send,
    b_recv,
):
    T, D, Z, TP, SP, CAP, HEADS, HD = dims
    LAST = Z // 2
    PL = TP * CORES
    CH = PL * CAP
    HALF = D // 2
    HOPS = (Z // 2, Z // 2 - 1)
    GR = 2 * CAP
    SEL = PL * GR

    s = lax.axis_index("sp")
    x = lax.axis_index("tp")
    z = lax.div(s, CORES)
    c = lax.rem(s, CORES)
    me = c * TP + x
    step_a = 1 - 2 * c + Z
    z_next = (lax.rem(z + step_a, Z), lax.rem(z + 2 * Z - step_a, Z))

    def chip(zz):
        return {"sp": zz * CORES + c, "tp": x}

    ahead = (chip(z_next[0]), chip(z_next[1]))
    behind = (ahead[1], ahead[0])

    def to_x(k):
        return {"sp": s, "tp": lax.rem(x + k + TP, TP)}

    def peer(k):
        cc = lax.rem(c + k // TP, CORES)
        return {"sp": z * CORES + cc, "tp": lax.rem(x + k % TP, TP)}

    def peer_rank(k):
        return lax.rem(c + k // TP, CORES) * TP + lax.rem(x + k % TP, TP)

    def from_rank(k):
        return lax.rem(c + CORES - k // TP, CORES) * TP + lax.rem(x + TP - k % TP, TP)

    s_after = {"sp": lax.rem(s + 1, SP), "tp": x}
    s_before = {"sp": lax.rem(s + SP - 1, SP), "tp": x}

    small = [
        pltpu.make_async_copy(src, dst, load_sem.at[i])
        for i, (src, dst) in enumerate(
            (
                (q_hbm, qv),
                (sink_hbm, sink_ref),
                (ids_hbm, ids_ref.at[0]),
                (rw_hbm, rw_ref),
            )
        )
    ]
    wo_load = pltpu.make_async_copy(wo_hbm, wo, load_sem.at[4])
    large = [
        pltpu.make_async_copy(src, dst, load_sem.at[5 + i])
        for i, (src, dst) in enumerate(
            (
                (res_hbm, res_ref),
                (gain_hbm, gain_ref),
                (wg_hbm.at[0], wg),
                (wu_hbm.at[0], wu),
                (wd_hbm.at[0], wd),
            )
        )
    ]
    kv_loads = []
    for b in range(TP):
        cols = pl.ds(b * T, T)
        for i, src in enumerate((kt_hbm, vt_hbm)):
            kv_loads.append(
                pltpu.make_async_copy(
                    src.at[:, cols], kv.at[b + 1, pl.ds(i * HD, HD)], kv_sem.at[2 * b + i]
                )
            )
    barrier = pltpu.get_barrier_semaphore()
    greeted = [ahead[0], ahead[1], s_after, s_before] + [peer(k) for k in range(1, PL)]
    for device in greeted:
        pl.semaphore_signal(barrier, inc=1, device_id=device, device_id_type=MESH)
    for copy in kv_loads + small + [wo_load]:
        copy.start()

    halo = pltpu.make_async_remote_copy(
        src_ref=kv.at[TP],
        dst_ref=kv.at[0],
        send_sem=halo_sem.at[0],
        recv_sem=halo_sem.at[1],
        device_id=s_after,
        device_id_type=MESH,
    )

    row_i = iota((T, 2 * T), 0)
    col_j = iota((T, 2 * T), 1)

    def attend(b, slot):
        first = jnp.where(s * TP + b == 0, T, 0)
        allowed = (col_j > row_i) & (col_j <= row_i + T) & (col_j >= first)
        rows = pl.ds(pl.multiple_of(b * T, T), T)
        low = kv[b].astype(F32)
        high = kv[b + 1].astype(F32)
        both = jnp.concatenate([low, high], axis=1)
        kt, vt = both[:HD], both[HD:]
        none = jnp.zeros((HD, 2 * T), F32)
        keys = (jnp.concatenate([kt, none], 0).astype(BF), jnp.concatenate([none, kt], 0).astype(BF))
        values = (jnp.concatenate([vt, none], 0).astype(BF), jnp.concatenate([none, vt], 0).astype(BF))
        for pair in range(HEADS // 2):
            lanes = pl.ds(pair * 2 * HD, 2 * HD)
            query = qv[rows, lanes]
            total = None
            for side in range(2):
                head = pair * 2 + side
                sink = sink_ref[0, head]
                score = mm(query, keys[side]) * (HD ** (-0.5))
                score = jnp.where(allowed, score, -jnp.inf)
                top = jnp.maximum(jnp.max(score, axis=1, keepdims=True), sink)
                grown = jnp.exp(score - top)
                weight = jnp.sum(grown, axis=1, keepdims=True) + jnp.exp(sink - top)
                mixed = mm_nt(grown.astype(BF), values[side]) / weight
                total = mixed if total is None else total + mixed
            att[slot, :, lanes] = total.astype(BF)

    E = Z * PL
    plane_bits = PL.bit_length() - 1
    e_sub = iota((E, T), 0)
    t_sub = iota((T, T), 0)
    t_col = iota((T, T), 1)
    rel = (lax.shift_right_logical(e_sub, plane_bits) - z) * (1 - 2 * c) + 2 * Z
    rel = rel & (Z - 1)
    is_a = (rel >= 1) & (rel <= HOPS[0])
    dist = (
        jnp.where(is_a, rel, 0).astype(F32),
        jnp.where(rel > HOPS[0], Z - rel, 0).astype(F32),
    )

    def rank_of(key):
        along = jnp.broadcast_to(key, (T, T))
        down = along.T
        ahead_of = (down > along) | ((down == along) & (t_sub < t_col))
        return jnp.sum(jnp.where(ahead_of, 1.0, 0.0), axis=0, keepdims=True)

    def orders(slot):
        took = [
            jnp.where(e_sub == ids_ref[slot, k : k + 1, :], 1.0, 0.0).astype(F32) for k in range(2)
        ]
        both = took[0] + took[1]
        ways = [rank_of(jnp.max(both * d, axis=0, keepdims=True)) for d in dist]
        return took, ways, rank_of(-jnp.minimum(ways[0], ways[1]))

    def placing(position):
        return jnp.where(position == t_sub.astype(F32), 1.0, 0.0).astype(BF)

    right, left = to_x(1), to_x(-1)
    QUARTERS = T // CH

    def rs_copy(kind, q):
        src, dst, half, device, group = (
            (s2, r2, 0, right, 0),
            (s2, r2, 1, left, 0),
            (sp, rp, 1, right, 1),
            (sm, rm, 0, left, 2),
            (sp, rp, 0, right, 1),
            (sm, rm, 1, left, 2),
        )[kind]
        rows = pl.ds(q * CH, CH)
        return pltpu.make_async_remote_copy(
            src_ref=src.at[half, rows],
            dst_ref=dst.at[half, rows],
            send_sem=rs_send.at[group],
            recv_sem=rs_recv.at[kind * QUARTERS + q],
            device_id=device,
            device_id_type=MESH,
        )

    def first_leg(q):
        rs_copy(0, q).start()
        rs_copy(1, q).start()

    def alone(q):
        rs_copy(2, q).start()
        rs_copy(3, q).start()

    def joined(q):
        rows = pl.ds(q * CH, CH)
        for kind, dst, half in ((0, sp, 0), (1, sm, 1)):
            rs_copy(kind, q).wait_recv()
            total = cbuf[half, rows, pl.ds(0, HALF)] + r2[half, rows].astype(F32)
            dst[half, rows] = total.astype(BF)
            rs_copy(4 + kind, q).start()

    def project(slot, half):
        return mm(att_c[slot], wo[:, pl.ds(half * HALF, HALF)])

    def ids_copy(m):
        return pltpu.make_async_remote_copy(
            src_ref=ids_ref.at[0],
            dst_ref=ids_ref.at[m],
            send_sem=ids_send.at[m],
            recv_sem=ids_recv.at[m],
            device_id=to_x(-m),
            device_id_type=MESH,
        )

    for copy in kv_loads + small:
        copy.wait()
    attend(1, 1)
    pl.semaphore_wait(barrier, len(greeted))
    halo.start()
    for m in range(1, TP):
        ids_copy(m).start()
    for copy in large:
        copy.start()
    for b in range(2, TP):
        attend(b, b)
    took, positions, position_c = orders(0)
    place[0] = placing(positions[0])
    place[1] = placing(positions[1])
    place[2] = placing(position_c)
    halo.wait_recv()
    attend(0, 0)
    for m in range(1, TP):
        ids_copy(m).wait_recv()

    def arrange(m, placed):
        att_c[m] = mm(placed, att[lax.rem(x + m, TP)]).astype(BF)

    far, after, prior = 2, 1, TP - 1
    arrange(far, placing(orders(far)[2]))
    wo_load.wait()
    for half in range(2):
        s2[half] = project(far, half).astype(BF)
        rs_copy(half, 0).start()
    for m in (after, prior):
        arrange(m, placing(orders(m)[2]))
    sp[1] = project(after, 1).astype(BF)
    sm[0] = project(prior, 0).astype(BF)
    alone(0)
    first_leg(1)
    first_leg(2)
    cbuf[0, :, pl.ds(0, HALF)] = project(after, 0)
    cbuf[1, :, pl.ds(0, HALF)] = project(prior, 1)
    joined(0)
    alone(1)
    first_leg(3)
    large[0].wait()
    large[1].wait()
    arrange(0, place[2])
    for half in range(2):
        cols = pl.ds(half * HALF, HALF)
        acc[:, cols] = project(0, half) + mm(place[2], res_ref[:, cols])
    joined(1)
    alone(2)

    t_lane = iota((E, T), 1)
    either = took[0] + took[1]
    before = jnp.where(t_sub < t_col, 1.0, 0.0).astype(BF)
    rank = mm(either.astype(BF), before)
    weight_a = rw_ref[0:1, :]
    weight_b = rw_ref[1:2, :]
    whole = weight_a + weight_b
    share = took[0] * (weight_a / whole) + took[1] * (weight_b / whole)
    slot_value = jnp.where(is_a, positions[0] + 1.0, positions[1] + (1.0 + T))
    base = (e_sub & (PL - 1)) * GR + jnp.where(is_a, 0, CAP)
    spread_t = jnp.zeros((E, T), F32)
    spread_w = jnp.zeros((E, T), F32)
    for r in range(CAP):
        here = either * jnp.where(rank == float(r), 1.0, 0.0)
        value_col = jnp.sum(here * slot_value, axis=1, keepdims=True)
        share_col = jnp.sum(here * share, axis=1, keepdims=True)
        hit = t_lane == base + r
        spread_t = spread_t + jnp.where(hit, value_col, 0.0)
        spread_w = spread_w + jnp.where(hit, share_col, 0.0)
    plane_of = jnp.where(
        lax.shift_right_logical(iota((Z, E), 1), plane_bits) == iota((Z, E), 0), 1.0, 0.0
    ).astype(BF)
    OWN = HOPS[0] - 1
    meta[OWN, 1, pl.ds(0, Z)] = mm(plane_of, spread_t.astype(BF)).astype(BF)
    meta[OWN, 1, pl.ds(Z, Z)] = mm(plane_of, spread_w.astype(BF)).astype(BF)
    for way in range(2):
        sorter[way] = mm_nt(place[way], place[2]).astype(BF)
    normed[...] = jnp.zeros((T, D), BF)

    prefix = prefix_rows(HOPS, T, CH)
    for way in range(2):
        for hop in range(1, HOPS[way] + 1):
            n = prefix(way, hop)
            if n < T:
                ring[hop - 1, way, pl.ds(n, T - n)] = jnp.zeros((T - n, D), BF)
    joined(2)
    alone(3)

    def prepare(q):
        for kind in range(2, 6):
            rs_copy(kind, q).wait_recv()
        rows = pl.ds(q * CH, CH)
        square = jnp.zeros((CH, 1), F32)
        for half in range(2):
            cols = pl.ds(half * HALF, HALF)
            total = acc[rows, cols] + rp[half, rows].astype(F32) + rm[half, rows].astype(F32)
            kept = total.astype(BF)
            stream[rows, cols] = kept
            wide = kept.astype(F32)
            square = square + jnp.sum(wide * wide, axis=1, keepdims=True)
        scale = lax.rsqrt(square * (1.0 / D) + EPS)
        for half in range(2):
            cols = pl.ds(half * HALF, HALF)
            wide = stream[rows, cols].astype(F32)
            normed[rows, cols] = (wide * scale * gain_ref[:, cols]).astype(BF)
        count = PIECE if q < QUARTERS - 1 else T - q * PIECE
        rows = pl.ds(q * PIECE, count)
        own_a[rows] = mm(sorter[0, rows], normed[...]).astype(BF)
        ring[OWN, 1, rows] = mm(sorter[1, rows], normed[...]).astype(BF)

    first_index, pieces = {}, 0
    for way in range(2):
        for hop in range(1, HOPS[way] + 1):
            first_index[way, hop] = pieces
            pieces += prefix(way, hop) // PIECE

    def d_index(way, hop, j):
        return first_index[way, hop] + j

    def hop_index(way, hop):
        return way * HOPS[0] + hop - 1

    def packet_copy(way, hop, j):
        rows = pl.ds(j * PIECE, PIECE)
        if hop == 1:
            src = own_a.at[rows] if way == 0 else ring.at[OWN, 1, rows]
        else:
            src = ring.at[hop - 2, way, rows]
        index = d_index(way, hop, j)
        return pltpu.make_async_remote_copy(
            src_ref=src,
            dst_ref=ring.at[hop - 1, way, rows],
            send_sem=d_send.at[hop_index(way, hop)],
            recv_sem=d_recv.at[index],
            device_id=ahead[way],
            device_id_type=MESH,
        )

    def meta_copy(way, hop):
        src = meta.at[OWN, 1] if hop == 1 else meta.at[hop - 2, way]
        index = hop_index(way, hop)
        return pltpu.make_async_remote_copy(
            src_ref=src,
            dst_ref=meta.at[hop - 1, way],
            send_sem=m_send.at[index],
            recv_sem=m_recv.at[index],
            device_id=ahead[way],
            device_id_type=MESH,
        )

    for way in range(2):
        meta_copy(way, 1).start()
    prepare(0)
    for way in range(2):
        packet_copy(way, 1, 0).start()
    joined(QUARTERS - 1)

    def hop_table(hop):
        picked_t = jnp.zeros((1, T), F32)
        picked_w = jnp.zeros((1, T), F32)
        mine = iota((Z, T), 0) == z
        for way in range(2):
            known = meta[hop - 1, way].astype(F32)
            picked_t = picked_t + jnp.sum(jnp.where(mine, known[:Z], 0.0), axis=0, keepdims=True)
            picked_w = picked_w + jnp.sum(jnp.where(mine, known[Z:], 0.0), axis=0, keepdims=True)
        table[hop - 1, 0:1] = picked_t
        table[hop - 1, 1:2] = picked_w

    def plane_copy(buffer_from, buffer_to, sends, recvs, hop, k):
        return pltpu.make_async_remote_copy(
            src_ref=buffer_from.at[hop - 1, peer_rank(k)],
            dst_ref=buffer_to.at[hop - 1, me],
            send_sem=sends.at[hop - 1],
            recv_sem=recvs.at[hop - 1],
            device_id=peer(k),
            device_id_type=MESH,
        )

    def plane_all(buffer_from, buffer_to, sends, recvs, hop):
        blocks = pl.ds(0, PL - 1)
        return pltpu.make_async_remote_copy(
            src_ref=buffer_from.at[hop - 1, blocks],
            dst_ref=buffer_to.at[hop - 1, blocks],
            send_sem=sends.at[hop - 1],
            recv_sem=recvs.at[hop - 1],
            device_id=peer(1),
            device_id_type=MESH,
        )

    COLS = 512

    def select(hop):
        hop_table(hop)
        spot = (iota((2 * T, SEL), 0) + 1).astype(F32)
        hot = jnp.where(spot == table[hop - 1, 0:1, 0:SEL], 1.0, 0.0).astype(BF)
        for n in range(D // COLS):
            cols = pl.ds(n * COLS, COLS)
            rows = ring[hop - 1, :, :, cols].reshape(2 * T, COLS)
            sel[hop - 1, :, :, cols] = mm_tn(hot, rows).reshape(PL, GR, COLS).astype(BF)
        for k in PEERS:
            plane_copy(sel, xin, p_send, p_recv, hop, k).start()
        xin[hop - 1, me] = sel[hop - 1, me]

    def experts(*hops):
        for hop in hops:
            plane_all(sel, xin, p_send, p_recv, hop).wait_recv()
        rows = jnp.concatenate(
            [xin[hop - 1].astype(F32).reshape(SEL, D).astype(BF) for hop in hops], axis=0
        )
        gate = mm(rows, wg[...])
        upward = mm(rows, wu[...])
        hidden = (gate / (1.0 + jnp.exp(-gate)) * upward).astype(BF)
        for n in range(D // COLS):
            cols = pl.ds(n * COLS, COLS)
            product = mm(hidden, wd[:, cols])
            for i, hop in enumerate(hops):
                part = product[i * SEL : (i + 1) * SEL]
                yout[hop - 1, :, :, cols] = part.reshape(PL, GR, COLS).astype(BF)
        for hop in hops:
            for k in PEERS:
                plane_copy(yout, zin, y_send, y_recv, hop, k).start()
            zin[hop - 1, me] = yout[hop - 1, me]

    def back_copy(way, hop, j):
        rows = pl.ds(j * PIECE, PIECE)
        index = d_index(way, hop, j)
        return pltpu.make_async_remote_copy(
            src_ref=ret.at[hop, way, rows],
            dst_ref=ret.at[hop - 1, way, rows],
            send_sem=b_send.at[hop_index(way, hop)],
            recv_sem=b_recv.at[index],
            device_id=behind[way],
            device_id_type=MESH,
        )

    def weighted(hop, ways):
        plane_all(yout, zin, y_send, y_recv, hop).wait_recv()
        mixes = []
        for way, n in ways:
            spot = (iota((n, SEL), 0) + (way * T + 1)).astype(F32)
            hit = spot == table[hop - 1, 0:1, 0:SEL]
            mixes.append(jnp.where(hit, table[hop - 1, 1:2, 0:SEL], 0.0).astype(BF))
        for n in range(D // COLS):
            cols = pl.ds(n * COLS, COLS)
            rows = zin[hop - 1, :, :, cols].astype(F32).reshape(SEL, COLS).astype(BF)
            for (way, count), mix in zip(ways, mixes):
                cbuf[way, pl.ds(0, count), cols] = mm(mix, rows)

    def send_back(hop):
        if hop == LAST:
            weighted(hop, [(0, prefix(0, hop)), (1, T)])
            acc[...] = cbuf[1]
        else:
            weighted(hop, [(way, prefix(way, hop)) for way in range(2)])
        for i in range(T // PIECE):
            for way in range(2):
                j = prefix(way, hop) // PIECE - 1 - i
                if j < 0:
                    continue
                rows = pl.ds(j * PIECE, PIECE)
                part = cbuf[way, rows]
                if j * PIECE < prefix(way, hop + 1):
                    back_copy(way, hop + 1, j).wait_recv()
                    part = part + ret[hop, way, rows].astype(F32)
                ret[hop, way, rows] = part.astype(BF)
                back_copy(way, hop, j).start()

    def pass_on(way, hop, j):
        if j * PIECE < prefix(way, hop):
            packet_copy(way, hop, j).wait_recv()
        if j * PIECE < prefix(way, hop + 1):
            packet_copy(way, hop + 1, j).start()

    for copy in large[2:]:
        copy.wait()
    def meta_on(way, hop):
        meta_copy(way, hop).wait_recv()
        if hop < HOPS[way]:
            meta_copy(way, hop + 1).start()

    ready = list(READY) + [READY[-1]] * (T // PIECE - QUARTERS)
    events = ring_order(prefix, ORDER, ready, WAITING, LATENCY)
    prepared = 1
    missing = {
        hop: sum(prefix(way, hop) // PIECE for way in range(2)) for hop in range(1, LAST + 1)
    }
    later = []
    seen = set()
    for when, action, way, piece, hop in events:
        while later and later[0][0] <= when:
            experts(*later.pop(0)[1])
        if action == "own":
            while prepared <= min(piece, QUARTERS - 1):
                prepare(prepared)
                prepared += 1
            if piece > 0:
                packet_copy(way, 1, piece).start()
            continue
        if (way, hop) not in seen:
            seen.add((way, hop))
            meta_on(way, hop)
        pass_on(way, hop, piece)
        missing[hop] -= 1
        if missing[hop] == 0:
            select(hop)
            for group in EARLY:
                if hop in group and not any(missing[h] for h in group):
                    later.append((when + 12.0, group))
    for _, group in later:
        experts(*group)
    if TAIL == 0:
        send_back(8)
        send_back(7)
        experts(6, 5)
        experts(1, 2)
        experts(3, 4)
        rest = range(6, 0, -1)
    elif TAIL == 1:
        send_back(8)
        send_back(7)
        experts(6)
        experts(5)
        send_back(6)
        experts(1, 2)
        experts(3, 4)
        rest = range(5, 0, -1)
    elif TAIL == 2:
        send_back(8)
        experts(5)
        send_back(7)
        experts(6)
        experts(3, 4)
        send_back(6)
        experts(1, 2)
        rest = range(5, 0, -1)
    elif TAIL == 3:
        send_back(8)
        send_back(7)
        experts(5)
        send_back(6)
        experts(1, 2)
        experts(3, 4)
        rest = range(5, 0, -1)
    for hop in rest:
        send_back(hop)

    for j in range(T // PIECE):
        rows = pl.ds(j * PIECE, PIECE)
        for way in range(2):
            back_copy(way, 1, j).wait_recv()
        ret[0, 1, rows] = (ret[0, 1, rows].astype(F32) + acc[rows]).astype(BF)
    unsort = place[pl.ds(0, 2)].reshape(2 * T, T)
    for n in range(D // COLS):
        cols = pl.ds(n * COLS, COLS)
        came = ret[0, :, :, cols].reshape(2 * T, COLS)
        out_ref[:, cols] = (mm_tn(place[2], stream[:, cols]) + mm_tn(unsort, came)).astype(BF)

    halo.wait_send()
    for m in range(1, TP):
        ids_copy(m).wait_send()
    for group, (src, dst) in enumerate(((s2, r2), (sp, rp), (sm, rm))):
        pltpu.make_async_remote_copy(
            src_ref=src,
            dst_ref=dst,
            send_sem=rs_send.at[group],
            recv_sem=rs_recv.at[0],
            device_id=right,
            device_id_type=MESH,
        ).wait_send()
    for way in range(2):
        for hop in range(1, HOPS[way] + 1):
            meta_copy(way, hop).wait_send()
            rows = pl.ds(0, prefix(way, hop))
            for buffer, sems, recvs in ((ring, d_send, d_recv), (ret, b_send, b_recv)):
                pltpu.make_async_remote_copy(
                    src_ref=buffer.at[hop - 1, way, rows],
                    dst_ref=buffer.at[hop - 1, way, rows],
                    send_sem=sems.at[hop_index(way, hop)],
                    recv_sem=recvs.at[0],
                    device_id=ahead[way],
                    device_id_type=MESH,
                ).wait_send()
    for hop in range(1, LAST + 1):
        plane_all(sel, xin, p_send, p_recv, hop).wait_send()
        plane_all(yout, zin, y_send, y_recv, hop).wait_send()


def solution(mesh):
    sp_count = mesh.shape["sp"]
    tp_count = mesh.shape["tp"]

    def on_device(
        queries,
        key_heads,
        value_heads,
        sink_logit,
        out_weight,
        residual,
        norm_gain,
        expert_ids,
        route_weights,
        gate_weight,
        up_weight,
        down_weight,
    ):
        T, D = residual.shape
        HD = key_heads.shape[2]
        HEADS = queries.shape[1] // HD
        FF = gate_weight.shape[2]
        Z = sp_count // CORES
        PL = tp_count * CORES
        top_k = expert_ids.shape[1]
        CAP = max(2, 2 * top_k * T // (sp_count * tp_count))
        GR = 2 * CAP
        HOP = Z // 2
        keys_t = jnp.transpose(key_heads, (1, 2, 0)).reshape(HD, -1)
        values_t = jnp.transpose(value_heads, (1, 2, 0)).reshape(HD, -1)
        dma = pltpu.SemaphoreType.DMA
        vm = pltpu.VMEM
        any_space = pl.BlockSpec(memory_space=pl.ANY)
        in_vmem = pl.BlockSpec(memory_space=pltpu.VMEM)
        dims = (T, D, Z, tp_count, sp_count, CAP, HEADS, HD)
        quarters = T // (PL * CAP)
        prefix = prefix_rows((HOP, HOP - 1), T, PL * CAP)
        pieces = sum(prefix(way, hop) // PIECE for way in range(2) for hop in range(1, HOP + 1))
        return pl.pallas_call(
            functools.partial(layer, dims),
            out_shape=jax.ShapeDtypeStruct((T, D), BF),
            in_specs=[any_space] * 12,
            out_specs=in_vmem,
            scratch_shapes=[
                vm(queries.shape, BF),
                vm((tp_count + 1, 2 * HD, T), BF),
                vm(out_weight.shape, BF),
                vm((D, FF), BF),
                vm((D, FF), BF),
                vm((FF, D), BF),
                pltpu.SMEM((1, HEADS), F32),
                vm((T, D), BF),
                vm((1, D), F32),
                vm((tp_count, top_k, T), jnp.int32),
                vm((top_k, T), F32),
                vm((tp_count, T, HEADS * HD), BF),
                vm((tp_count, T, HEADS * HD), BF),
                vm((2, T, D // 2), BF),
                vm((2, T, D // 2), BF),
                vm((2, T, D // 2), BF),
                vm((2, T, D // 2), BF),
                vm((2, T, D // 2), BF),
                vm((2, T, D // 2), BF),
                vm((T, D), F32),
                vm((T, D), BF),
                vm((T, D), BF),
                vm((T, D), BF),
                vm((HOP, 2, T, D), BF),
                vm((HOP, 2, 2 * Z, T), BF),
                vm((HOP, 8, T), F32),
                vm((3, T, T), BF),
                vm((2, T, T), BF),
                vm((HOP, PL, GR, D), BF),
                vm((HOP, PL, GR, D), BF),
                vm((HOP, PL, GR, D), BF),
                vm((HOP, PL, GR, D), BF),
                vm((HOP + 1, 2, T, D), BF),
                vm((2, T, D), F32),
                dma((10,)),
                dma((2 * tp_count,)),
                dma((2,)),
                dma((tp_count,)),
                dma((tp_count,)),
                dma((3,)),
                dma((6 * quarters,)),
                dma((2 * HOP,)),
                dma((pieces,)),
                dma((2 * HOP,)),
                dma((2 * HOP,)),
                dma((HOP,)),
                dma((HOP,)),
                dma((HOP,)),
                dma((HOP,)),
                dma((2 * HOP,)),
                dma((pieces,)),
            ],
            compiler_params=pltpu.CompilerParams(
                collective_id=0, has_side_effects=True, vmem_limit_bytes=62 * 1024 * 1024
            ),
        )(
            queries,
            keys_t,
            values_t,
            sink_logit.reshape(1, HEADS),
            out_weight,
            residual,
            norm_gain.reshape(1, D),
            expert_ids.T,
            route_weights.T,
            gate_weight,
            up_weight,
            down_weight,
        )

    return jax.shard_map(
        on_device,
        mesh=mesh,
        in_specs=(
            P(("grp", "sp"), "tp"),
            P(("grp", "sp"), "tp", None),
            P(("grp", "sp"), "tp", None),
            P("tp"),
            P("tp", None),
            P(("grp", "sp", "tp"), None),
            P(),
            P(("grp", "sp", "tp"), None),
            P(("grp", "sp", "tp"), None),
            P(("sp", "tp"), None, None),
            P(("sp", "tp"), None, None),
            P(("sp", "tp"), None, None),
        ),
        out_specs=P(("grp", "sp", "tp"), None),
        check_vma=False,
    )
```

```python
import functools

import jax
import jax.numpy as jnp
from jax import lax
from jax.experimental import pallas as pl
from jax.experimental.pallas import tpu as pltpu
from jax.sharding import PartitionSpec as P

MESH = pl.DeviceIdType.MESH
BF = jnp.bfloat16
F32 = jnp.float32
CORES = 2
WINDOW = 128
EPS = 1e-06


def mm(a, b):
    return jnp.dot(a, b, preferred_element_type=F32)


def mm_nt(a, b):
    return lax.dot_general(a, b, (((1,), (1,)), ((), ())), preferred_element_type=F32)


def mm_tn(a, b):
    return lax.dot_general(a, b, (((0,), (0,)), ((), ())), preferred_element_type=F32)


def iota(shape, dim):
    return lax.broadcasted_iota(jnp.int32, shape, dim)


PIECE = 16
ORDER = (0, 1, 2, 3, 4, 5, 6, 7)
WAITING = (1, 1, 1, 1, 1, 1, 1, 1)
READY = (0.0, 3.9, 11.6, 15.4)
SUMS = 6.0
LATENCY = 3.9
EARLY = ((8, 7),)
TAIL = 0
PEERS = (1, 2, 3, 4, 5, 6, 7)


def prefix_rows(hops, rows, share):
    def prefix(way, hop):
        return min(rows, share * (hops[way] - hop + 1)) if hop <= hops[way] else 0

    return prefix


def ring_order(prefix, order, ready, waiting, latency=3.0):
    queue, left, now, clock = ([], []), [0.0, 0.0], [None, None], 0.0
    own = [list(order), list(order)]
    coming, events = [], []
    while True:
        for way in range(2):
            while (
                own[way]
                and ready[own[way][0]] <= clock + 1e-6
                and len(queue[way]) + (now[way] is not None) <= waiting[own[way][0]]
            ):
                piece = own[way].pop(0)
                queue[way].append((piece, 1))
                events.append((clock, "own", way, piece, 1))
            if now[way] is None and queue[way]:
                now[way], left[way] = queue[way].pop(0), 1.0
        busy = [way for way in range(2) if now[way] is not None]
        steps = [clock + left[way] * len(busy) for way in busy]
        steps += [item[0] for item in coming]
        steps += [ready[own[way][0]] for way in range(2) if own[way] and ready[own[way][0]] > clock]
        if not steps:
            return events
        later = min(steps)
        for way in busy:
            left[way] -= (later - clock) / len(busy)
        clock = later
        for way in busy:
            if left[way] < 1e-6:
                coming.append((clock + latency, way) + now[way])
                now[way] = None
        coming.sort()
        while coming and coming[0][0] <= clock + 1e-6:
            _, way, piece, hop = coming.pop(0)
            events.append((clock, "pass", way, piece, hop))
            if piece * PIECE < prefix(way, hop + 1):
                queue[way].append((piece, hop + 1))


def layer(
    dims,
    q_hbm,
    kt_hbm,
    vt_hbm,
    sink_hbm,
    wo_hbm,
    res_hbm,
    gain_hbm,
    ids_hbm,
    rw_hbm,
    wg_hbm,
    wu_hbm,
    wd_hbm,
    out_ref,
    qv,
    kv,
    wo,
    wg,
    wu,
    wd,
    sink_ref,
    res_ref,
    gain_ref,
    ids_ref,
    rw_ref,
    att,
    att_c,
    s2,
    r2,
    sp,
    sm,
    rp,
    rm,
    acc,
    stream,
    normed,
    own_a,
    ring,
    meta,
    table,
    place,
    sorter,
    sel,
    xin,
    yout,
    zin,
    ret,
    cbuf,
    load_sem,
    kv_sem,
    halo_sem,
    ids_sem,
    rs_send,
    rs_recv,
    d_send,
    d_recv,
    m_send,
    m_recv,
    p_send,
    p_recv,
    y_send,
    y_recv,
    b_send,
    b_recv,
):
    T, D, Z, TP, SP, CAP, HEADS, HD = dims
    LAST = Z // 2
    PL = TP * CORES
    CH = PL * CAP
    HALF = D // 2
    HOPS = (Z // 2, Z // 2 - 1)
    GR = 2 * CAP
    SEL = PL * GR

    s = lax.axis_index("sp")
    x = lax.axis_index("tp")
    z = lax.div(s, CORES)
    c = lax.rem(s, CORES)
    me = c * TP + x
    step_a = 1 - 2 * c + Z
    z_next = (lax.rem(z + step_a, Z), lax.rem(z + 2 * Z - step_a, Z))

    def chip(zz):
        return {"sp": zz * CORES + c, "tp": x}

    ahead = (chip(z_next[0]), chip(z_next[1]))
    behind = (ahead[1], ahead[0])

    def to_x(k):
        return {"sp": s, "tp": lax.rem(x + k + TP, TP)}

    def peer(k):
        cc = lax.rem(c + k // TP, CORES)
        return {"sp": z * CORES + cc, "tp": lax.rem(x + k % TP, TP)}

    def peer_rank(k):
        return lax.rem(c + k // TP, CORES) * TP + lax.rem(x + k % TP, TP)

    def from_rank(k):
        return lax.rem(c + CORES - k // TP, CORES) * TP + lax.rem(x + TP - k % TP, TP)

    s_after = {"sp": lax.rem(s + 1, SP), "tp": x}
    s_before = {"sp": lax.rem(s + SP - 1, SP), "tp": x}

    small = [
        pltpu.make_async_copy(src, dst, load_sem.at[i])
        for i, (src, dst) in enumerate(
            (
                (q_hbm, qv),
                (sink_hbm, sink_ref),
                (ids_hbm, ids_ref.at[0]),
                (rw_hbm, rw_ref),
            )
        )
    ]
    wo_load = pltpu.make_async_copy(wo_hbm, wo, load_sem.at[4])
    large = [
        pltpu.make_async_copy(src, dst, load_sem.at[5 + i])
        for i, (src, dst) in enumerate(
            (
                (res_hbm, res_ref),
                (gain_hbm, gain_ref),
                (wg_hbm.at[0], wg),
                (wu_hbm.at[0], wu),
                (wd_hbm.at[0], wd),
            )
        )
    ]
    kv_loads = []
    for b in range(TP):
        cols = pl.ds(b * T, T)
        for i, src in enumerate((kt_hbm, vt_hbm)):
            kv_loads.append(
                pltpu.make_async_copy(
                    src.at[:, cols], kv.at[b + 1, pl.ds(i * HD, HD)], kv_sem.at[0]
                )
            )
    barrier = pltpu.get_barrier_semaphore()
    greeted = [ahead[0], ahead[1], s_after, s_before] + [peer(k) for k in range(1, PL)]
    for device in greeted:
        pl.semaphore_signal(barrier, inc=1, device_id=device, device_id_type=MESH)
    for copy in kv_loads + small + [wo_load]:
        copy.start()

    halo = pltpu.make_async_remote_copy(
        src_ref=kv.at[TP],
        dst_ref=kv.at[0],
        send_sem=halo_sem.at[0],
        recv_sem=halo_sem.at[1],
        device_id=s_after,
        device_id_type=MESH,
    )

    row_i = iota((T, 2 * T), 0)
    col_j = iota((T, 2 * T), 1)

    def attend(b, slot):
        first = jnp.where(s * TP + b == 0, T, 0)
        allowed = (col_j > row_i) & (col_j <= row_i + T) & (col_j >= first)
        rows = pl.ds(pl.multiple_of(b * T, T), T)
        low = kv[b].astype(F32)
        high = kv[b + 1].astype(F32)
        both = jnp.concatenate([low, high], axis=1)
        kt, vt = both[:HD], both[HD:]
        none = jnp.zeros((HD, 2 * T), F32)
        keys = (jnp.concatenate([kt, none], 0).astype(BF), jnp.concatenate([none, kt], 0).astype(BF))
        values = (jnp.concatenate([vt, none], 0).astype(BF), jnp.concatenate([none, vt], 0).astype(BF))
        for pair in range(HEADS // 2):
            lanes = pl.ds(pair * 2 * HD, 2 * HD)
            query = qv[rows, lanes]
            total = None
            for side in range(2):
                head = pair * 2 + side
                sink = sink_ref[0, head]
                score = mm(query, keys[side]) * (HD ** (-0.5))
                score = jnp.where(allowed, score, -jnp.inf)
                top = jnp.maximum(jnp.max(score, axis=1, keepdims=True), sink)
                grown = jnp.exp(score - top)
                weight = jnp.sum(grown, axis=1, keepdims=True) + jnp.exp(sink - top)
                mixed = mm_nt(grown.astype(BF), values[side]) / weight
                total = mixed if total is None else total + mixed
            att[slot, :, lanes] = total.astype(BF)

    E = Z * PL
    plane_bits = PL.bit_length() - 1
    e_sub = iota((E, T), 0)
    t_sub = iota((T, T), 0)
    t_col = iota((T, T), 1)
    rel = (lax.shift_right_logical(e_sub, plane_bits) - z) * (1 - 2 * c) + 2 * Z
    rel = rel & (Z - 1)
    is_a = (rel >= 1) & (rel <= HOPS[0])
    dist = (
        jnp.where(is_a, rel, 0).astype(F32),
        jnp.where(rel > HOPS[0], Z - rel, 0).astype(F32),
    )

    def rank_of(key):
        along = jnp.broadcast_to(key, (T, T))
        down = along.T
        ahead_of = (down > along) | ((down == along) & (t_sub < t_col))
        return jnp.sum(jnp.where(ahead_of, 1.0, 0.0), axis=0, keepdims=True)

    def orders(slot):
        took = [
            jnp.where(e_sub == ids_ref[slot, k : k + 1, :], 1.0, 0.0).astype(F32) for k in range(2)
        ]
        both = took[0] + took[1]
        ways = [rank_of(jnp.max(both * d, axis=0, keepdims=True)) for d in dist]
        return took, ways, rank_of(-jnp.minimum(ways[0], ways[1]))

    def placing(position):
        return jnp.where(position == t_sub.astype(F32), 1.0, 0.0).astype(BF)

    right, left = to_x(1), to_x(-1)
    QUARTERS = T // CH

    def rs_copy(kind, q):
        src, dst, half, device, group = (
            (s2, r2, 0, right, 0),
            (s2, r2, 1, left, 0),
            (sp, rp, 1, right, 1),
            (sm, rm, 0, left, 2),
            (sp, rp, 0, right, 1),
            (sm, rm, 1, left, 2),
        )[kind]
        rows = pl.ds(q * CH, CH)
        return pltpu.make_async_remote_copy(
            src_ref=src.at[half, rows],
            dst_ref=dst.at[half, rows],
            send_sem=rs_send.at[group],
            recv_sem=rs_recv.at[min(kind, 2) * QUARTERS + q],
            device_id=device,
            device_id_type=MESH,
        )

    def first_leg(q):
        rs_copy(0, q).start()
        rs_copy(1, q).start()

    def alone(q):
        rs_copy(2, q).start()
        rs_copy(3, q).start()

    def joined(q):
        rows = pl.ds(q * CH, CH)
        for kind, dst, half in ((0, sp, 0), (1, sm, 1)):
            rs_copy(kind, q).wait_recv()
            total = cbuf[half, rows, pl.ds(0, HALF)] + r2[half, rows].astype(F32)
            dst[half, rows] = total.astype(BF)
            rs_copy(4 + kind, q).start()

    def project(slot, half):
        return mm(att_c[slot], wo[:, pl.ds(half * HALF, HALF)])

    def ids_copy(m):
        return pltpu.make_async_remote_copy(
            src_ref=ids_ref.at[0],
            dst_ref=ids_ref.at[m],
            send_sem=ids_sem.at[0],
            recv_sem=ids_sem.at[1],
            device_id=to_x(-m),
            device_id_type=MESH,
        )

    pltpu.make_async_copy(kv.at[pl.ds(1, TP)], kv.at[pl.ds(1, TP)], kv_sem.at[0]).wait()
    for copy in small:
        copy.wait()
    attend(1, 1)
    pl.semaphore_wait(barrier, len(greeted))
    halo.start()
    for m in range(1, TP):
        ids_copy(m).start()
    for copy in large:
        copy.start()
    for b in range(2, TP):
        attend(b, b)
    took, positions, position_c = orders(0)
    place[0] = placing(positions[0])
    place[1] = placing(positions[1])
    place[2] = placing(position_c)
    halo.wait_recv()
    attend(0, 0)
    others = ids_ref.at[pl.ds(1, TP - 1)]
    ids_all = pltpu.make_async_remote_copy(
        src_ref=others,
        dst_ref=others,
        send_sem=ids_sem.at[0],
        recv_sem=ids_sem.at[1],
        device_id=right,
        device_id_type=MESH,
    )
    ids_all.wait_recv()

    def arrange(m, placed):
        att_c[m] = mm(placed, att[lax.rem(x + m, TP)]).astype(BF)

    far, after, prior = 2, 1, TP - 1
    arrange(far, placing(orders(far)[2]))
    wo_load.wait()
    for half in range(2):
        s2[half] = project(far, half).astype(BF)
        rs_copy(half, 0).start()
    for m in (after, prior):
        arrange(m, placing(orders(m)[2]))
    sp[1] = project(after, 1).astype(BF)
    sm[0] = project(prior, 0).astype(BF)
    alone(0)
    first_leg(1)
    cbuf[0, :, pl.ds(0, HALF)] = project(after, 0)
    cbuf[1, :, pl.ds(0, HALF)] = project(prior, 1)
    joined(0)
    alone(1)
    large[0].wait()
    large[1].wait()
    arrange(0, place[2])
    for half in range(2):
        cols = pl.ds(half * HALF, HALF)
        acc[:, cols] = project(0, half) + mm(place[2], res_ref[:, cols])
    joined(1)
    first_leg(2)
    first_leg(3)
    alone(2)

    t_lane = iota((E, T), 1)
    either = took[0] + took[1]
    before = jnp.where(t_sub < t_col, 1.0, 0.0).astype(BF)
    rank = mm(either.astype(BF), before)
    weight_a = rw_ref[0:1, :]
    weight_b = rw_ref[1:2, :]
    whole = weight_a + weight_b
    share = took[0] * (weight_a / whole) + took[1] * (weight_b / whole)
    slot_value = jnp.where(is_a, positions[0] + 1.0, positions[1] + (1.0 + T))
    base = (e_sub & (PL - 1)) * GR + jnp.where(is_a, 0, CAP)
    spread_t = jnp.zeros((E, T), F32)
    spread_w = jnp.zeros((E, T), F32)
    for r in range(CAP):
        here = either * jnp.where(rank == float(r), 1.0, 0.0)
        value_col = jnp.sum(here * slot_value, axis=1, keepdims=True)
        share_col = jnp.sum(here * share, axis=1, keepdims=True)
        hit = t_lane == base + r
        spread_t = spread_t + jnp.where(hit, value_col, 0.0)
        spread_w = spread_w + jnp.where(hit, share_col, 0.0)
    plane_of = jnp.where(
        lax.shift_right_logical(iota((Z, E), 1), plane_bits) == iota((Z, E), 0), 1.0, 0.0
    ).astype(BF)
    OWN = HOPS[0] - 1
    meta[OWN, 1, pl.ds(0, Z)] = mm(plane_of, spread_t.astype(BF)).astype(BF)
    meta[OWN, 1, pl.ds(Z, Z)] = mm(plane_of, spread_w.astype(BF)).astype(BF)
    for way in range(2):
        sorter[way] = mm_nt(place[way], place[2]).astype(BF)
    normed[...] = jnp.zeros((T, D), BF)

    prefix = prefix_rows(HOPS, T, CH)
    for way in range(2):
        for hop in range(1, HOPS[way] + 1):
            n = prefix(way, hop)
            if n < T:
                ring[hop - 1, way, pl.ds(n, T - n)] = jnp.zeros((T - n, D), BF)

    def prepare(q):
        rows = pl.ds(q * CH, CH)
        pltpu.make_async_remote_copy(
            src_ref=acc.at[rows],
            dst_ref=acc.at[rows],
            send_sem=rs_send.at[0],
            recv_sem=rs_recv.at[2 * QUARTERS + q],
            device_id=right,
            device_id_type=MESH,
        ).wait_recv()
        square = jnp.zeros((CH, 1), F32)
        for half in range(2):
            cols = pl.ds(half * HALF, HALF)
            total = acc[rows, cols] + rp[half, rows].astype(F32) + rm[half, rows].astype(F32)
            kept = total.astype(BF)
            stream[rows, cols] = kept
            wide = kept.astype(F32)
            square = square + jnp.sum(wide * wide, axis=1, keepdims=True)
        scale = lax.rsqrt(square * (1.0 / D) + EPS)
        for half in range(2):
            cols = pl.ds(half * HALF, HALF)
            wide = stream[rows, cols].astype(F32)
            normed[rows, cols] = (wide * scale * gain_ref[:, cols]).astype(BF)
        count = PIECE if q < QUARTERS - 1 else T - q * PIECE
        rows = pl.ds(q * PIECE, count)
        own_a[rows] = mm(sorter[0, rows], normed[...]).astype(BF)
        ring[OWN, 1, rows] = mm(sorter[1, rows], normed[...]).astype(BF)

    first_index, pieces = {}, 0
    for way in range(2):
        for hop in range(1, HOPS[way] + 1):
            first_index[way, hop] = pieces
            pieces += prefix(way, hop) // PIECE

    def d_index(way, hop, j):
        return first_index[way, hop] + j

    def hop_index(way, hop):
        return way * HOPS[0] + hop - 1

    def packet_copy(way, hop, j):
        rows = pl.ds(j * PIECE, PIECE)
        if hop == 1:
            src = own_a.at[rows] if way == 0 else ring.at[OWN, 1, rows]
        else:
            src = ring.at[hop - 2, way, rows]
        index = d_index(way, hop, j)
        return pltpu.make_async_remote_copy(
            src_ref=src,
            dst_ref=ring.at[hop - 1, way, rows],
            send_sem=d_send.at[hop - 1],
            recv_sem=d_recv.at[index],
            device_id=ahead[way],
            device_id_type=MESH,
        )

    def meta_copy(way, hop):
        src = meta.at[OWN, 1] if hop == 1 else meta.at[hop - 2, way]
        index = hop_index(way, hop)
        return pltpu.make_async_remote_copy(
            src_ref=src,
            dst_ref=meta.at[hop - 1, way],
            send_sem=m_send.at[way],
            recv_sem=m_recv.at[index],
            device_id=ahead[way],
            device_id_type=MESH,
        )

    for way in range(2):
        meta_copy(way, 1).start()
    prepare(0)
    for way in range(2):
        packet_copy(way, 1, 0).start()

    def hop_table(hop):
        picked_t = jnp.zeros((1, T), F32)
        picked_w = jnp.zeros((1, T), F32)
        mine = iota((Z, T), 0) == z
        for way in range(2):
            known = meta[hop - 1, way].astype(F32)
            picked_t = picked_t + jnp.sum(jnp.where(mine, known[:Z], 0.0), axis=0, keepdims=True)
            picked_w = picked_w + jnp.sum(jnp.where(mine, known[Z:], 0.0), axis=0, keepdims=True)
        table[hop - 1, 0:1] = picked_t
        table[hop - 1, 1:2] = picked_w

    def plane_copy(buffer_from, buffer_to, sends, recvs, hop, k):
        return pltpu.make_async_remote_copy(
            src_ref=buffer_from.at[hop - 1, peer_rank(k)],
            dst_ref=buffer_to.at[hop - 1, me],
            send_sem=sends.at[0],
            recv_sem=recvs.at[hop - 1],
            device_id=peer(k),
            device_id_type=MESH,
        )

    def plane_all(buffer_from, buffer_to, sends, recvs, hop):
        blocks = pl.ds(0, PL - 1)
        return pltpu.make_async_remote_copy(
            src_ref=buffer_from.at[hop - 1, blocks],
            dst_ref=buffer_to.at[hop - 1, blocks],
            send_sem=sends.at[0],
            recv_sem=recvs.at[hop - 1],
            device_id=peer(1),
            device_id_type=MESH,
        )

    COLS = 512

    def select(hop):
        hop_table(hop)
        spot = (iota((2 * T, SEL), 0) + 1).astype(F32)
        hot = jnp.where(spot == table[hop - 1, 0:1, 0:SEL], 1.0, 0.0).astype(BF)
        for n in range(D // COLS):
            cols = pl.ds(n * COLS, COLS)
            rows = ring[hop - 1, :, :, cols].reshape(2 * T, COLS)
            sel[hop - 1, :, :, cols] = mm_tn(hot, rows).reshape(PL, GR, COLS).astype(BF)
        for k in PEERS:
            plane_copy(sel, xin, p_send, p_recv, hop, k).start()
        xin[hop - 1, me] = sel[hop - 1, me]

    def experts(*hops):
        for hop in hops:
            plane_all(sel, xin, p_send, p_recv, hop).wait_recv()
        rows = jnp.concatenate(
            [xin[hop - 1].astype(F32).reshape(SEL, D).astype(BF) for hop in hops], axis=0
        )
        gate = mm(rows, wg[...])
        upward = mm(rows, wu[...])
        hidden = (gate / (1.0 + jnp.exp(-gate)) * upward).astype(BF)
        for n in range(D // COLS):
            cols = pl.ds(n * COLS, COLS)
            product = mm(hidden, wd[:, cols])
            for i, hop in enumerate(hops):
                part = product[i * SEL : (i + 1) * SEL]
                yout[hop - 1, :, :, cols] = part.reshape(PL, GR, COLS).astype(BF)
        for hop in hops:
            for k in PEERS:
                plane_copy(yout, zin, y_send, y_recv, hop, k).start()
            zin[hop - 1, me] = yout[hop - 1, me]

    def back_copy(way, hop, j):
        rows = pl.ds(j * PIECE, PIECE)
        index = d_index(way, hop, j)
        return pltpu.make_async_remote_copy(
            src_ref=ret.at[hop, way, rows],
            dst_ref=ret.at[hop - 1, way, rows],
            send_sem=b_send.at[hop - 1],
            recv_sem=b_recv.at[index],
            device_id=behind[way],
            device_id_type=MESH,
        )

    def weighted(hop, ways):
        plane_all(yout, zin, y_send, y_recv, hop).wait_recv()
        mixes = []
        for way, n in ways:
            spot = (iota((n, SEL), 0) + (way * T + 1)).astype(F32)
            hit = spot == table[hop - 1, 0:1, 0:SEL]
            mixes.append(jnp.where(hit, table[hop - 1, 1:2, 0:SEL], 0.0).astype(BF))
        for n in range(D // COLS):
            cols = pl.ds(n * COLS, COLS)
            rows = zin[hop - 1, :, :, cols].astype(F32).reshape(SEL, COLS).astype(BF)
            for (way, count), mix in zip(ways, mixes):
                cbuf[way, pl.ds(0, count), cols] = mm(mix, rows)

    def send_back(hop):
        if hop == LAST:
            weighted(hop, [(0, prefix(0, hop)), (1, T)])
            acc[...] = cbuf[1]
        else:
            weighted(hop, [(way, prefix(way, hop)) for way in range(2)])
        for i in range(T // PIECE):
            for way in range(2):
                j = prefix(way, hop) // PIECE - 1 - i
                if j < 0:
                    continue
                rows = pl.ds(j * PIECE, PIECE)
                part = cbuf[way, rows]
                if j * PIECE < prefix(way, hop + 1):
                    back_copy(way, hop + 1, j).wait_recv()
                    part = part + ret[hop, way, rows].astype(F32)
                ret[hop, way, rows] = part.astype(BF)
                back_copy(way, hop, j).start()

    def pass_on(way, hop, j):
        if j * PIECE < prefix(way, hop):
            packet_copy(way, hop, j).wait_recv()
        if j * PIECE < prefix(way, hop + 1):
            packet_copy(way, hop + 1, j).start()

    for copy in large[2:]:
        copy.wait()
    def meta_on(way, hop):
        meta_copy(way, hop).wait_recv()
        if hop < HOPS[way]:
            meta_copy(way, hop + 1).start()

    ready = list(READY) + [READY[-1]] * (T // PIECE - QUARTERS)
    events = ring_order(prefix, ORDER, ready, WAITING, LATENCY)
    prepared = 1
    sums_left = True
    missing = {
        hop: sum(prefix(way, hop) // PIECE for way in range(2)) for hop in range(1, LAST + 1)
    }
    later = []
    seen = set()
    for when, action, way, piece, hop in events:
        if sums_left and when >= SUMS:
            joined(2)
            alone(3)
            joined(3)
            sums_left = False
        while later and later[0][0] <= when:
            experts(*later.pop(0)[1])
        if action == "own":
            while prepared <= min(piece, QUARTERS - 1):
                prepare(prepared)
                prepared += 1
            if piece > 0:
                packet_copy(way, 1, piece).start()
            continue
        if (way, hop) not in seen:
            seen.add((way, hop))
            meta_on(way, hop)
        pass_on(way, hop, piece)
        missing[hop] -= 1
        if missing[hop] == 0:
            if hop == LAST - 3 and missing[LAST - 2]:
                continue
            select(hop)
            if hop == LAST - 2 and not missing[LAST - 3]:
                select(LAST - 3)
            for group in EARLY:
                if hop in group and not any(missing[h] for h in group):
                    later.append((when + 12.0, group))
    for _, group in later:
        experts(*group)
    if TAIL == 0:
        send_back(8)
        send_back(7)
        experts(6, 5)
        experts(1, 2)
        experts(3, 4)
        rest = range(6, 0, -1)
    elif TAIL == 1:
        send_back(8)
        send_back(7)
        experts(6)
        experts(5)
        send_back(6)
        experts(1, 2)
        experts(3, 4)
        rest = range(5, 0, -1)
    elif TAIL == 2:
        send_back(8)
        experts(5)
        send_back(7)
        experts(6)
        experts(3, 4)
        send_back(6)
        experts(1, 2)
        rest = range(5, 0, -1)
    elif TAIL == 3:
        send_back(8)
        send_back(7)
        experts(5)
        send_back(6)
        experts(1, 2)
        experts(3, 4)
        rest = range(5, 0, -1)
    for hop in rest:
        send_back(hop)

    for j in range(T // PIECE):
        rows = pl.ds(j * PIECE, PIECE)
        for way in range(2):
            back_copy(way, 1, j).wait_recv()
        ret[0, 1, rows] = (ret[0, 1, rows].astype(F32) + acc[rows]).astype(BF)
    unsort = place[pl.ds(0, 2)].reshape(2 * T, T)
    for n in range(D // COLS):
        cols = pl.ds(n * COLS, COLS)
        came = ret[0, :, :, cols].reshape(2 * T, COLS)
        out_ref[:, cols] = (mm_tn(place[2], stream[:, cols]) + mm_tn(unsort, came)).astype(BF)

    halo.wait_send()
    ids_all.wait_send()
    for group, (src, dst) in enumerate(((s2, r2), (sp, rp), (sm, rm))):
        pltpu.make_async_remote_copy(
            src_ref=src,
            dst_ref=dst,
            send_sem=rs_send.at[group],
            recv_sem=rs_recv.at[0],
            device_id=right,
            device_id_type=MESH,
        ).wait_send()
    def all_left(ref, sem):
        pltpu.make_async_remote_copy(
            src_ref=ref,
            dst_ref=ref,
            send_sem=sem,
            recv_sem=halo_sem.at[1],
            device_id=right,
            device_id_type=MESH,
        ).wait_send()

    for hop in range(1, LAST + 1):
        count = prefix(0, hop) + prefix(1, hop)
        all_left(acc.at[pl.ds(0, count // 2)], d_send.at[hop - 1])
        all_left(acc.at[pl.ds(0, count // 2)], b_send.at[hop - 1])
    for way in range(2):
        all_left(meta.at[pl.ds(0, HOPS[way]), way], m_send.at[way])
    all_left(xin.at[:, pl.ds(0, PL - 1)], p_send.at[0])
    all_left(zin.at[:, pl.ds(0, PL - 1)], y_send.at[0])


def solution(mesh):
    sp_count = mesh.shape["sp"]
    tp_count = mesh.shape["tp"]

    def on_device(
        queries,
        key_heads,
        value_heads,
        sink_logit,
        out_weight,
        residual,
        norm_gain,
        expert_ids,
        route_weights,
        gate_weight,
        up_weight,
        down_weight,
    ):
        T, D = residual.shape
        HD = key_heads.shape[2]
        HEADS = queries.shape[1] // HD
        FF = gate_weight.shape[2]
        Z = sp_count // CORES
        PL = tp_count * CORES
        top_k = expert_ids.shape[1]
        CAP = max(2, 2 * top_k * T // (sp_count * tp_count))
        GR = 2 * CAP
        HOP = Z // 2
        keys_t = jnp.transpose(key_heads, (1, 2, 0)).reshape(HD, -1)
        values_t = jnp.transpose(value_heads, (1, 2, 0)).reshape(HD, -1)
        dma = pltpu.SemaphoreType.DMA
        vm = pltpu.VMEM
        any_space = pl.BlockSpec(memory_space=pl.ANY)
        in_vmem = pl.BlockSpec(memory_space=pltpu.VMEM)
        dims = (T, D, Z, tp_count, sp_count, CAP, HEADS, HD)
        quarters = T // (PL * CAP)
        prefix = prefix_rows((HOP, HOP - 1), T, PL * CAP)
        pieces = sum(prefix(way, hop) // PIECE for way in range(2) for hop in range(1, HOP + 1))
        return pl.pallas_call(
            functools.partial(layer, dims),
            out_shape=jax.ShapeDtypeStruct((T, D), BF),
            in_specs=[any_space] * 12,
            out_specs=in_vmem,
            scratch_shapes=[
                vm(queries.shape, BF),
                vm((tp_count + 1, 2 * HD, T), BF),
                vm(out_weight.shape, BF),
                vm((D, FF), BF),
                vm((D, FF), BF),
                vm((FF, D), BF),
                pltpu.SMEM((1, HEADS), F32),
                vm((T, D), BF),
                vm((1, D), F32),
                vm((tp_count, top_k, T), jnp.int32),
                vm((top_k, T), F32),
                vm((tp_count, T, HEADS * HD), BF),
                vm((tp_count, T, HEADS * HD), BF),
                vm((2, T, D // 2), BF),
                vm((2, T, D // 2), BF),
                vm((2, T, D // 2), BF),
                vm((2, T, D // 2), BF),
                vm((2, T, D // 2), BF),
                vm((2, T, D // 2), BF),
                vm((T, D), F32),
                vm((T, D), BF),
                vm((T, D), BF),
                vm((T, D), BF),
                vm((HOP, 2, T, D), BF),
                vm((HOP, 2, 2 * Z, T), BF),
                vm((HOP, 8, T), F32),
                vm((3, T, T), BF),
                vm((2, T, T), BF),
                vm((HOP, PL, GR, D), BF),
                vm((HOP, PL, GR, D), BF),
                vm((HOP, PL, GR, D), BF),
                vm((HOP, PL, GR, D), BF),
                vm((HOP + 1, 2, T, D), BF),
                vm((2, T, D), F32),
                dma((10,)),
                dma((1,)),
                dma((2,)),
                dma((2,)),
                dma((3,)),
                dma((3 * quarters,)),
                dma((HOP,)),
                dma((pieces,)),
                dma((2,)),
                dma((2 * HOP - 1,)),
                dma((1,)),
                dma((HOP,)),
                dma((1,)),
                dma((HOP,)),
                dma((HOP,)),
                dma((pieces,)),
            ],
            compiler_params=pltpu.CompilerParams(
                collective_id=0, has_side_effects=True, vmem_limit_bytes=62 * 1024 * 1024
            ),
        )(
            queries,
            keys_t,
            values_t,
            sink_logit.reshape(1, HEADS),
            out_weight,
            residual,
            norm_gain.reshape(1, D),
            expert_ids.T,
            route_weights.T,
            gate_weight,
            up_weight,
            down_weight,
        )

    return jax.shard_map(
        on_device,
        mesh=mesh,
        in_specs=(
            P(("grp", "sp"), "tp"),
            P(("grp", "sp"), "tp", None),
            P(("grp", "sp"), "tp", None),
            P("tp"),
            P("tp", None),
            P(("grp", "sp", "tp"), None),
            P(),
            P(("grp", "sp", "tp"), None),
            P(("grp", "sp", "tp"), None),
            P(("sp", "tp"), None, None),
            P(("sp", "tp"), None, None),
            P(("sp", "tp"), None, None),
        ),
        out_specs=P(("grp", "sp", "tp"), None),
        check_vma=False,
    )
```

```python
import functools

import jax
import jax.numpy as jnp
from jax import lax
from jax.experimental import pallas as pl
from jax.experimental.pallas import tpu as pltpu
from jax.sharding import PartitionSpec as P

MESH = pl.DeviceIdType.MESH
BF = jnp.bfloat16
F32 = jnp.float32
CORES = 2
WINDOW = 128
EPS = 1e-06


def mm(a, b):
    return jnp.dot(a, b, preferred_element_type=F32)


def mm_nt(a, b):
    return lax.dot_general(a, b, (((1,), (1,)), ((), ())), preferred_element_type=F32)


def mm_tn(a, b):
    return lax.dot_general(a, b, (((0,), (0,)), ((), ())), preferred_element_type=F32)


def iota(shape, dim):
    return lax.broadcasted_iota(jnp.int32, shape, dim)


PIECE = 16
ORDER = (0, 1, 2, 3, 4, 5, 6, 7)
WAITING = (1, 1, 1, 1, 1, 1, 1, 1)
READY = (0.0, 3.9, 11.6, 15.4)
SUMS = 6.0
LATENCY = 3.0


def prefix_rows(hops, rows, share):
    def prefix(way, hop):
        return min(rows, share * (hops[way] - hop + 1)) if hop <= hops[way] else 0

    return prefix


def ring_order(prefix, order, ready, waiting, latency=3.0):
    queue, left, now, clock = ([], []), [0.0, 0.0], [None, None], 0.0
    own = [list(order), list(order)]
    coming, events = [], []
    while True:
        for way in range(2):
            while (
                own[way]
                and ready[own[way][0]] <= clock + 1e-6
                and len(queue[way]) + (now[way] is not None) <= waiting[own[way][0]]
            ):
                piece = own[way].pop(0)
                queue[way].append((piece, 1))
                events.append((clock, "own", way, piece, 1))
            if now[way] is None and queue[way]:
                now[way], left[way] = queue[way].pop(0), 1.0
        busy = [way for way in range(2) if now[way] is not None]
        steps = [clock + left[way] * len(busy) for way in busy]
        steps += [item[0] for item in coming]
        steps += [ready[own[way][0]] for way in range(2) if own[way] and ready[own[way][0]] > clock]
        if not steps:
            return events
        later = min(steps)
        for way in busy:
            left[way] -= (later - clock) / len(busy)
        clock = later
        for way in busy:
            if left[way] < 1e-6:
                coming.append((clock + latency, way) + now[way])
                now[way] = None
        coming.sort()
        while coming and coming[0][0] <= clock + 1e-6:
            _, way, piece, hop = coming.pop(0)
            events.append((clock, "pass", way, piece, hop))
            if piece * PIECE < prefix(way, hop + 1):
                queue[way].append((piece, hop + 1))


def layer(
    dims,
    q_hbm,
    kt_hbm,
    vt_hbm,
    sink_hbm,
    wo_hbm,
    res_hbm,
    gain_hbm,
    ids_hbm,
    rw_hbm,
    wg_hbm,
    wu_hbm,
    wd_hbm,
    out_hbm,
    qv,
    kv,
    wo,
    wg,
    wu,
    wd,
    sink_ref,
    res_ref,
    gain_ref,
    ids_ref,
    rw_ref,
    att,
    att_c,
    s2,
    r2,
    sp,
    sm,
    rp,
    rm,
    acc,
    stream,
    normed,
    own_a,
    ring,
    meta,
    table,
    place,
    sorter,
    sel,
    xin,
    yout,
    zin,
    ret,
    cbuf,
    outv,
    load_sem,
    kv_sem,
    halo_sem,
    ids_sem,
    rs_send,
    rs_recv,
    d_send,
    d_recv,
    m_send,
    m_recv,
    p_send,
    p_recv,
    y_send,
    y_recv,
    b_send,
    b_recv,
):
    T, D, Z, TP, SP, CAP, HEADS, HD = dims
    LAST = Z // 2
    PL = TP * CORES
    CH = PL * CAP
    HALF = D // 2
    HOPS = (Z // 2, Z // 2 - 1)
    GR = 2 * CAP
    SEL = PL * GR

    s = lax.axis_index("sp")
    x = lax.axis_index("tp")
    z = lax.div(s, CORES)
    c = lax.rem(s, CORES)
    me = c * TP + x
    step_a = 1 - 2 * c + Z
    z_next = (lax.rem(z + step_a, Z), lax.rem(z + 2 * Z - step_a, Z))

    def chip(zz):
        return {"sp": zz * CORES + c, "tp": x}

    ahead = (chip(z_next[0]), chip(z_next[1]))
    behind = (ahead[1], ahead[0])

    def to_x(k):
        return {"sp": s, "tp": lax.rem(x + k + TP, TP)}

    def peer(k):
        cc = lax.rem(c + k // TP, CORES)
        return {"sp": z * CORES + cc, "tp": lax.rem(x + k % TP, TP)}

    def peer_rank(k):
        return lax.rem(c + k // TP, CORES) * TP + lax.rem(x + k % TP, TP)

    def from_rank(k):
        return lax.rem(c + CORES - k // TP, CORES) * TP + lax.rem(x + TP - k % TP, TP)

    s_after = {"sp": lax.rem(s + 1, SP), "tp": x}
    s_before = {"sp": lax.rem(s + SP - 1, SP), "tp": x}

    small = [
        pltpu.make_async_copy(src, dst, load_sem.at[i])
        for i, (src, dst) in enumerate(
            (
                (q_hbm, qv),
                (sink_hbm, sink_ref),
                (ids_hbm, ids_ref.at[0]),
                (rw_hbm, rw_ref),
            )
        )
    ]
    wo_load = pltpu.make_async_copy(wo_hbm, wo, load_sem.at[4])
    large = [
        pltpu.make_async_copy(src, dst, load_sem.at[5 + i])
        for i, (src, dst) in enumerate(
            (
                (res_hbm, res_ref),
                (gain_hbm, gain_ref),
                (wg_hbm.at[0], wg),
                (wu_hbm.at[0], wu),
                (wd_hbm.at[0], wd),
            )
        )
    ]
    kv_loads = []
    for b in range(TP):
        cols = pl.ds(b * T, T)
        for i, src in enumerate((kt_hbm, vt_hbm)):
            kv_loads.append(
                pltpu.make_async_copy(
                    src.at[:, cols], kv.at[b + 1, pl.ds(i * HD, HD)], kv_sem.at[0]
                )
            )
    barrier = pltpu.get_barrier_semaphore()
    greeted = [ahead[0], ahead[1], s_after, s_before] + [peer(k) for k in range(1, PL)]
    for device in greeted:
        pl.semaphore_signal(barrier, inc=1, device_id=device, device_id_type=MESH)
    for copy in kv_loads + small + [wo_load]:
        copy.start()

    halo = pltpu.make_async_remote_copy(
        src_ref=kv.at[TP],
        dst_ref=kv.at[0],
        send_sem=halo_sem.at[0],
        recv_sem=halo_sem.at[1],
        device_id=s_after,
        device_id_type=MESH,
    )

    row_i = iota((T, 2 * T), 0)
    col_j = iota((T, 2 * T), 1)

    def attend(b, slot):
        first = jnp.where(s * TP + b == 0, T, 0)
        allowed = (col_j > row_i) & (col_j <= row_i + T) & (col_j >= first)
        rows = pl.ds(pl.multiple_of(b * T, T), T)
        low = kv[b].astype(F32)
        high = kv[b + 1].astype(F32)
        both = jnp.concatenate([low, high], axis=1)
        kt, vt = both[:HD], both[HD:]
        none = jnp.zeros((HD, 2 * T), F32)
        keys = (jnp.concatenate([kt, none], 0).astype(BF), jnp.concatenate([none, kt], 0).astype(BF))
        values = (jnp.concatenate([vt, none], 0).astype(BF), jnp.concatenate([none, vt], 0).astype(BF))
        for pair in range(HEADS // 2):
            lanes = pl.ds(pair * 2 * HD, 2 * HD)
            query = qv[rows, lanes]
            total = None
            for side in range(2):
                head = pair * 2 + side
                sink = sink_ref[0, head]
                score = mm(query, keys[side]) * (HD ** (-0.5))
                score = jnp.where(allowed, score, -jnp.inf)
                top = jnp.maximum(jnp.max(score, axis=1, keepdims=True), sink)
                grown = jnp.exp(score - top)
                weight = jnp.sum(grown, axis=1, keepdims=True) + jnp.exp(sink - top)
                mixed = mm_nt(grown.astype(BF), values[side]) / weight
                total = mixed if total is None else total + mixed
            att[slot, :, lanes] = total.astype(BF)

    E = Z * PL
    plane_bits = PL.bit_length() - 1
    e_sub = iota((E, T), 0)
    t_sub = iota((T, T), 0)
    t_col = iota((T, T), 1)
    rel = (lax.shift_right_logical(e_sub, plane_bits) - z) * (1 - 2 * c) + 2 * Z
    rel = rel & (Z - 1)
    is_a = (rel >= 1) & (rel <= HOPS[0])
    dist = (
        jnp.where(is_a, rel, 0).astype(F32),
        jnp.where(rel > HOPS[0], Z - rel, 0).astype(F32),
    )

    def rank_of(key):
        along = jnp.broadcast_to(key, (T, T))
        down = along.T
        ahead_of = (down > along) | ((down == along) & (t_sub < t_col))
        return jnp.sum(jnp.where(ahead_of, 1.0, 0.0), axis=0, keepdims=True)

    def orders(slot):
        took = [
            jnp.where(e_sub == ids_ref[slot, k : k + 1, :], 1.0, 0.0).astype(F32) for k in range(2)
        ]
        both = took[0] + took[1]
        ways = [rank_of(jnp.max(both * d, axis=0, keepdims=True)) for d in dist]
        return took, ways, rank_of(-jnp.minimum(ways[0], ways[1]))

    def placing(position):
        return jnp.where(position == t_sub.astype(F32), 1.0, 0.0).astype(BF)

    right, left = to_x(1), to_x(-1)
    QUARTERS = T // CH

    def rs_copy(kind, q):
        src, dst, half, device, group = (
            (s2, r2, 0, right, 0),
            (s2, r2, 1, left, 0),
            (sp, rp, 1, right, 1),
            (sm, rm, 0, left, 2),
            (sp, rp, 0, right, 1),
            (sm, rm, 1, left, 2),
        )[kind]
        rows = pl.ds(q * CH, CH)
        return pltpu.make_async_remote_copy(
            src_ref=src.at[half, rows],
            dst_ref=dst.at[half, rows],
            send_sem=rs_send.at[group],
            recv_sem=rs_recv.at[min(kind, 2) * QUARTERS + q],
            device_id=device,
            device_id_type=MESH,
        )

    def first_leg(q):
        rs_copy(0, q).start()
        rs_copy(1, q).start()

    def alone(q):
        rs_copy(2, q).start()
        rs_copy(3, q).start()

    def joined(q):
        rows = pl.ds(q * CH, CH)
        for kind, dst, half in ((0, sp, 0), (1, sm, 1)):
            rs_copy(kind, q).wait_recv()
            total = cbuf[half, rows, pl.ds(0, HALF)] + r2[half, rows].astype(F32)
            dst[half, rows] = total.astype(BF)
            rs_copy(4 + kind, q).start()

    def project(slot, half):
        return mm(att_c[slot], wo[:, pl.ds(half * HALF, HALF)])

    def ids_copy(m):
        return pltpu.make_async_remote_copy(
            src_ref=ids_ref.at[0],
            dst_ref=ids_ref.at[m],
            send_sem=ids_sem.at[0],
            recv_sem=ids_sem.at[1],
            device_id=to_x(-m),
            device_id_type=MESH,
        )

    pltpu.make_async_copy(kv.at[pl.ds(1, TP)], kv.at[pl.ds(1, TP)], kv_sem.at[0]).wait()
    for copy in small:
        copy.wait()
    attend(1, 1)
    pl.semaphore_wait(barrier, len(greeted))
    halo.start()
    for m in range(1, TP):
        ids_copy(m).start()
    for copy in large:
        copy.start()
    for b in range(2, TP):
        attend(b, b)
    took, positions, position_c = orders(0)
    place[0] = placing(positions[0])
    place[1] = placing(positions[1])
    place[2] = placing(position_c)
    halo.wait_recv()
    attend(0, 0)
    others = ids_ref.at[pl.ds(1, TP - 1)]
    ids_all = pltpu.make_async_remote_copy(
        src_ref=others,
        dst_ref=others,
        send_sem=ids_sem.at[0],
        recv_sem=ids_sem.at[1],
        device_id=right,
        device_id_type=MESH,
    )
    ids_all.wait_recv()

    def arrange(m, placed):
        att_c[m] = mm(placed, att[lax.rem(x + m, TP)]).astype(BF)

    far, after, prior = 2, 1, TP - 1
    arrange(far, placing(orders(far)[2]))
    wo_load.wait()
    for half in range(2):
        s2[half] = project(far, half).astype(BF)
        rs_copy(half, 0).start()
    for m in (after, prior):
        arrange(m, placing(orders(m)[2]))
    sp[1] = project(after, 1).astype(BF)
    sm[0] = project(prior, 0).astype(BF)
    alone(0)
    first_leg(1)
    cbuf[0, :, pl.ds(0, HALF)] = project(after, 0)
    cbuf[1, :, pl.ds(0, HALF)] = project(prior, 1)
    joined(0)
    alone(1)
    large[0].wait()
    large[1].wait()
    arrange(0, place[2])
    for half in range(2):
        cols = pl.ds(half * HALF, HALF)
        acc[:, cols] = project(0, half) + mm(place[2], res_ref[:, cols])
    joined(1)
    first_leg(2)
    first_leg(3)
    alone(2)

    t_lane = iota((E, T), 1)
    either = took[0] + took[1]
    before = jnp.where(t_sub < t_col, 1.0, 0.0).astype(BF)
    rank = mm(either.astype(BF), before)
    weight_a = rw_ref[0:1, :]
    weight_b = rw_ref[1:2, :]
    whole = weight_a + weight_b
    share = took[0] * (weight_a / whole) + took[1] * (weight_b / whole)
    slot_value = jnp.where(is_a, positions[0] + 1.0, positions[1] + (1.0 + T))
    base = (e_sub & (PL - 1)) * GR + jnp.where(is_a, 0, CAP)
    spread_t = jnp.zeros((E, T), F32)
    spread_w = jnp.zeros((E, T), F32)
    for r in range(CAP):
        here = either * jnp.where(rank == float(r), 1.0, 0.0)
        value_col = jnp.sum(here * slot_value, axis=1, keepdims=True)
        share_col = jnp.sum(here * share, axis=1, keepdims=True)
        hit = t_lane == base + r
        spread_t = spread_t + jnp.where(hit, value_col, 0.0)
        spread_w = spread_w + jnp.where(hit, share_col, 0.0)
    plane_of = jnp.where(
        lax.shift_right_logical(iota((Z, E), 1), plane_bits) == iota((Z, E), 0), 1.0, 0.0
    ).astype(BF)
    OWN = HOPS[0] - 1
    meta[OWN, 1, pl.ds(0, Z)] = mm(plane_of, spread_t.astype(BF)).astype(BF)
    meta[OWN, 1, pl.ds(Z, Z)] = mm(plane_of, spread_w.astype(BF)).astype(BF)
    for way in range(2):
        sorter[way] = mm_nt(place[way], place[2]).astype(BF)
    normed[...] = jnp.zeros((T, D), BF)

    prefix = prefix_rows(HOPS, T, CH)
    for way in range(2):
        for hop in range(1, HOPS[way] + 1):
            n = prefix(way, hop)
            if n < T:
                ring[hop - 1, way, pl.ds(n, T - n)] = jnp.zeros((T - n, D), BF)

    def prepare(q):
        rows = pl.ds(q * CH, CH)
        pltpu.make_async_remote_copy(
            src_ref=acc.at[rows],
            dst_ref=acc.at[rows],
            send_sem=rs_send.at[0],
            recv_sem=rs_recv.at[2 * QUARTERS + q],
            device_id=right,
            device_id_type=MESH,
        ).wait_recv()
        square = jnp.zeros((CH, 1), F32)
        for half in range(2):
            cols = pl.ds(half * HALF, HALF)
            total = acc[rows, cols] + rp[half, rows].astype(F32) + rm[half, rows].astype(F32)
            kept = total.astype(BF)
            stream[rows, cols] = kept
            wide = kept.astype(F32)
            square = square + jnp.sum(wide * wide, axis=1, keepdims=True)
        scale = lax.rsqrt(square * (1.0 / D) + EPS)
        for half in range(2):
            cols = pl.ds(half * HALF, HALF)
            wide = stream[rows, cols].astype(F32)
            normed[rows, cols] = (wide * scale * gain_ref[:, cols]).astype(BF)
        count = PIECE if q < QUARTERS - 1 else T - q * PIECE
        rows = pl.ds(q * PIECE, count)
        own_a[rows] = mm(sorter[0, rows], normed[...]).astype(BF)
        ring[OWN, 1, rows] = mm(sorter[1, rows], normed[...]).astype(BF)

    first_index, pieces = {}, 0
    for way in range(2):
        for hop in range(1, HOPS[way] + 1):
            first_index[way, hop] = pieces
            pieces += prefix(way, hop) // PIECE

    def d_index(way, hop, j):
        return first_index[way, hop] + j

    def hop_index(way, hop):
        return way * HOPS[0] + hop - 1

    def packet_copy(way, hop, j):
        rows = pl.ds(j * PIECE, PIECE)
        if hop == 1:
            src = own_a.at[rows] if way == 0 else ring.at[OWN, 1, rows]
        else:
            src = ring.at[hop - 2, way, rows]
        index = d_index(way, hop, j)
        return pltpu.make_async_remote_copy(
            src_ref=src,
            dst_ref=ring.at[hop - 1, way, rows],
            send_sem=d_send.at[hop - 1],
            recv_sem=d_recv.at[index],
            device_id=ahead[way],
            device_id_type=MESH,
        )

    def meta_copy(way, hop):
        src = meta.at[OWN, 1] if hop == 1 else meta.at[hop - 2, way]
        index = hop_index(way, hop)
        return pltpu.make_async_remote_copy(
            src_ref=src,
            dst_ref=meta.at[hop - 1, way],
            send_sem=m_send.at[way],
            recv_sem=m_recv.at[index],
            device_id=ahead[way],
            device_id_type=MESH,
        )

    for way in range(2):
        meta_copy(way, 1).start()
    prepare(0)
    for way in range(2):
        packet_copy(way, 1, 0).start()

    def hop_table(hop):
        picked_t = jnp.zeros((1, T), F32)
        picked_w = jnp.zeros((1, T), F32)
        mine = iota((Z, T), 0) == z
        for way in range(2):
            known = meta[hop - 1, way].astype(F32)
            picked_t = picked_t + jnp.sum(jnp.where(mine, known[:Z], 0.0), axis=0, keepdims=True)
            picked_w = picked_w + jnp.sum(jnp.where(mine, known[Z:], 0.0), axis=0, keepdims=True)
        table[hop - 1, 0:1] = picked_t
        table[hop - 1, 1:2] = picked_w

    def plane_copy(buffer_from, buffer_to, sends, recvs, hop, k):
        return pltpu.make_async_remote_copy(
            src_ref=buffer_from.at[hop - 1, peer_rank(k)],
            dst_ref=buffer_to.at[hop - 1, me],
            send_sem=sends.at[0],
            recv_sem=recvs.at[hop - 1],
            device_id=peer(k),
            device_id_type=MESH,
        )

    def plane_all(buffer_from, buffer_to, sends, recvs, hop):
        blocks = pl.ds(0, PL - 1)
        return pltpu.make_async_remote_copy(
            src_ref=buffer_from.at[hop - 1, blocks],
            dst_ref=buffer_to.at[hop - 1, blocks],
            send_sem=sends.at[0],
            recv_sem=recvs.at[hop - 1],
            device_id=peer(1),
            device_id_type=MESH,
        )

    COLS = 512

    def select(hop):
        hop_table(hop)
        spot = (iota((2 * T, SEL), 0) + 1).astype(F32)
        hot = jnp.where(spot == table[hop - 1, 0:1, 0:SEL], 1.0, 0.0).astype(BF)
        for n in range(D // COLS):
            cols = pl.ds(n * COLS, COLS)
            rows = ring[hop - 1, :, :, cols].reshape(2 * T, COLS)
            sel[hop - 1, :, :, cols] = mm_tn(hot, rows).reshape(PL, GR, COLS).astype(BF)
        for k in range(1, PL):
            plane_copy(sel, xin, p_send, p_recv, hop, k).start()
        xin[hop - 1, me] = sel[hop - 1, me]

    def experts(*hops):
        for hop in hops:
            plane_all(sel, xin, p_send, p_recv, hop).wait_recv()
        rows = jnp.concatenate(
            [xin[hop - 1].astype(F32).reshape(SEL, D).astype(BF) for hop in hops], axis=0
        )
        gate = mm(rows, wg[...])
        upward = mm(rows, wu[...])
        hidden = (gate / (1.0 + jnp.exp(-gate)) * upward).astype(BF)
        for n in range(D // COLS):
            cols = pl.ds(n * COLS, COLS)
            product = mm(hidden, wd[:, cols])
            for i, hop in enumerate(hops):
                part = product[i * SEL : (i + 1) * SEL]
                yout[hop - 1, :, :, cols] = part.reshape(PL, GR, COLS).astype(BF)
        for hop in hops:
            for k in range(1, PL):
                plane_copy(yout, zin, y_send, y_recv, hop, k).start()
            zin[hop - 1, me] = yout[hop - 1, me]

    def back_copy(way, hop, j):
        rows = pl.ds(j * PIECE, PIECE)
        index = d_index(way, hop, j)
        return pltpu.make_async_remote_copy(
            src_ref=ret.at[hop, way, rows],
            dst_ref=ret.at[hop - 1, way, rows],
            send_sem=b_send.at[hop - 1],
            recv_sem=b_recv.at[index],
            device_id=behind[way],
            device_id_type=MESH,
        )

    def weighted(hop, ways):
        plane_all(yout, zin, y_send, y_recv, hop).wait_recv()
        mixes = []
        for way, n in ways:
            spot = (iota((n, SEL), 0) + (way * T + 1)).astype(F32)
            hit = spot == table[hop - 1, 0:1, 0:SEL]
            mixes.append(jnp.where(hit, table[hop - 1, 1:2, 0:SEL], 0.0).astype(BF))
        for n in range(D // COLS):
            cols = pl.ds(n * COLS, COLS)
            rows = zin[hop - 1, :, :, cols].astype(F32).reshape(SEL, COLS).astype(BF)
            for (way, count), mix in zip(ways, mixes):
                cbuf[way, pl.ds(0, count), cols] = mm(mix, rows)

    def send_back(hop):
        if hop == LAST:
            weighted(hop, [(0, prefix(0, hop)), (1, T)])
            acc[...] = cbuf[1]
        else:
            weighted(hop, [(way, prefix(way, hop)) for way in range(2)])
        for i in range(T // PIECE):
            for way in range(2):
                j = prefix(way, hop) // PIECE - 1 - i
                if j < 0:
                    continue
                rows = pl.ds(j * PIECE, PIECE)
                part = cbuf[way, rows]
                if j * PIECE < prefix(way, hop + 1):
                    back_copy(way, hop + 1, j).wait_recv()
                    part = part + ret[hop, way, rows].astype(F32)
                ret[hop, way, rows] = part.astype(BF)
                back_copy(way, hop, j).start()

    def pass_on(way, hop, j):
        if j * PIECE < prefix(way, hop):
            packet_copy(way, hop, j).wait_recv()
        if j * PIECE < prefix(way, hop + 1):
            packet_copy(way, hop + 1, j).start()

    for copy in large[2:]:
        copy.wait()
    def meta_on(way, hop):
        meta_copy(way, hop).wait_recv()
        if hop < HOPS[way]:
            meta_copy(way, hop + 1).start()

    ready = list(READY) + [READY[-1]] * (T // PIECE - QUARTERS)
    events = ring_order(prefix, ORDER, ready, WAITING, LATENCY)
    prepared = 1
    sums_left = True
    missing = {
        hop: sum(prefix(way, hop) // PIECE for way in range(2)) for hop in range(1, LAST + 1)
    }
    later = []
    seen = set()
    for when, action, way, piece, hop in events:
        if sums_left and when >= SUMS:
            joined(2)
            alone(3)
            joined(3)
            sums_left = False
        while later and later[0][0] <= when:
            experts(*later.pop(0)[1])
        if action == "own":
            while prepared <= min(piece, QUARTERS - 1):
                prepare(prepared)
                prepared += 1
            if piece > 0:
                packet_copy(way, 1, piece).start()
            continue
        if (way, hop) not in seen:
            seen.add((way, hop))
            meta_on(way, hop)
        pass_on(way, hop, piece)
        missing[hop] -= 1
        if missing[hop] == 0:
            if hop == LAST - 3 and missing[LAST - 2]:
                continue
            select(hop)
            if hop == LAST - 2 and not missing[LAST - 3]:
                select(LAST - 3)
            for group in ((LAST, LAST - 1),):
                if hop in group and not any(missing[h] for h in group):
                    later.append((when + 12.0, group))
    for _, group in later:
        experts(*group)
    send_back(LAST)
    send_back(LAST - 1)
    experts(LAST - 2)
    experts(LAST - 3)
    send_back(LAST - 2)
    experts(1, 2)
    experts(3, 4)
    for hop in range(LAST - 3, 0, -1):
        send_back(hop)

    for j in range(T // PIECE):
        rows = pl.ds(j * PIECE, PIECE)
        for way in range(2):
            back_copy(way, 1, j).wait_recv()
        ret[0, 1, rows] = (ret[0, 1, rows].astype(F32) + acc[rows]).astype(BF)
    stores = []
    unsort = place[pl.ds(0, 2)].reshape(2 * T, T)
    for n in range(D // COLS):
        cols = pl.ds(n * COLS, COLS)
        came = ret[0, :, :, cols].reshape(2 * T, COLS)
        outv[:, cols] = (mm_tn(place[2], stream[:, cols]) + mm_tn(unsort, came)).astype(BF)
        stores.append(
            pltpu.make_async_copy(outv.at[:, cols], out_hbm.at[:, cols], load_sem.at[n])
        )
        stores[-1].start()

    halo.wait_send()
    ids_all.wait_send()
    for group, (src, dst) in enumerate(((s2, r2), (sp, rp), (sm, rm))):
        pltpu.make_async_remote_copy(
            src_ref=src,
            dst_ref=dst,
            send_sem=rs_send.at[group],
            recv_sem=rs_recv.at[0],
            device_id=right,
            device_id_type=MESH,
        ).wait_send()
    def all_left(ref, sem):
        pltpu.make_async_remote_copy(
            src_ref=ref,
            dst_ref=ref,
            send_sem=sem,
            recv_sem=halo_sem.at[1],
            device_id=right,
            device_id_type=MESH,
        ).wait_send()

    for hop in range(1, LAST + 1):
        count = prefix(0, hop) + prefix(1, hop)
        all_left(acc.at[pl.ds(0, count // 2)], d_send.at[hop - 1])
        all_left(acc.at[pl.ds(0, count // 2)], b_send.at[hop - 1])
    for way in range(2):
        all_left(meta.at[pl.ds(0, HOPS[way]), way], m_send.at[way])
    all_left(xin.at[:, pl.ds(0, PL - 1)], p_send.at[0])
    all_left(zin.at[:, pl.ds(0, PL - 1)], y_send.at[0])
    for copy in stores:
        copy.wait()


def solution(mesh):
    sp_count = mesh.shape["sp"]
    tp_count = mesh.shape["tp"]

    def on_device(
        queries,
        key_heads,
        value_heads,
        sink_logit,
        out_weight,
        residual,
        norm_gain,
        expert_ids,
        route_weights,
        gate_weight,
        up_weight,
        down_weight,
    ):
        T, D = residual.shape
        HD = key_heads.shape[2]
        HEADS = queries.shape[1] // HD
        FF = gate_weight.shape[2]
        Z = sp_count // CORES
        PL = tp_count * CORES
        top_k = expert_ids.shape[1]
        CAP = max(2, 2 * top_k * T // (sp_count * tp_count))
        GR = 2 * CAP
        HOP = Z // 2
        keys_t = jnp.transpose(key_heads, (1, 2, 0)).reshape(HD, -1)
        values_t = jnp.transpose(value_heads, (1, 2, 0)).reshape(HD, -1)
        dma = pltpu.SemaphoreType.DMA
        vm = pltpu.VMEM
        any_space = pl.BlockSpec(memory_space=pl.ANY)
        dims = (T, D, Z, tp_count, sp_count, CAP, HEADS, HD)
        quarters = T // (PL * CAP)
        prefix = prefix_rows((HOP, HOP - 1), T, PL * CAP)
        pieces = sum(prefix(way, hop) // PIECE for way in range(2) for hop in range(1, HOP + 1))
        return pl.pallas_call(
            functools.partial(layer, dims),
            out_shape=jax.ShapeDtypeStruct((T, D), BF),
            in_specs=[any_space] * 12,
            out_specs=any_space,
            scratch_shapes=[
                vm(queries.shape, BF),
                vm((tp_count + 1, 2 * HD, T), BF),
                vm(out_weight.shape, BF),
                vm((D, FF), BF),
                vm((D, FF), BF),
                vm((FF, D), BF),
                pltpu.SMEM((1, HEADS), F32),
                vm((T, D), BF),
                vm((1, D), F32),
                vm((tp_count, top_k, T), jnp.int32),
                vm((top_k, T), F32),
                vm((tp_count, T, HEADS * HD), BF),
                vm((tp_count, T, HEADS * HD), BF),
                vm((2, T, D // 2), BF),
                vm((2, T, D // 2), BF),
                vm((2, T, D // 2), BF),
                vm((2, T, D // 2), BF),
                vm((2, T, D // 2), BF),
                vm((2, T, D // 2), BF),
                vm((T, D), F32),
                vm((T, D), BF),
                vm((T, D), BF),
                vm((T, D), BF),
                vm((HOP, 2, T, D), BF),
                vm((HOP, 2, 2 * Z, T), BF),
                vm((HOP, 8, T), F32),
                vm((3, T, T), BF),
                vm((2, T, T), BF),
                vm((HOP, PL, GR, D), BF),
                vm((HOP, PL, GR, D), BF),
                vm((HOP, PL, GR, D), BF),
                vm((HOP, PL, GR, D), BF),
                vm((HOP + 1, 2, T, D), BF),
                vm((2, T, D), F32),
                vm((T, D), BF),
                dma((10,)),
                dma((1,)),
                dma((2,)),
                dma((2,)),
                dma((3,)),
                dma((3 * quarters,)),
                dma((HOP,)),
                dma((pieces,)),
                dma((2,)),
                dma((2 * HOP - 1,)),
                dma((1,)),
                dma((HOP,)),
                dma((1,)),
                dma((HOP,)),
                dma((HOP,)),
                dma((pieces,)),
            ],
            compiler_params=pltpu.CompilerParams(
                collective_id=0, has_side_effects=True, vmem_limit_bytes=62 * 1024 * 1024
            ),
        )(
            queries,
            keys_t,
            values_t,
            sink_logit.reshape(1, HEADS),
            out_weight,
            residual,
            norm_gain.reshape(1, D),
            expert_ids.T,
            route_weights.T,
            gate_weight,
            up_weight,
            down_weight,
        )

    return jax.shard_map(
        on_device,
        mesh=mesh,
        in_specs=(
            P(("grp", "sp"), "tp"),
            P(("grp", "sp"), "tp", None),
            P(("grp", "sp"), "tp", None),
            P("tp"),
            P("tp", None),
            P(("grp", "sp", "tp"), None),
            P(),
            P(("grp", "sp", "tp"), None),
            P(("grp", "sp", "tp"), None),
            P(("sp", "tp"), None, None),
            P(("sp", "tp"), None, None),
            P(("sp", "tp"), None, None),
        ),
        out_specs=P(("grp", "sp", "tp"), None),
        check_vma=False,
    )
```

```python
import functools

import jax
import jax.numpy as jnp
from jax import lax
from jax.experimental import pallas as pl
from jax.experimental.pallas import tpu as pltpu
from jax.sharding import PartitionSpec as P

MESH = pl.DeviceIdType.MESH
BF = jnp.bfloat16
F32 = jnp.float32
CORES = 2
WINDOW = 128
EPS = 1e-06


def mm(a, b):
    return jnp.dot(a, b, preferred_element_type=F32)


def mm_nt(a, b):
    return lax.dot_general(a, b, (((1,), (1,)), ((), ())), preferred_element_type=F32)


def mm_tn(a, b):
    return lax.dot_general(a, b, (((0,), (0,)), ((), ())), preferred_element_type=F32)


def iota(shape, dim):
    return lax.broadcasted_iota(jnp.int32, shape, dim)


PIECE = 16
ORDER = (0, 1, 2, 3, 4, 5, 6, 7)
WAITING = (1, 1, 1, 1, 1, 1, 1, 1)
READY = (0.0, 3.9, 11.6, 15.4)
SUMS = 6.0
LATENCY = 3.0


def prefix_rows(hops, rows, share):
    def prefix(way, hop):
        return min(rows, share * (hops[way] - hop + 1)) if hop <= hops[way] else 0

    return prefix


def ring_order(prefix, order, ready, waiting, latency=3.0):
    queue, left, now, clock = ([], []), [0.0, 0.0], [None, None], 0.0
    own = [list(order), list(order)]
    coming, events = [], []
    while True:
        for way in range(2):
            while (
                own[way]
                and ready[own[way][0]] <= clock + 1e-6
                and len(queue[way]) + (now[way] is not None) <= waiting[own[way][0]]
            ):
                piece = own[way].pop(0)
                queue[way].append((piece, 1))
                events.append((clock, "own", way, piece, 1))
            if now[way] is None and queue[way]:
                now[way], left[way] = queue[way].pop(0), 1.0
        busy = [way for way in range(2) if now[way] is not None]
        steps = [clock + left[way] * len(busy) for way in busy]
        steps += [item[0] for item in coming]
        steps += [ready[own[way][0]] for way in range(2) if own[way] and ready[own[way][0]] > clock]
        if not steps:
            return events
        later = min(steps)
        for way in busy:
            left[way] -= (later - clock) / len(busy)
        clock = later
        for way in busy:
            if left[way] < 1e-6:
                coming.append((clock + latency, way) + now[way])
                now[way] = None
        coming.sort()
        while coming and coming[0][0] <= clock + 1e-6:
            _, way, piece, hop = coming.pop(0)
            events.append((clock, "pass", way, piece, hop))
            if piece * PIECE < prefix(way, hop + 1):
                queue[way].append((piece, hop + 1))


def layer(
    dims,
    q_hbm,
    kt_hbm,
    vt_hbm,
    sink_hbm,
    wo_hbm,
    res_hbm,
    gain_hbm,
    ids_hbm,
    rw_hbm,
    wg_hbm,
    wu_hbm,
    wd_hbm,
    out_hbm,
    qv,
    kv,
    wo,
    wg,
    wu,
    wd,
    sink_ref,
    res_ref,
    gain_ref,
    ids_ref,
    rw_ref,
    att,
    att_c,
    s2,
    r2,
    sp,
    sm,
    rp,
    rm,
    acc,
    stream,
    normed,
    own_a,
    ring,
    meta,
    table,
    place,
    sorter,
    sel,
    xin,
    yout,
    zin,
    ret,
    cbuf,
    outv,
    load_sem,
    kv_sem,
    halo_sem,
    ids_sem,
    rs_send,
    rs_recv,
    d_send,
    d_recv,
    m_send,
    m_recv,
    p_send,
    p_recv,
    y_send,
    y_recv,
    b_send,
    b_recv,
):
    T, D, Z, TP, SP, CAP, HEADS, HD = dims
    LAST = Z // 2
    PL = TP * CORES
    CH = PL * CAP
    HALF = D // 2
    HOPS = (Z // 2, Z // 2 - 1)
    GR = 2 * CAP
    SEL = PL * GR

    s = lax.axis_index("sp")
    x = lax.axis_index("tp")
    z = lax.div(s, CORES)
    c = lax.rem(s, CORES)
    me = c * TP + x
    step_a = 1 - 2 * c + Z
    z_next = (lax.rem(z + step_a, Z), lax.rem(z + 2 * Z - step_a, Z))

    def chip(zz):
        return {"sp": zz * CORES + c, "tp": x}

    ahead = (chip(z_next[0]), chip(z_next[1]))
    behind = (ahead[1], ahead[0])

    def to_x(k):
        return {"sp": s, "tp": lax.rem(x + k + TP, TP)}

    def peer(k):
        cc = lax.rem(c + k // TP, CORES)
        return {"sp": z * CORES + cc, "tp": lax.rem(x + k % TP, TP)}

    def peer_rank(k):
        return lax.rem(c + k // TP, CORES) * TP + lax.rem(x + k % TP, TP)

    def from_rank(k):
        return lax.rem(c + CORES - k // TP, CORES) * TP + lax.rem(x + TP - k % TP, TP)

    s_after = {"sp": lax.rem(s + 1, SP), "tp": x}
    s_before = {"sp": lax.rem(s + SP - 1, SP), "tp": x}

    small = [
        pltpu.make_async_copy(src, dst, load_sem.at[i])
        for i, (src, dst) in enumerate(
            (
                (q_hbm, qv),
                (sink_hbm, sink_ref),
                (ids_hbm, ids_ref.at[0]),
                (rw_hbm, rw_ref),
            )
        )
    ]
    wo_load = pltpu.make_async_copy(wo_hbm, wo, load_sem.at[4])
    large = [
        pltpu.make_async_copy(src, dst, load_sem.at[5 + i])
        for i, (src, dst) in enumerate(
            (
                (res_hbm, res_ref),
                (gain_hbm, gain_ref),
                (wg_hbm.at[0], wg),
                (wu_hbm.at[0], wu),
                (wd_hbm.at[0], wd),
            )
        )
    ]
    kv_loads = []
    for b in range(TP):
        cols = pl.ds(b * T, T)
        for i, src in enumerate((kt_hbm, vt_hbm)):
            kv_loads.append(
                pltpu.make_async_copy(
                    src.at[:, cols], kv.at[b + 1, pl.ds(i * HD, HD)], kv_sem.at[0]
                )
            )
    barrier = pltpu.get_barrier_semaphore()
    greeted = [ahead[0], ahead[1], s_after, s_before] + [peer(k) for k in range(1, PL)]
    for device in greeted:
        pl.semaphore_signal(barrier, inc=1, device_id=device, device_id_type=MESH)
    for copy in kv_loads + small + [wo_load]:
        copy.start()

    halo = pltpu.make_async_remote_copy(
        src_ref=kv.at[TP],
        dst_ref=kv.at[0],
        send_sem=halo_sem.at[0],
        recv_sem=halo_sem.at[1],
        device_id=s_after,
        device_id_type=MESH,
    )

    row_i = iota((T, 2 * T), 0)
    col_j = iota((T, 2 * T), 1)

    def attend(b, slot):
        first = jnp.where(s * TP + b == 0, T, 0)
        allowed = (col_j > row_i) & (col_j <= row_i + T) & (col_j >= first)
        rows = pl.ds(pl.multiple_of(b * T, T), T)
        low = kv[b].astype(F32)
        high = kv[b + 1].astype(F32)
        both = jnp.concatenate([low, high], axis=1)
        kt, vt = both[:HD], both[HD:]
        none = jnp.zeros((HD, 2 * T), F32)
        keys = (jnp.concatenate([kt, none], 0).astype(BF), jnp.concatenate([none, kt], 0).astype(BF))
        values = (jnp.concatenate([vt, none], 0).astype(BF), jnp.concatenate([none, vt], 0).astype(BF))
        for pair in range(HEADS // 2):
            lanes = pl.ds(pair * 2 * HD, 2 * HD)
            query = qv[rows, lanes]
            total = None
            for side in range(2):
                head = pair * 2 + side
                sink = sink_ref[0, head]
                score = mm(query, keys[side]) * (HD ** (-0.5))
                score = jnp.where(allowed, score, -jnp.inf)
                top = jnp.maximum(jnp.max(score, axis=1, keepdims=True), sink)
                grown = jnp.exp(score - top)
                weight = jnp.sum(grown, axis=1, keepdims=True) + jnp.exp(sink - top)
                mixed = mm_nt(grown.astype(BF), values[side]) / weight
                total = mixed if total is None else total + mixed
            att[slot, :, lanes] = total.astype(BF)

    E = Z * PL
    plane_bits = PL.bit_length() - 1
    e_sub = iota((E, T), 0)
    t_sub = iota((T, T), 0)
    t_col = iota((T, T), 1)
    rel = (lax.shift_right_logical(e_sub, plane_bits) - z) * (1 - 2 * c) + 2 * Z
    rel = rel & (Z - 1)
    is_a = (rel >= 1) & (rel <= HOPS[0])
    dist = (
        jnp.where(is_a, rel, 0).astype(F32),
        jnp.where(rel > HOPS[0], Z - rel, 0).astype(F32),
    )

    def rank_of(key):
        along = jnp.broadcast_to(key, (T, T))
        down = along.T
        ahead_of = (down > along) | ((down == along) & (t_sub < t_col))
        return jnp.sum(jnp.where(ahead_of, 1.0, 0.0), axis=0, keepdims=True)

    def orders(slot):
        took = [
            jnp.where(e_sub == ids_ref[slot, k : k + 1, :], 1.0, 0.0).astype(F32) for k in range(2)
        ]
        both = took[0] + took[1]
        ways = [rank_of(jnp.max(both * d, axis=0, keepdims=True)) for d in dist]
        return took, ways, rank_of(-jnp.minimum(ways[0], ways[1]))

    def placing(position):
        return jnp.where(position == t_sub.astype(F32), 1.0, 0.0).astype(BF)

    right, left = to_x(1), to_x(-1)
    QUARTERS = T // CH

    def rs_copy(kind, q):
        src, dst, half, device, group = (
            (s2, r2, 0, right, 0),
            (s2, r2, 1, left, 0),
            (sp, rp, 1, right, 1),
            (sm, rm, 0, left, 2),
            (sp, rp, 0, right, 1),
            (sm, rm, 1, left, 2),
        )[kind]
        rows = pl.ds(q * CH, CH)
        return pltpu.make_async_remote_copy(
            src_ref=src.at[half, rows],
            dst_ref=dst.at[half, rows],
            send_sem=rs_send.at[group],
            recv_sem=rs_recv.at[min(kind, 2) * QUARTERS + q],
            device_id=device,
            device_id_type=MESH,
        )

    def first_leg(q):
        rs_copy(0, q).start()
        rs_copy(1, q).start()

    def alone(q):
        rs_copy(2, q).start()
        rs_copy(3, q).start()

    def joined(q):
        rows = pl.ds(q * CH, CH)
        for kind, dst, half in ((0, sp, 0), (1, sm, 1)):
            rs_copy(kind, q).wait_recv()
            total = cbuf[half, rows, pl.ds(0, HALF)] + r2[half, rows].astype(F32)
            dst[half, rows] = total.astype(BF)
            rs_copy(4 + kind, q).start()

    def project(slot, half):
        return mm(att_c[slot], wo[:, pl.ds(half * HALF, HALF)])

    def ids_copy(m):
        return pltpu.make_async_remote_copy(
            src_ref=ids_ref.at[0],
            dst_ref=ids_ref.at[m],
            send_sem=ids_sem.at[0],
            recv_sem=ids_sem.at[1],
            device_id=to_x(-m),
            device_id_type=MESH,
        )

    pltpu.make_async_copy(kv.at[pl.ds(1, TP)], kv.at[pl.ds(1, TP)], kv_sem.at[0]).wait()
    for copy in small:
        copy.wait()
    attend(1, 1)
    pl.semaphore_wait(barrier, len(greeted))
    halo.start()
    for m in range(1, TP):
        ids_copy(m).start()
    for copy in large:
        copy.start()
    for b in range(2, TP):
        attend(b, b)
    took, positions, position_c = orders(0)
    place[0] = placing(positions[0])
    place[1] = placing(positions[1])
    place[2] = placing(position_c)
    halo.wait_recv()
    attend(0, 0)
    others = ids_ref.at[pl.ds(1, TP - 1)]
    ids_all = pltpu.make_async_remote_copy(
        src_ref=others,
        dst_ref=others,
        send_sem=ids_sem.at[0],
        recv_sem=ids_sem.at[1],
        device_id=right,
        device_id_type=MESH,
    )
    ids_all.wait_recv()

    def arrange(m, placed):
        att_c[m] = mm(placed, att[lax.rem(x + m, TP)]).astype(BF)

    far, after, prior = 2, 1, TP - 1
    arrange(far, placing(orders(far)[2]))
    wo_load.wait()
    for half in range(2):
        s2[half] = project(far, half).astype(BF)
        rs_copy(half, 0).start()
    for m in (after, prior):
        arrange(m, placing(orders(m)[2]))
    sp[1] = project(after, 1).astype(BF)
    sm[0] = project(prior, 0).astype(BF)
    alone(0)
    first_leg(1)
    cbuf[0, :, pl.ds(0, HALF)] = project(after, 0)
    cbuf[1, :, pl.ds(0, HALF)] = project(prior, 1)
    joined(0)
    alone(1)
    large[0].wait()
    large[1].wait()
    arrange(0, place[2])
    for half in range(2):
        cols = pl.ds(half * HALF, HALF)
        acc[:, cols] = project(0, half) + mm(place[2], res_ref[:, cols])
    joined(1)
    first_leg(2)
    first_leg(3)
    alone(2)

    t_lane = iota((E, T), 1)
    either = took[0] + took[1]
    before = jnp.where(t_sub < t_col, 1.0, 0.0).astype(BF)
    rank = mm(either.astype(BF), before)
    weight_a = rw_ref[0:1, :]
    weight_b = rw_ref[1:2, :]
    whole = weight_a + weight_b
    share = took[0] * (weight_a / whole) + took[1] * (weight_b / whole)
    slot_value = jnp.where(is_a, positions[0] + 1.0, positions[1] + (1.0 + T))
    base = (e_sub & (PL - 1)) * GR + jnp.where(is_a, 0, CAP)
    spread_t = jnp.zeros((E, T), F32)
    spread_w = jnp.zeros((E, T), F32)
    for r in range(CAP):
        here = either * jnp.where(rank == float(r), 1.0, 0.0)
        value_col = jnp.sum(here * slot_value, axis=1, keepdims=True)
        share_col = jnp.sum(here * share, axis=1, keepdims=True)
        hit = t_lane == base + r
        spread_t = spread_t + jnp.where(hit, value_col, 0.0)
        spread_w = spread_w + jnp.where(hit, share_col, 0.0)
    plane_of = jnp.where(
        lax.shift_right_logical(iota((Z, E), 1), plane_bits) == iota((Z, E), 0), 1.0, 0.0
    ).astype(BF)
    OWN = HOPS[0] - 1
    meta[OWN, 1, pl.ds(0, Z)] = mm(plane_of, spread_t.astype(BF)).astype(BF)
    meta[OWN, 1, pl.ds(Z, Z)] = mm(plane_of, spread_w.astype(BF)).astype(BF)
    for way in range(2):
        sorter[way] = mm_nt(place[way], place[2]).astype(BF)
    normed[...] = jnp.zeros((T, D), BF)

    prefix = prefix_rows(HOPS, T, CH)
    for way in range(2):
        for hop in range(1, HOPS[way] + 1):
            n = prefix(way, hop)
            if n < T:
                ring[hop - 1, way, pl.ds(n, T - n)] = jnp.zeros((T - n, D), BF)

    def prepare(q):
        rows = pl.ds(q * CH, CH)
        pltpu.make_async_remote_copy(
            src_ref=acc.at[rows],
            dst_ref=acc.at[rows],
            send_sem=rs_send.at[0],
            recv_sem=rs_recv.at[2 * QUARTERS + q],
            device_id=right,
            device_id_type=MESH,
        ).wait_recv()
        square = jnp.zeros((CH, 1), F32)
        for half in range(2):
            cols = pl.ds(half * HALF, HALF)
            total = acc[rows, cols] + rp[half, rows].astype(F32) + rm[half, rows].astype(F32)
            kept = total.astype(BF)
            stream[rows, cols] = kept
            wide = kept.astype(F32)
            square = square + jnp.sum(wide * wide, axis=1, keepdims=True)
        scale = lax.rsqrt(square * (1.0 / D) + EPS)
        for half in range(2):
            cols = pl.ds(half * HALF, HALF)
            wide = stream[rows, cols].astype(F32)
            normed[rows, cols] = (wide * scale * gain_ref[:, cols]).astype(BF)
        count = PIECE if q < QUARTERS - 1 else T - q * PIECE
        rows = pl.ds(q * PIECE, count)
        own_a[rows] = mm(sorter[0, rows], normed[...]).astype(BF)
        ring[OWN, 1, rows] = mm(sorter[1, rows], normed[...]).astype(BF)

    first_index, pieces = {}, 0
    for way in range(2):
        for hop in range(1, HOPS[way] + 1):
            first_index[way, hop] = pieces
            pieces += prefix(way, hop) // PIECE

    def d_index(way, hop, j):
        return first_index[way, hop] + j

    def hop_index(way, hop):
        return way * HOPS[0] + hop - 1

    def packet_copy(way, hop, j):
        rows = pl.ds(j * PIECE, PIECE)
        if hop == 1:
            src = own_a.at[rows] if way == 0 else ring.at[OWN, 1, rows]
        else:
            src = ring.at[hop - 2, way, rows]
        index = d_index(way, hop, j)
        return pltpu.make_async_remote_copy(
            src_ref=src,
            dst_ref=ring.at[hop - 1, way, rows],
            send_sem=d_send.at[hop - 1],
            recv_sem=d_recv.at[index],
            device_id=ahead[way],
            device_id_type=MESH,
        )

    def meta_copy(way, hop):
        src = meta.at[OWN, 1] if hop == 1 else meta.at[hop - 2, way]
        index = hop_index(way, hop)
        return pltpu.make_async_remote_copy(
            src_ref=src,
            dst_ref=meta.at[hop - 1, way],
            send_sem=m_send.at[way],
            recv_sem=m_recv.at[index],
            device_id=ahead[way],
            device_id_type=MESH,
        )

    for way in range(2):
        meta_copy(way, 1).start()
    prepare(0)
    for way in range(2):
        packet_copy(way, 1, 0).start()

    def hop_table(hop):
        picked_t = jnp.zeros((1, T), F32)
        picked_w = jnp.zeros((1, T), F32)
        mine = iota((Z, T), 0) == z
        for way in range(2):
            known = meta[hop - 1, way].astype(F32)
            picked_t = picked_t + jnp.sum(jnp.where(mine, known[:Z], 0.0), axis=0, keepdims=True)
            picked_w = picked_w + jnp.sum(jnp.where(mine, known[Z:], 0.0), axis=0, keepdims=True)
        table[hop - 1, 0:1] = picked_t
        table[hop - 1, 1:2] = picked_w

    def plane_copy(buffer_from, buffer_to, sends, recvs, hop, k):
        return pltpu.make_async_remote_copy(
            src_ref=buffer_from.at[hop - 1, peer_rank(k)],
            dst_ref=buffer_to.at[hop - 1, me],
            send_sem=sends.at[0],
            recv_sem=recvs.at[hop - 1],
            device_id=peer(k),
            device_id_type=MESH,
        )

    def plane_all(buffer_from, buffer_to, sends, recvs, hop):
        blocks = pl.ds(0, PL - 1)
        return pltpu.make_async_remote_copy(
            src_ref=buffer_from.at[hop - 1, blocks],
            dst_ref=buffer_to.at[hop - 1, blocks],
            send_sem=sends.at[0],
            recv_sem=recvs.at[hop - 1],
            device_id=peer(1),
            device_id_type=MESH,
        )

    COLS = 512
    far_first = sorted(range(1, PL), key=lambda k: -min(k % TP, TP - k % TP))

    def select(hop):
        spot = (iota((2 * T, SEL), 0) + 1).astype(F32)
        hot = jnp.where(spot == table[hop - 1, 0:1, 0:SEL], 1.0, 0.0).astype(BF)
        for n in range(D // COLS):
            cols = pl.ds(n * COLS, COLS)
            rows = ring[hop - 1, :, :, cols].reshape(2 * T, COLS)
            sel[hop - 1, :, :, cols] = mm_tn(hot, rows).reshape(PL, GR, COLS).astype(BF)
        for k in far_first:
            plane_copy(sel, xin, p_send, p_recv, hop, k).start()
        xin[hop - 1, me] = sel[hop - 1, me]

    def experts(*hops):
        for hop in hops:
            plane_all(sel, xin, p_send, p_recv, hop).wait_recv()
        rows = jnp.concatenate(
            [xin[hop - 1].astype(F32).reshape(SEL, D).astype(BF) for hop in hops], axis=0
        )
        gate = mm(rows, wg[...])
        upward = mm(rows, wu[...])
        hidden = (gate / (1.0 + jnp.exp(-gate)) * upward).astype(BF)
        for n in range(D // COLS):
            cols = pl.ds(n * COLS, COLS)
            product = mm(hidden, wd[:, cols])
            for i, hop in enumerate(hops):
                part = product[i * SEL : (i + 1) * SEL]
                yout[hop - 1, :, :, cols] = part.reshape(PL, GR, COLS).astype(BF)
        for hop in hops:
            for k in far_first:
                plane_copy(yout, zin, y_send, y_recv, hop, k).start()
            zin[hop - 1, me] = yout[hop - 1, me]

    def back_copy(way, hop, j):
        rows = pl.ds(j * PIECE, PIECE)
        index = d_index(way, hop, j)
        return pltpu.make_async_remote_copy(
            src_ref=ret.at[hop, way, rows],
            dst_ref=ret.at[hop - 1, way, rows],
            send_sem=b_send.at[hop - 1],
            recv_sem=b_recv.at[index],
            device_id=behind[way],
            device_id_type=MESH,
        )

    def weighted(hop, ways):
        plane_all(yout, zin, y_send, y_recv, hop).wait_recv()
        mixes = []
        for way, n in ways:
            spot = (iota((n, SEL), 0) + (way * T + 1)).astype(F32)
            hit = spot == table[hop - 1, 0:1, 0:SEL]
            mixes.append(jnp.where(hit, table[hop - 1, 1:2, 0:SEL], 0.0).astype(BF))
        for n in range(D // COLS):
            cols = pl.ds(n * COLS, COLS)
            rows = zin[hop - 1, :, :, cols].astype(F32).reshape(SEL, COLS).astype(BF)
            for (way, count), mix in zip(ways, mixes):
                cbuf[way, pl.ds(0, count), cols] = mm(mix, rows)

    def send_back(hop):
        if hop == LAST:
            weighted(hop, [(0, prefix(0, hop)), (1, T)])
            acc[...] = cbuf[1]
        else:
            weighted(hop, [(way, prefix(way, hop)) for way in range(2)])
        for i in range(T // PIECE):
            for way in range(2):
                j = prefix(way, hop) // PIECE - 1 - i
                if j < 0:
                    continue
                rows = pl.ds(j * PIECE, PIECE)
                part = cbuf[way, rows]
                if j * PIECE < prefix(way, hop + 1):
                    back_copy(way, hop + 1, j).wait_recv()
                    part = part + ret[hop, way, rows].astype(F32)
                ret[hop, way, rows] = part.astype(BF)
                back_copy(way, hop, j).start()

    def pass_on(way, hop, j):
        if j * PIECE < prefix(way, hop):
            packet_copy(way, hop, j).wait_recv()
        if j * PIECE < prefix(way, hop + 1):
            packet_copy(way, hop + 1, j).start()

    for copy in large[2:]:
        copy.wait()
    def meta_on(way, hop):
        meta_copy(way, hop).wait_recv()
        if hop < HOPS[way]:
            meta_copy(way, hop + 1).start()

    ready = list(READY) + [READY[-1]] * (T // PIECE - QUARTERS)
    events = ring_order(prefix, ORDER, ready, WAITING, LATENCY)
    prepared = 1
    sums_left = True
    missing = {
        hop: sum(prefix(way, hop) // PIECE for way in range(2)) for hop in range(1, LAST + 1)
    }
    later = []
    seen = set()
    for when, action, way, piece, hop in events:
        if sums_left and when >= SUMS:
            joined(2)
            alone(3)
            joined(3)
            sums_left = False
        while later and later[0][0] <= when:
            experts(*later.pop(0)[1])
        if action == "own":
            while prepared <= min(piece, QUARTERS - 1):
                prepare(prepared)
                prepared += 1
            if piece > 0:
                packet_copy(way, 1, piece).start()
            continue
        if (way, hop) not in seen:
            seen.add((way, hop))
            meta_on(way, hop)
            if all((w, hop) in seen for w in range(2) if hop <= HOPS[w]):
                hop_table(hop)
        pass_on(way, hop, piece)
        missing[hop] -= 1
        if missing[hop] == 0:
            if hop == LAST - 3 and missing[LAST - 2]:
                continue
            select(hop)
            if hop == LAST - 2 and not missing[LAST - 3]:
                select(LAST - 3)
            for group in ((LAST, LAST - 1),):
                if hop in group and not any(missing[h] for h in group):
                    later.append((when + 10.0, group))
    for _, group in later:
        experts(*group)
    send_back(LAST)
    send_back(LAST - 1)
    experts(LAST - 2)
    experts(LAST - 3)
    send_back(LAST - 2)
    experts(1, 2)
    experts(3, 4)
    for hop in range(LAST - 3, 0, -1):
        send_back(hop)

    for j in range(T // PIECE):
        rows = pl.ds(j * PIECE, PIECE)
        for way in range(2):
            back_copy(way, 1, j).wait_recv()
        ret[0, 1, rows] = (ret[0, 1, rows].astype(F32) + acc[rows]).astype(BF)
    stores = []
    unsort = place[pl.ds(0, 2)].reshape(2 * T, T)
    for n in range(D // COLS):
        cols = pl.ds(n * COLS, COLS)
        came = ret[0, :, :, cols].reshape(2 * T, COLS)
        outv[:, cols] = (mm_tn(place[2], stream[:, cols]) + mm_tn(unsort, came)).astype(BF)
        stores.append(
            pltpu.make_async_copy(outv.at[:, cols], out_hbm.at[:, cols], load_sem.at[n])
        )
        stores[-1].start()

    halo.wait_send()
    ids_all.wait_send()
    for group, (src, dst) in enumerate(((s2, r2), (sp, rp), (sm, rm))):
        pltpu.make_async_remote_copy(
            src_ref=src,
            dst_ref=dst,
            send_sem=rs_send.at[group],
            recv_sem=rs_recv.at[0],
            device_id=right,
            device_id_type=MESH,
        ).wait_send()
    def all_left(ref, sem):
        pltpu.make_async_remote_copy(
            src_ref=ref,
            dst_ref=ref,
            send_sem=sem,
            recv_sem=halo_sem.at[1],
            device_id=right,
            device_id_type=MESH,
        ).wait_send()

    for hop in range(1, LAST + 1):
        count = prefix(0, hop) + prefix(1, hop)
        all_left(acc.at[pl.ds(0, count // 2)], d_send.at[hop - 1])
        all_left(acc.at[pl.ds(0, count // 2)], b_send.at[hop - 1])
    for way in range(2):
        all_left(meta.at[pl.ds(0, HOPS[way]), way], m_send.at[way])
    all_left(xin.at[:, pl.ds(0, PL - 1)], p_send.at[0])
    all_left(zin.at[:, pl.ds(0, PL - 1)], y_send.at[0])
    for copy in stores:
        copy.wait()


def solution(mesh):
    sp_count = mesh.shape["sp"]
    tp_count = mesh.shape["tp"]

    def on_device(
        queries,
        key_heads,
        value_heads,
        sink_logit,
        out_weight,
        residual,
        norm_gain,
        expert_ids,
        route_weights,
        gate_weight,
        up_weight,
        down_weight,
    ):
        T, D = residual.shape
        HD = key_heads.shape[2]
        HEADS = queries.shape[1] // HD
        FF = gate_weight.shape[2]
        Z = sp_count // CORES
        PL = tp_count * CORES
        top_k = expert_ids.shape[1]
        CAP = max(2, 2 * top_k * T // (sp_count * tp_count))
        GR = 2 * CAP
        HOP = Z // 2
        keys_t = jnp.transpose(key_heads, (1, 2, 0)).reshape(HD, -1)
        values_t = jnp.transpose(value_heads, (1, 2, 0)).reshape(HD, -1)
        dma = pltpu.SemaphoreType.DMA
        vm = pltpu.VMEM
        any_space = pl.BlockSpec(memory_space=pl.ANY)
        dims = (T, D, Z, tp_count, sp_count, CAP, HEADS, HD)
        quarters = T // (PL * CAP)
        prefix = prefix_rows((HOP, HOP - 1), T, PL * CAP)
        pieces = sum(prefix(way, hop) // PIECE for way in range(2) for hop in range(1, HOP + 1))
        return pl.pallas_call(
            functools.partial(layer, dims),
            out_shape=jax.ShapeDtypeStruct((T, D), BF),
            in_specs=[any_space] * 12,
            out_specs=any_space,
            scratch_shapes=[
                vm(queries.shape, BF),
                vm((tp_count + 1, 2 * HD, T), BF),
                vm(out_weight.shape, BF),
                vm((D, FF), BF),
                vm((D, FF), BF),
                vm((FF, D), BF),
                pltpu.SMEM((1, HEADS), F32),
                vm((T, D), BF),
                vm((1, D), F32),
                vm((tp_count, top_k, T), jnp.int32),
                vm((top_k, T), F32),
                vm((tp_count, T, HEADS * HD), BF),
                vm((tp_count, T, HEADS * HD), BF),
                vm((2, T, D // 2), BF),
                vm((2, T, D // 2), BF),
                vm((2, T, D // 2), BF),
                vm((2, T, D // 2), BF),
                vm((2, T, D // 2), BF),
                vm((2, T, D // 2), BF),
                vm((T, D), F32),
                vm((T, D), BF),
                vm((T, D), BF),
                vm((T, D), BF),
                vm((HOP, 2, T, D), BF),
                vm((HOP, 2, 2 * Z, T), BF),
                vm((HOP, 8, T), F32),
                vm((3, T, T), BF),
                vm((2, T, T), BF),
                vm((HOP, PL, GR, D), BF),
                vm((HOP, PL, GR, D), BF),
                vm((HOP, PL, GR, D), BF),
                vm((HOP, PL, GR, D), BF),
                vm((HOP + 1, 2, T, D), BF),
                vm((2, T, D), F32),
                vm((T, D), BF),
                dma((10,)),
                dma((1,)),
                dma((2,)),
                dma((2,)),
                dma((3,)),
                dma((3 * quarters,)),
                dma((HOP,)),
                dma((pieces,)),
                dma((2,)),
                dma((2 * HOP - 1,)),
                dma((1,)),
                dma((HOP,)),
                dma((1,)),
                dma((HOP,)),
                dma((HOP,)),
                dma((pieces,)),
            ],
            compiler_params=pltpu.CompilerParams(
                collective_id=0, has_side_effects=True, vmem_limit_bytes=62 * 1024 * 1024
            ),
        )(
            queries,
            keys_t,
            values_t,
            sink_logit.reshape(1, HEADS),
            out_weight,
            residual,
            norm_gain.reshape(1, D),
            expert_ids.T,
            route_weights.T,
            gate_weight,
            up_weight,
            down_weight,
        )

    return jax.shard_map(
        on_device,
        mesh=mesh,
        in_specs=(
            P(("grp", "sp"), "tp"),
            P(("grp", "sp"), "tp", None),
            P(("grp", "sp"), "tp", None),
            P("tp"),
            P("tp", None),
            P(("grp", "sp", "tp"), None),
            P(),
            P(("grp", "sp", "tp"), None),
            P(("grp", "sp", "tp"), None),
            P(("sp", "tp"), None, None),
            P(("sp", "tp"), None, None),
            P(("sp", "tp"), None, None),
        ),
        out_specs=P(("grp", "sp", "tp"), None),
        check_vma=False,
    )
```
